128 devices in a mesh: sp: 64 (over z, y, x), tp: 2 (over core).
Axes of the slice: x: 4, y: 4, z: 4, core: 2. Of those that a mesh axis runs over, the one named last changes fastest.
Arguments:
- residual: bfloat16 [16384, 2048], P(('sp', 'tp')), may hold values from -6 to 6
- query_nope: bfloat16 [16384, 1024], P('sp', 'tp'), may hold values from -24 to 24
- query_rope: bfloat16 [16384, 512], P('sp', 'tp'), may hold values from -400 to 400
- latent: bfloat16 [16384, 256], P(('sp', 'tp')), may hold values from -6 to 6
- key_rope: bfloat16 [16384, 64], P(('sp', 'tp')), may hold values from -6 to 6
- key_up: bfloat16 [256, 1024], P(None, 'tp'), may hold values from -0.375 to 0.375
- value_up: bfloat16 [256, 1024], P(None, 'tp'), may hold values from -0.375 to 0.375
- out_proj: bfloat16 [1024, 2048], replicated, may hold values from -0.375 to 0.375
- norm_gain: float32 [2048], replicated, may hold values from 0.1 to 1.9
- routes: int32 [16384, 2], P(('sp', 'tp')), may hold values from 0 to 63, all different within a row; in each aligned block of 128 rows (0 to 127, 128 to 255, ...) at most 8 rows name the same one
- route_weight: float32 [16384, 2], P(('sp', 'tp')), may hold values from 0.3 to 2.5
- w_gate: bfloat16 [64, 2048, 512], P('sp', None, 'tp'), may hold values from -0.125 to 0.125
- w_up: bfloat16 [64, 2048, 512], P('sp', None, 'tp'), may hold values from -0.125 to 0.125
- w_down: bfloat16 [64, 512, 2048], P('sp', 'tp'), may hold values from -0.25 to 0.25
Outputs:
- mixed: bfloat16 [16384, 2048], P(('sp', 'tp'))
The draws below stay inside these ranges and needn't reach their ends.
Inputs may be any that keep to these rules, and one draw needn't show every extreme that they name: `routes`: each row names 2 different experts. Among the rows of one device no expert is named more than 8 times, a bound that some block reaches by the rows of some device.
All inputs are finite; a program needn't handle non-finite values.
Results may differ from the reference program's by a relative error of at most 0.015.
Values may be sent and summed in bfloat16 or wider, within the bound.
No kernel may reach another device: no remote copies, remote signals or barrier semaphores. Data moves between devices by JAX's collectives and lax.ppermute only.
A program may use at most 128 MiB of HBM per device.

```python
import math
import jax
import jax.numpy as jnp
import numpy as np
from jax import lax

D = 2048
HEADS = 8
QK_NOPE = 128
QK_ROPE = 64
V_DIM = 128
LATENT = 256
FF = 512
TOP = 2
SEGMENT = 64
TOK_DEV = 256
TOKENS = 16384
EXPERTS = 64
CAP = 8
N_SP = 64
N_TP = 2


def draw_key_rope(key, part):
    noise = jax.random.truncated_normal(jax.random.fold_in(key, 31), -6.0, 6.0, (TOKENS, QK_ROPE), jnp.float32)
    return noise.astype(jnp.bfloat16)


def draw_query_rope(key, part):
    noise = jax.random.truncated_normal(jax.random.fold_in(key, 32), -6.0, 6.0, (TOKENS, HEADS * QK_ROPE), jnp.float32)
    return noise.astype(jnp.bfloat16)


def steps_of(rng, dims, shards, low, largest):
    loudness, own = 1.0, jax.random.fold_in(rng, 6)
    for dim, blocks in shards:
        heights = jnp.exp(jax.random.uniform(jax.random.fold_in(own, dim), (blocks,), jnp.float32, low / len(shards), largest / len(shards)))
        loudness = loudness * jnp.repeat(heights, dims[dim] // blocks).reshape([-1 if axis == dim else 1 for axis in range(len(dims))])
    return loudness


def routed_block(key, own, number, rows, number_of, top, reach, skew):
    order = jax.random.permutation(key, number_of)
    crowded, usual = load_shares(number_of, rows * top, reach, skew, True), load_shares(number_of, rows * top, reach, skew, False)
    places = jnp.arange(number_of)

    def named(sizes, turn):
        used = int((sizes > 0).sum())
        fixed = max(1, used // 4)
        moved = fixed + (places - fixed + turn * (used - fixed)) % max(1, number_of - fixed)
        return jnp.zeros((number_of,), jnp.int32).at[order[jnp.where(places < fixed, places, moved)]].set(jnp.asarray(sizes, jnp.int32))

    sizes = jnp.where(number % 4 == 0, named(crowded, number // 4), named(usual, number - number // 4 - 1))
    mixed = jax.random.permutation(jax.random.fold_in(own, 3), number_of)
    donor, taker = mixed[0:number_of // 2 * 2:2], mixed[1:number_of // 2 * 2:2]
    slack = jnp.minimum(sizes[donor] - 1, reach - sizes[taker]) // 2
    slack = jnp.where((donor == order[0]) | (taker == order[0]) | (sizes[taker] == 0), 0, jnp.maximum(slack, 0))
    moved = jax.random.randint(jax.random.fold_in(own, 4), (number_of // 2,), 0, 1 << 20) % (slack + 1)
    sizes = sizes.at[donor].add(-moved).at[taker].add(moved)
    items = jnp.searchsorted(jnp.cumsum(sizes), jnp.arange(rows * top), side="right").astype(jnp.int32)
    grid = items.reshape(top, rows).T
    grid = grid[jax.random.permutation(jax.random.fold_in(own, 1), rows)]
    turn = jax.random.randint(jax.random.fold_in(own, 2), (rows, 1), 0, top)
    return jnp.take_along_axis(grid, (jnp.arange(top)[None, :] + turn) % top, axis=1)


def load_shares(count, total, most, slope, full):
    weights = [(1 << 20) // math.isqrt(standing ** slope) + 1 for standing in range(1, count + 1)]
    largest = most if full else min(most, max(-(-total // count), total * weights[0] // sum(weights)))
    least = 1 if total - largest >= count - 1 else 0
    holding, surplus = [largest] + [least] * (count - 1), total - largest - least * (count - 1)
    while surplus > 0:
        movable = [i for i in range(1, count) if holding[i] < largest] or [i for i in range(1, count) if holding[i] < most]
        whole, budget = sum([weights[i] for i in movable]), surplus
        for i in movable:
            addition = min(most - holding[i], max(1, budget * weights[i] // whole), surplus)
            holding[i] = holding[i] + addition
            surplus = surplus - addition
    return np.array(holding)


def normal_values(own_key, shape, width, most, split=(), held_as=jnp.bfloat16):
    values = jax.random.normal(own_key, shape, jnp.float32) * width
    if len(split) > 0:
        values = steps_of(own_key, shape, split, -0.22, 0.18) * values
    return jnp.clip(values, min=-most, max=most).astype(held_as)


def setup_inputs(seed: int = 0) -> dict:
    keys = jax.random.split(jax.random.key(seed), 15)
    residual = normal_values(keys[0], (TOKENS, D), 1.0, 6.0, ((0, 128),))
    query_nope = normal_values(keys[1], (TOKENS, HEADS * QK_NOPE), 4.0, 24.0, ((0, 64), (1, 2)))
    query_rope = draw_query_rope(jax.random.fold_in(keys[14], 71), 0)
    latent = normal_values(keys[3], (TOKENS, LATENT), 1.0, 6.0, ((0, 128),))
    key_rope = draw_key_rope(jax.random.fold_in(keys[14], 71), 0)
    key_up = normal_values(keys[5], (LATENT, HEADS * QK_NOPE), LATENT ** -0.5, 0.375, ((1, 2),))
    value_up = normal_values(keys[6], (LATENT, HEADS * V_DIM), LATENT ** -0.5, 0.375, ((1, 2),))
    out_proj = normal_values(keys[7], (HEADS * V_DIM, D), (HEADS * V_DIM // 4) ** -0.5, 0.375)
    norm_gain = jnp.clip(1.0 + 0.18 * jax.random.normal(keys[8], (D,), jnp.float32), 0.1, 1.9)
    routes_keys = jax.random.split(jax.random.fold_in(keys[9], 1), TOKENS // (TOK_DEV // N_TP))
    routes_turns = jax.random.permutation(jax.random.fold_in(keys[9], 3), TOKENS // (TOK_DEV // N_TP))
    routes = jax.vmap(lambda own, number: routed_block(jax.random.fold_in(keys[9], 2), own, number, TOK_DEV // N_TP, EXPERTS, TOP, CAP, 2))(routes_keys, routes_turns).reshape((TOKENS, TOP))
    route_weight = jnp.clip(jnp.exp(math.log(2.5) - 2.1202635 * jax.random.uniform(keys[10], (TOKENS, TOP), jnp.float32) ** steps_of(keys[10], (TOKENS, TOP), ((0, 128),), -0.2, 0.2)), 0.3, 2.5)
    w_gate = normal_values(keys[11], (EXPERTS, D, FF), D ** -0.5, 0.125, ((0, 64), (2, 2)))
    w_up = normal_values(keys[12], (EXPERTS, D, FF), D ** -0.5, 0.125, ((0, 64), (2, 2)))
    w_down = normal_values(keys[13], (EXPERTS, FF, D), FF ** -0.5, 0.25, ((0, 64), (1, 2)))
    return dict(residual=residual, query_nope=query_nope, query_rope=query_rope, latent=latent, key_rope=key_rope, key_up=key_up, value_up=value_up, out_proj=out_proj, norm_gain=norm_gain, routes=routes, route_weight=route_weight, w_gate=w_gate, w_up=w_up, w_down=w_down)


EPSILON = 1e-06
ROPE_BASE = 10000.0

def rotary(values, positions):
    half_width = values.shape[-1] // 2
    inverse = ROPE_BASE ** (-2.0 * jnp.arange(half_width, dtype=jnp.float32) / values.shape[-1])
    angles = positions.astype(jnp.float32)[:, None] * inverse[None, :]
    cosine = jnp.cos(angles)
    sine_part = jnp.sin(angles)
    if values.ndim == 3:
        cosine = cosine[:, None, :]
        sine_part = sine_part[:, None, :]
    first_half = values[..., :half_width]
    second = values[..., half_width:]
    return jnp.concatenate([first_half * cosine - second * sine_part, second * cosine + first_half * sine_part], axis=-1)

def reference(residual, query_nope, query_rope, latent, key_rope, key_up, value_up, out_proj, norm_gain, routes, route_weight, w_gate, w_up, w_down):
    positions = jnp.arange(TOKENS, dtype=jnp.int32)
    query_rot = rotary(query_rope.astype(jnp.float32).reshape(TOKENS, HEADS, QK_ROPE), positions).astype(jnp.bfloat16)
    key_rot = rotary(key_rope.astype(jnp.float32), positions).astype(jnp.bfloat16)
    key_nope = jnp.dot(latent, key_up, preferred_element_type=jnp.float32).astype(jnp.bfloat16)
    value_rows = jnp.dot(latent, value_up, preferred_element_type=jnp.float32).astype(jnp.bfloat16)
    keys_wide = key_nope.astype(jnp.float32).reshape(TOKENS, HEADS, QK_NOPE)
    values_wide = value_rows.astype(jnp.float32).reshape(TOKENS, HEADS, V_DIM)
    rot_wide = key_rot.astype(jnp.float32)
    query_wide = query_nope.astype(jnp.float32).reshape(TOKENS, HEADS, QK_NOPE)
    query_rot_wide = query_rot.astype(jnp.float32)
    score_scale = (QK_NOPE + QK_ROPE) ** (-0.5)
    key_segment = positions // SEGMENT
    query_block = math.gcd(TOKENS, 512)

    def one_block(block_index):
        first_row = (block_index * query_block).astype(jnp.int32)
        query_part = lax.dynamic_slice_in_dim(query_wide, first_row, query_block, 0)
        rot_part = lax.dynamic_slice_in_dim(query_rot_wide, first_row, query_block, 0)
        scores = jnp.einsum('qhd,khd->hqk', query_part, keys_wide)
        scores = (scores + jnp.einsum('qhr,kr->hqk', rot_part, rot_wide)) * score_scale
        query_segment = (first_row + jnp.arange(query_block, dtype=jnp.int32)) // SEGMENT
        allowed = (key_segment[None, :] <= query_segment[:, None])[None]
        scores = jnp.where(allowed, scores, -jnp.inf)
        row_max = lax.optimization_barrier(jnp.max(scores, axis=-1, keepdims=True))
        weights = jnp.exp(scores - row_max)
        weight_sum = lax.optimization_barrier(jnp.sum(weights, axis=-1))
        weights_low = lax.optimization_barrier(weights.astype(jnp.bfloat16)).astype(jnp.float32)
        weighted = jnp.einsum('hqk,khv->qhv', weights_low, values_wide)
        return weighted / weight_sum.T[:, :, None]
    attn_out = lax.map(one_block, jnp.arange(TOKENS // query_block, dtype=jnp.int32))
    attn_out = attn_out.reshape(TOKENS, HEADS * V_DIM).astype(jnp.bfloat16)
    projected = jnp.dot(attn_out, out_proj, preferred_element_type=jnp.float32)
    hidden = (residual.astype(jnp.float32) + projected).astype(jnp.bfloat16)
    hidden_wide = hidden.astype(jnp.float32)
    normed = hidden_wide * lax.rsqrt(lax.optimization_barrier(jnp.mean(hidden_wide * hidden_wide, axis=-1, keepdims=True)) + EPSILON)
    normed = (normed * norm_gain[None, :]).astype(jnp.bfloat16)
    buffer_rows = N_TP * N_SP * CAP
    flat_expert = routes.reshape(-1).astype(jnp.int32)
    onehot = (flat_expert[:, None] == jnp.arange(EXPERTS, dtype=jnp.int32)[None, :]).astype(jnp.int32)
    slot_rank = lax.optimization_barrier(jnp.sum(jnp.cumsum(onehot, axis=0) * onehot, axis=1)) - 1
    slot_index = (flat_expert * buffer_rows + slot_rank).astype(jnp.int32)
    buffer = jnp.zeros((EXPERTS * buffer_rows, D), jnp.bfloat16).at[slot_index].set(jnp.repeat(normed, TOP, axis=0))

    def expert_rows(inputs):
        rows_in, gate_weight, up_weight, down_weight = inputs
        gate_part = jnp.dot(rows_in, gate_weight, preferred_element_type=jnp.float32)
        up_part = jnp.dot(rows_in, up_weight, preferred_element_type=jnp.float32)
        activated = lax.optimization_barrier((jax.nn.silu(gate_part) * up_part).astype(jnp.bfloat16))
        parts = jnp.einsum('bpf,pfd->pbd', activated.astype(jnp.float32).reshape(buffer_rows, N_TP, FF // N_TP), down_weight.astype(jnp.float32).reshape(N_TP, FF // N_TP, D))
        half_out = lax.optimization_barrier(parts.astype(jnp.bfloat16)).astype(jnp.float32)
        return lax.optimization_barrier(jnp.sum(half_out, axis=0)).astype(jnp.bfloat16)
    outputs = lax.map(expert_rows, (buffer.reshape(EXPERTS, buffer_rows, D), w_gate, w_up, w_down))
    picked = outputs.reshape(EXPERTS * buffer_rows, D)[slot_index]
    combined = lax.optimization_barrier(jnp.sum(picked.astype(jnp.float32).reshape(TOKENS, TOP, D) * route_weight[:, :, None], axis=1))
    return (hidden_wide + combined).astype(jnp.bfloat16)
```

```python
import functools
import jax
import jax.numpy as jnp
import numpy as np
from jax import lax
from jax.experimental import pallas as pl
from jax.experimental.pallas import tpu as pltpu
from jax.sharding import PartitionSpec as P

QK_NOPE = 128
QK_ROPE = 64
V_DIM = 128
LATENT = 256
SEGMENT = 64
EPSILON = 1e-06
ROPE_BASE = 10000.0
NEG_LARGE = -1e30

N_SP = 64
N_TP = 2
HEADS_HERE = 4
ROWS = 128
SHARD = 160
UNIT = 4
KEYS = UNIT * ROWS
QROWS = HEADS_HERE * ROWS
CAP = 8
AXES = ("sp", "tp")
STEP = {"x": 1, "y": 4, "z": 16}
ORDER = (("z", "y", "x"), ("x", "z", "y"))
SHIFTS = (0, 1, -1, 2)
SCALE2 = float((QK_NOPE + QK_ROPE) ** (-0.5) * np.log2(np.e))


def moved(s, dim, by):
    step = STEP[dim]
    c = (s // step) % 4
    return s + step * ((c + by) % 4 - c)


def shift_pairs(phase, by):
    return [
        (s * N_TP + t, moved(s, ORDER[t][phase], by) * N_TP + t)
        for s in range(N_SP)
        for t in range(N_TP)
    ]


def shard_origin(s, t, k3, k2, k1):
    for phase, k in ((2, k3), (1, k2), (0, k1)):
        s = moved(s, ORDER[t][phase], -SHIFTS[k])
    return s


UNITS = 33
COLS = 12


@functools.lru_cache(None)
def work_table():
    table = np.zeros((N_SP * N_TP, UNITS + 1, COLS), np.int32)
    for s in range(N_SP):
        for t in range(N_TP):
            firsts = []
            for own in range(2):
                core = t if own == 0 else 1 - t
                for k3 in range(4):
                    for k2 in range(4):
                        for k1 in range(4):
                            firsts.append(4 * shard_origin(s, core, k3, k2, k1) + 2 * core)
            rows = []
            for group in range(2):
                base = 4 * s if group == 0 else 4 * (N_SP - 1 - s) + 2
                needed = [n for n in range(128) if firsts[n] <= base + 1]
                for at in range(0, len(needed), UNIT):
                    part = needed[at : at + UNIT]
                    segs = [firsts[n] for n in part]
                    masked = int(len(part) < UNIT or any(f + 1 > base for f in segs))
                    segs += [1 << 20] * (UNIT - len(part))
                    part = part + [part[-1]] * (UNIT - len(part))
                    rows.append([group, masked, base, t] + part + segs)
            assert len(rows) == UNITS
            rows.append(rows[-1])
            table[s * N_TP + t] = np.array(rows, np.int32)
    return table


def attention_body(
    units, qn_ref, q4_ref, key_up_ref, value_up_ref, *rest
):
    parts = rest[:8]
    out_ref = rest[8]
    keys, qabs, m_ref, l_ref, acc_ref, s0, s1, sems = rest[9:]
    part_rows = parts[0].shape[0]
    copies = []
    for n in range(8):
        copy = pltpu.make_async_copy(parts[n], keys.at[pl.ds(n * part_rows, part_rows)], sems.at[n])
        copy.start()
        copies.append(copy)
    nt = (((1,), (1,)), ((), ()))
    for g in range(2):
        for h in range(HEADS_HERE):
            cols = pl.ds(h * QK_NOPE, QK_NOPE)
            qabs[g, pl.ds(h * ROWS, ROWS), :] = lax.dot_general(
                qn_ref[g, :, cols], key_up_ref[:, cols], nt, preferred_element_type=jnp.float32
            ).astype(jnp.bfloat16)
    m_ref[...] = jnp.full(m_ref.shape, NEG_LARGE, jnp.float32)
    l_ref[...] = jnp.zeros(l_ref.shape, jnp.float32)
    acc_ref[...] = jnp.zeros(acc_ref.shape, jnp.float32)
    for copy in copies:
        copy.wait()

    def latent_tile(u, half):
        return jnp.concatenate(
            [keys[pl.ds(pl.multiple_of(units[u, 4 + j] * SHARD + half * SEGMENT, 32), SEGMENT), :] for j in range(UNIT)],
            axis=0,
        )

    def scores(u, s_ref):
        g = units[u, 0]
        rot = jnp.concatenate(
            [
                keys[pl.ds(pl.multiple_of(units[u, 4 + j] * SHARD + ROWS, 32), 32), pl.ds(h * 128, 128)]
                for j in range(UNIT)
                for h in range(2)
            ],
            axis=0,
        )
        q = qabs[g]
        for half in range(2):
            s_ref[:, pl.ds(half * 256, 256)] = lax.dot_general(
                q, latent_tile(u, half), nt, preferred_element_type=jnp.float32
            ) + lax.dot_general(q4_ref[g, half], rot, nt, preferred_element_type=jnp.float32)

    def fix(u, s_ref):
        @pl.when(units[u, 1] == 1)
        def _():
            lane = lax.broadcasted_iota(jnp.int32, (1, KEYS), 1)
            which = (lane % 256) // SEGMENT
            seg = jnp.full((1, KEYS), units[u, 8], jnp.int32)
            for j in range(1, UNIT):
                seg = jnp.where(which == j, units[u, 8 + j], seg)
            seg = seg + lane // 256
            row = lax.broadcasted_iota(jnp.int32, (QROWS, 1), 0)
            limit = units[u, 2] + (row % ROWS) // SEGMENT
            s_ref[...] = jnp.where(seg <= limit, s_ref[...], NEG_LARGE)

    def absorb(u, s_ref):
        g = units[u, 0]
        s = s_ref[...]
        before = m_ref[g][:, :1]
        after = jnp.maximum(before, jnp.max(s, axis=1, keepdims=True))
        p = jnp.exp2(s * SCALE2 - after * SCALE2)
        shrink = jnp.exp2((before - after) * SCALE2)
        partial = p[:, :128]
        for k in range(1, KEYS // 128):
            partial = partial + p[:, k * 128 : (k + 1) * 128]
        l_ref[g] = l_ref[g] * shrink + partial
        m_ref[g] = jnp.broadcast_to(after, (QROWS, 128))
        values = jnp.concatenate([latent_tile(u, 0), latent_tile(u, 1)], axis=0)
        acc_ref[g] = acc_ref[g] * shrink + jnp.dot(
            p.astype(jnp.bfloat16), values, preferred_element_type=jnp.float32
        )

    scores(0, s0)

    def pair(k, carry):
        u = k * 2
        fix(u, s0)
        scores(u + 1, s1)
        absorb(u, s0)
        fix(u + 1, s1)
        scores(u + 2, s0)
        absorb(u + 1, s1)
        return carry

    lax.fori_loop(0, UNITS // 2, pair, 0)
    fix(UNITS - 1, s0)
    absorb(UNITS - 1, s0)
    core = units[0, 3]
    for g in range(2):
        slot = 1 - core if g == 0 else core
        total = jnp.sum(l_ref[g], axis=1, keepdims=True)
        mean = (acc_ref[g] / total).astype(jnp.bfloat16)
        for h in range(HEADS_HERE):
            cols = pl.ds(h * V_DIM, V_DIM)
            out_ref[slot, :, cols] = jnp.dot(
                mean[h * ROWS : (h + 1) * ROWS], value_up_ref[:, cols], preferred_element_type=jnp.float32
            ).astype(jnp.bfloat16)


def attention(units, qn, q4, key_up, value_up, parts):
    vmem = pl.BlockSpec(memory_space=pltpu.VMEM)
    return pl.pallas_call(
        attention_body,
        out_shape=jax.ShapeDtypeStruct((2, ROWS, HEADS_HERE * V_DIM), jnp.bfloat16),
        in_specs=[pl.BlockSpec(memory_space=pltpu.SMEM)] + [vmem] * 4 + [pl.BlockSpec(memory_space=pl.ANY)] * 8,
        out_specs=vmem,
        scratch_shapes=[
            pltpu.VMEM((128 * SHARD, LATENT), jnp.bfloat16),
            pltpu.VMEM((2, QROWS, LATENT), jnp.bfloat16),
            pltpu.VMEM((2, QROWS, 128), jnp.float32),
            pltpu.VMEM((2, QROWS, 128), jnp.float32),
            pltpu.VMEM((2, QROWS, LATENT), jnp.float32),
            pltpu.VMEM((QROWS, KEYS), jnp.float32),
            pltpu.VMEM((QROWS, KEYS), jnp.float32),
            pltpu.SemaphoreType.DMA((8,)),
        ],
        compiler_params=pltpu.CompilerParams(vmem_limit_bytes=48 * 2**20),
        name="attention",
    )(units, qn, q4, key_up, value_up, *parts)


def project_body(first, second, out_proj, residual, gain, slots, hidden_ref, outgoing_ref):
    half = first.shape[1]
    projected = jnp.dot(first[...], out_proj[:half], preferred_element_type=jnp.float32) + jnp.dot(
        second[...], out_proj[half:], preferred_element_type=jnp.float32
    )
    hidden = (residual[...].astype(jnp.float32) + projected).astype(jnp.bfloat16)
    hidden_ref[...] = hidden
    wide = hidden.astype(jnp.float32)
    normed = wide * lax.rsqrt(jnp.mean(wide * wide, axis=-1, keepdims=True) + EPSILON)
    normed = (normed * gain[...]).astype(jnp.bfloat16)
    slot = lax.broadcasted_iota(jnp.int32, (outgoing_ref.shape[0], first.shape[0]), 0)
    pick = (slot == slots[0:1, :]) | (slot == slots[1:2, :])
    pick = jnp.where(pick, 1.0, 0.0).astype(jnp.bfloat16)
    outgoing_ref[...] = jnp.dot(pick, normed, preferred_element_type=jnp.float32).astype(jnp.bfloat16)


def project(first, second, out_proj, residual, gain, slots):
    width = residual.shape[1]
    vmem = pl.BlockSpec(memory_space=pltpu.VMEM)
    return pl.pallas_call(
        project_body,
        out_shape=(
            jax.ShapeDtypeStruct((ROWS, width), jnp.bfloat16),
            jax.ShapeDtypeStruct((N_SP * CAP, width), jnp.bfloat16),
        ),
        in_specs=[vmem] * 6,
        out_specs=(vmem, vmem),
        compiler_params=pltpu.CompilerParams(vmem_limit_bytes=40 * 2**20),
        name="project",
    )(first, second, out_proj, residual, gain, slots)


def experts_body(rows, gate_a, up_a, down_a, gate_b, up_b, down_b, out_ref):
    x = rows[...]
    halves = []
    for gate, up, down in ((gate_a, up_a, down_a), (gate_b, up_b, down_b)):
        gated = jnp.dot(x, gate[...], preferred_element_type=jnp.float32)
        raised = jnp.dot(x, up[...], preferred_element_type=jnp.float32)
        active = (gated / (1.0 + jnp.exp(-gated)) * raised).astype(jnp.bfloat16)
        halves.append(jnp.dot(active, down[...], preferred_element_type=jnp.float32).astype(jnp.bfloat16))
    out_ref[...] = (halves[0].astype(jnp.float32) + halves[1].astype(jnp.float32)).astype(jnp.bfloat16)


def experts(rows, own, other):
    count, width = rows.shape
    block = 256
    whole = lambda a: pl.BlockSpec(a.shape, lambda n: (0, 0))
    return pl.pallas_call(
        experts_body,
        grid=(count // block,),
        out_shape=jax.ShapeDtypeStruct((count, width), jnp.bfloat16),
        in_specs=[pl.BlockSpec((block, width), lambda n: (n, 0))] + [whole(a) for a in (*own, *other)],
        out_specs=pl.BlockSpec((block, width), lambda n: (n, 0)),
        compiler_params=pltpu.CompilerParams(
            dimension_semantics=("arbitrary",), vmem_limit_bytes=48 * 2**20
        ),
        name="experts",
    )(rows, *own, *other)


def combine_body(back, hidden, slots, weights, out_ref):
    slot = lax.broadcasted_iota(jnp.int32, (hidden.shape[0], back.shape[0]), 1)
    pick = jnp.where(slot == slots[:, 0:1], weights[:, 0:1], 0.0) + jnp.where(
        slot == slots[:, 1:2], weights[:, 1:2], 0.0
    )
    high = pick.astype(jnp.bfloat16)
    low = (pick - high.astype(jnp.float32)).astype(jnp.bfloat16)
    rows = back[...]
    mixed = jnp.dot(high, rows, preferred_element_type=jnp.float32) + jnp.dot(
        low, rows, preferred_element_type=jnp.float32
    )
    out_ref[...] = (hidden[...].astype(jnp.float32) + mixed).astype(jnp.bfloat16)


def combine(back, hidden, slots, weights):
    vmem = pl.BlockSpec(memory_space=pltpu.VMEM)
    return pl.pallas_call(
        combine_body,
        out_shape=jax.ShapeDtypeStruct(hidden.shape, jnp.bfloat16),
        in_specs=[vmem] * 4,
        out_specs=vmem,
        compiler_params=pltpu.CompilerParams(vmem_limit_bytes=32 * 2**20),
        name="combine",
    )(back, hidden, slots, weights)


def rotary(values, positions):
    half_width = values.shape[-1] // 2
    inverse = ROPE_BASE ** (-2.0 * jnp.arange(half_width, dtype=jnp.float32) / values.shape[-1])
    angles = positions.astype(jnp.float32)[:, None] * inverse[None, :]
    cosine = jnp.cos(angles)
    sine_part = jnp.sin(angles)
    if values.ndim == 3:
        cosine = cosine[:, None, :]
        sine_part = sine_part[:, None, :]
    first_half = values[..., :half_width]
    second = values[..., half_width:]
    return jnp.concatenate(
        [first_half * cosine - second * sine_part, second * cosine + first_half * sine_part],
        axis=-1,
    )


def gathered(shard):
    both = shard
    for phase in range(2):
        got = [both] + [lax.ppermute(both, AXES, shift_pairs(phase, by)) for by in SHIFTS[1:]]
        both = jnp.concatenate(got, axis=0)
    parts = [both] + [lax.ppermute(both, AXES, shift_pairs(2, by)) for by in SHIFTS[1:]]
    return parts


def local(
    residual,
    query_nope,
    query_rope,
    latent,
    key_rope,
    key_up,
    value_up,
    out_proj,
    norm_gain,
    routes,
    route_weight,
    w_gate,
    w_up,
    w_down,
):
    tp_index = lax.axis_index("tp")
    sp_index = lax.axis_index("sp")
    tok_dev = query_nope.shape[0]
    query_first = sp_index * tok_dev
    swap = [(0, 1), (1, 0)]

    key_pos = query_first + tp_index * ROWS + jnp.arange(ROWS, dtype=jnp.int32)
    key_rot = rotary(key_rope.astype(jnp.float32), key_pos).astype(jnp.bfloat16)
    packed = jnp.concatenate([key_rot[0:32], key_rot[64:96], key_rot[32:64], key_rot[96:128]], axis=1)
    shard = jnp.concatenate([latent, packed], axis=0)
    own_parts = gathered(shard)
    other_parts = [lax.ppermute(part, "tp", swap) for part in own_parts]

    query_pos = query_first + jnp.arange(tok_dev, dtype=jnp.int32)
    query_rot = rotary(
        query_rope.astype(jnp.float32).reshape(tok_dev, HEADS_HERE, QK_ROPE), query_pos
    ).astype(jnp.bfloat16)
    queries = jnp.concatenate([query_nope, query_rot.reshape(tok_dev, HEADS_HERE * QK_ROPE)], axis=1)
    mirror = [
        (s * N_TP + t, (N_SP - 1 - s) * N_TP + t) for s in range(N_SP) for t in range(N_TP)
    ]
    received = lax.ppermute(queries[ROWS:], AXES, mirror)
    sets = jnp.stack([queries[:ROWS], received])
    qn = sets[:, :, : HEADS_HERE * QK_NOPE]
    rot = sets[:, :, HEADS_HERE * QK_NOPE :].reshape(2, ROWS, HEADS_HERE, QK_ROPE)
    rot = jnp.swapaxes(rot, 1, 2).reshape(2, QROWS, QK_ROPE)
    none = jnp.zeros_like(rot)
    q4 = jnp.stack(
        [jnp.concatenate([rot, none], axis=-1), jnp.concatenate([none, rot], axis=-1)], axis=1
    )

    units = lax.dynamic_index_in_dim(
        jnp.asarray(work_table()), sp_index * N_TP + tp_index, 0, keepdims=False
    )
    attn = attention(units, qn, q4, key_up, value_up, own_parts + other_parts)
    cross = [(s * N_TP + 1, s * N_TP) for s in range(N_SP)] + [
        (s * N_TP, (N_SP - 1 - s) * N_TP + 1) for s in range(N_SP)
    ]
    straight = [(s * N_TP, s * N_TP) for s in range(N_SP)] + [
        (s * N_TP + 1, (N_SP - 1 - s) * N_TP + 1) for s in range(N_SP)
    ]
    crossed = lax.ppermute(attn[0], AXES, cross)
    kept = lax.ppermute(attn[1], AXES, straight)
    first = jnp.where(tp_index == 0, kept, crossed)
    second = jnp.where(tp_index == 0, crossed, kept)

    flat = routes.reshape(-1)
    order = jnp.arange(flat.shape[0], dtype=jnp.int32)
    earlier = (flat[:, None] == flat[None, :]) & (order[None, :] < order[:, None])
    rank = jnp.sum(earlier.astype(jnp.int32), axis=1)
    slots = (flat * CAP + rank).reshape(routes.shape)

    hidden, outgoing = project(first, second, out_proj, residual, norm_gain[None, :], slots.T)
    width = residual.shape[1]
    arrived = lax.all_to_all(
        outgoing.reshape(N_SP, CAP, width), "sp", split_axis=0, concat_axis=0, tiled=True
    ).reshape(N_SP * CAP, width)
    own = (w_gate[0], w_up[0], w_down[0])
    other = tuple(lax.ppermute(w, "tp", swap) for w in own)
    produced = experts(arrived, own, other)
    back = lax.all_to_all(
        produced.reshape(N_SP, CAP, width), "sp", split_axis=0, concat_axis=0, tiled=True
    ).reshape(N_SP * CAP, width)
    return combine(back, hidden, slots, route_weight)


def solution(mesh):
    return jax.shard_map(
        local,
        mesh=mesh,
        in_specs=(
            P(("sp", "tp"), None),
            P("sp", "tp"),
            P("sp", "tp"),
            P(("sp", "tp"), None),
            P(("sp", "tp"), None),
            P(None, "tp"),
            P(None, "tp"),
            P(),
            P(),
            P(("sp", "tp"), None),
            P(("sp", "tp"), None),
            P("sp", None, "tp"),
            P("sp", None, "tp"),
            P("sp", "tp", None),
        ),
        out_specs=P(("sp", "tp"), None),
        check_vma=False,
    )
```

```python
import functools
import jax
import jax.numpy as jnp
import numpy as np
from jax import lax
from jax.experimental import pallas as pl
from jax.experimental.pallas import tpu as pltpu
from jax.sharding import PartitionSpec as P

QK_NOPE = 128
QK_ROPE = 64
V_DIM = 128
LATENT = 256
SEGMENT = 64
EPSILON = 1e-06
ROPE_BASE = 10000.0
NEG_LARGE = -1e30

N_SP = 64
N_TP = 2
HEADS_HERE = 4
ROWS = 128
SHARD = 160
UNIT = 4
KEYS = UNIT * ROWS
QROWS = HEADS_HERE * ROWS
CAP = 8
AXES = ("sp", "tp")
STEP = {"x": 1, "y": 4, "z": 16}
Z_FIRST = {(0, 0): (3, 0), (1, 0): (2, 0), (0, 1): (1, 0), (1, 1): (0, 0), (2, 1): (1, 1), (3, 1): (0, 1), (2, 0): (3, 1), (3, 0): (2, 1)}
Z_SECOND = {(0, 1): (2, 0), (1, 1): (3, 0), (2, 0): (0, 1), (3, 0): (1, 1)}
ORDER = (("y", "x"), ("x", "y"))
SHIFTS = (0, 1, -1, 2)
SCALE2 = float((QK_NOPE + QK_ROPE) ** (-0.5) * np.log2(np.e))
PLANE = 16
COLS = 12
GROUPS = 4
CHUNK = 64
MESSAGE = HEADS_HERE * V_DIM + 128


def moved(s, dim, by):
    step = STEP[dim]
    c = (s // step) % 4
    return s + step * ((c + by) % 4 - c)


def shift_pairs(phase, by):
    return [
        (s * N_TP + t, moved(s, ORDER[t][phase], by) * N_TP + t)
        for s in range(N_SP)
        for t in range(N_TP)
    ]


def plane_pairs(table):
    return [
        ((from_z * PLANE + r) * N_TP + from_core, (z * PLANE + r) * N_TP + core)
        for (z, core), (from_z, from_core) in table.items()
        for r in range(PLANE)
    ]


def shard_first(s, t, k3, k2, kz):
    s = moved(s, ORDER[t][1], -SHIFTS[k3])
    s = moved(s, ORDER[t][0], -SHIFTS[k2])
    z, r = divmod(s, PLANE)
    source = (z, t)
    if kz == 1:
        source = Z_FIRST[source]
    elif source in Z_SECOND:
        source = Z_SECOND[source]
    return 4 * (source[0] * PLANE + r) + 2 * source[1]


@functools.lru_cache(None)
def work_table():
    lists = []
    for s in range(N_SP):
        for t in range(N_TP):
            firsts = [
                shard_first(s, core, k3, k2, kz)
                for core in (t, 1 - t)
                for k3 in range(4)
                for k2 in range(4)
                for kz in range(2)
            ]
            rows = []
            for group in range(GROUPS):
                block = s if group < 2 else N_SP - 1 - s
                base = 4 * block + 2 * (group % 2)
                needed = [n for n in range(len(firsts)) if firsts[n] <= base + 1]
                for at in range(0, len(needed), UNIT):
                    part = needed[at : at + UNIT]
                    segs = [firsts[n] for n in part]
                    masked = int(len(part) < UNIT or any(f + 1 > base for f in segs))
                    segs += [1 << 20] * (UNIT - len(part))
                    part = part + [part[-1]] * (UNIT - len(part))
                    rows.append([group, masked, base, t] + part + segs)
            lists.append(rows)
    count = max(len(rows) for rows in lists)
    count += 1 - count % 2
    table = []
    for rows in lists:
        idle = [rows[-1][:1] + [1] + rows[-1][2:8] + [1 << 20] * UNIT]
        table.append(rows + idle * (count + 1 - len(rows)))
    return count, np.array(table, np.int32).reshape(len(lists), -1)


def attention_body(steps, table, qn_ref, q4_ref, key_up_ref, value_up_ref, *rest):
    parts = rest[:8]
    out_ref = rest[8]
    keys, qabs, m_ref, l_ref, acc_ref, s0, s1, p_ref, shrink_ref, sems = rest[9:]
    part_rows = parts[0].shape[0]
    copies = []
    for n in range(8):
        copy = pltpu.make_async_copy(parts[n], keys.at[pl.ds(n * part_rows, part_rows)], sems.at[n])
        copy.start()
        copies.append(copy)
    nt = (((1,), (1,)), ((), ()))
    for g in range(GROUPS):
        for h in range(HEADS_HERE):
            cols = pl.ds(h * QK_NOPE, QK_NOPE)
            qabs[g, pl.ds(h * ROWS, ROWS), :] = lax.dot_general(
                qn_ref[g, :, cols], key_up_ref[:, cols], nt, preferred_element_type=jnp.float32
            ).astype(jnp.bfloat16)
    m_ref[...] = jnp.full(m_ref.shape, NEG_LARGE, jnp.float32)
    l_ref[...] = jnp.zeros(l_ref.shape, jnp.float32)
    acc_ref[...] = jnp.zeros(acc_ref.shape, jnp.float32)
    for copy in copies:
        copy.wait()

    def field(u, n):
        return table[u * COLS + n]

    def latent_tile(u, half):
        return jnp.concatenate(
            [
                keys[pl.ds(pl.multiple_of(field(u, 4 + j) * SHARD + half * SEGMENT, 32), SEGMENT), :]
                for j in range(UNIT)
            ],
            axis=0,
        )

    def scores(u, s_ref):
        g = field(u, 0)
        rot = jnp.concatenate(
            [
                keys[pl.ds(pl.multiple_of(field(u, 4 + j) * SHARD + ROWS, 32), 32), pl.ds(h * 128, 128)]
                for j in range(UNIT)
                for h in range(2)
            ],
            axis=0,
        )
        q = qabs[g]
        for half in range(2):
            s_ref[:, pl.ds(half * 256, 256)] = lax.dot_general(
                q, latent_tile(u, half), nt, preferred_element_type=jnp.float32
            ) + lax.dot_general(q4_ref[g, half], rot, nt, preferred_element_type=jnp.float32)

    def fix(u, s_ref):
        @pl.when(field(u, 1) == 1)
        def _():
            lane = lax.broadcasted_iota(jnp.int32, (1, KEYS), 1)
            which = (lane % 256) // SEGMENT
            seg = jnp.full((1, KEYS), field(u, 8), jnp.int32)
            for j in range(1, UNIT):
                seg = jnp.where(which == j, field(u, 8 + j), seg)
            seg = seg + lane // 256
            base = field(u, 2)
            for at in range(0, QROWS, SEGMENT):
                rows = pl.ds(at, SEGMENT)
                limit = base + (at % ROWS) // SEGMENT
                s_ref[rows, :] = jnp.where(seg <= limit, s_ref[rows, :], NEG_LARGE)

    def absorb(u, s_ref):
        g = field(u, 0)
        for at in range(0, QROWS, CHUNK):
            rows = pl.ds(at, CHUNK)
            s = s_ref[rows, :]
            before = m_ref[g, rows, :]
            top = s[:, :128]
            for k in range(1, KEYS // 128):
                top = jnp.maximum(top, s[:, k * 128 : (k + 1) * 128])
            after = jnp.maximum(before, jnp.max(top, axis=1, keepdims=True))
            m_ref[g, rows, :] = after
            shrink = jnp.exp2((before - after) * SCALE2)
            shrink_ref[rows, :] = shrink
            after = after * SCALE2
            partial = l_ref[g, rows, :] * shrink
            for k in range(KEYS // 128):
                p = jnp.exp2(s[:, k * 128 : (k + 1) * 128] * SCALE2 - after)
                partial = partial + p
                p_ref[rows, pl.ds(k * 128, 128)] = p.astype(jnp.bfloat16)
            l_ref[g, rows, :] = partial
        values = jnp.concatenate([latent_tile(u, 0), latent_tile(u, 1)], axis=0)
        product = jnp.dot(p_ref[...], values, preferred_element_type=jnp.float32)
        for k in range(LATENT // 128):
            cols = pl.ds(k * 128, 128)
            acc_ref[g, :, cols] = acc_ref[g, :, cols] * shrink_ref[...] + product[:, k * 128 : (k + 1) * 128]

    scores(0, s0)

    def pair(k, carry):
        u = k * 2
        fix(u, s0)
        scores(u + 1, s1)
        absorb(u, s0)
        fix(u + 1, s1)
        scores(u + 2, s0)
        absorb(u + 1, s1)
        return carry

    lax.fori_loop(0, steps // 2, pair, 0)
    fix(steps - 1, s0)
    absorb(steps - 1, s0)
    core = field(0, 3)
    lane = lax.broadcasted_iota(jnp.int32, (ROWS, 128), 1)
    for g in range(GROUPS):
        place = 2 * (g // 2) + jnp.where(core == g % 2, 0, 1)
        total = jnp.sum(l_ref[g], axis=1, keepdims=True)
        total = jnp.where(total > 0.0, total, 1.0)
        mean = (acc_ref[g] / total).astype(jnp.bfloat16)
        size = m_ref[g] * SCALE2 + jnp.log2(total)
        notes = jnp.zeros((ROWS, 128), jnp.bfloat16)
        for h in range(HEADS_HERE):
            cols = pl.ds(h * V_DIM, V_DIM)
            rows = slice(h * ROWS, (h + 1) * ROWS)
            out_ref[place, :, cols] = jnp.dot(
                mean[rows], value_up_ref[:, cols], preferred_element_type=jnp.float32
            ).astype(jnp.bfloat16)
            left = size[rows]
            for n in range(3):
                term = left.astype(jnp.bfloat16)
                notes = jnp.where(lane == n * HEADS_HERE + h, term, notes)
                left = left - term.astype(jnp.float32)
        out_ref[place, :, pl.ds(HEADS_HERE * V_DIM, 128)] = notes


def attention(table, qn, q4, key_up, value_up, parts):
    vmem = pl.BlockSpec(memory_space=pltpu.VMEM)
    steps = work_table()[0]
    return pl.pallas_call(
        functools.partial(attention_body, steps),
        out_shape=jax.ShapeDtypeStruct((4, ROWS, MESSAGE), jnp.bfloat16),
        in_specs=[pl.BlockSpec(memory_space=pltpu.SMEM)] + [vmem] * 4 + [pl.BlockSpec(memory_space=pl.ANY)] * 8,
        out_specs=vmem,
        scratch_shapes=[
            pltpu.VMEM((64 * SHARD, LATENT), jnp.bfloat16),
            pltpu.VMEM((GROUPS, QROWS, LATENT), jnp.bfloat16),
            pltpu.VMEM((GROUPS, QROWS, 128), jnp.float32),
            pltpu.VMEM((GROUPS, QROWS, 128), jnp.float32),
            pltpu.VMEM((GROUPS, QROWS, LATENT), jnp.float32),
            pltpu.VMEM((QROWS, KEYS), jnp.float32),
            pltpu.VMEM((QROWS, KEYS), jnp.float32),
            pltpu.VMEM((QROWS, KEYS), jnp.bfloat16),
            pltpu.VMEM((QROWS, 128), jnp.float32),
            pltpu.SemaphoreType.DMA((8,)),
        ],
        compiler_params=pltpu.CompilerParams(vmem_limit_bytes=24 * 2**20),
        name="attention",
    )(table, qn, q4, key_up, value_up, *parts)


def merged(one, two):
    width = HEADS_HERE * V_DIM
    outs = []
    for h in range(HEADS_HERE):
        sizes = []
        for part in (one, two):
            notes = part[:, width : width + 128].astype(jnp.float32)
            sizes.append(
                notes[:, h : h + 1] + notes[:, HEADS_HERE + h : HEADS_HERE + h + 1]
                + notes[:, 2 * HEADS_HERE + h : 2 * HEADS_HERE + h + 1]
            )
        most = jnp.maximum(sizes[0], sizes[1])
        first, second = (jnp.exp2(size - most) for size in sizes)
        cols = slice(h * V_DIM, (h + 1) * V_DIM)
        value = first * one[:, cols].astype(jnp.float32) + second * two[:, cols].astype(jnp.float32)
        outs.append((value / (first + second)).astype(jnp.bfloat16))
    return jnp.concatenate(outs, axis=1)


def project_body(core, local_part, mirror_same, swapped, mirror_cross, out_proj, residual, gain, slots, hidden_ref, outgoing_ref):
    half = HEADS_HERE * V_DIM
    mine = merged(local_part[...], mirror_same[...])
    theirs = merged(swapped[...], mirror_cross[...])
    at = pl.multiple_of(core[0] * half, half)
    other = pl.multiple_of((1 - core[0]) * half, half)
    projected = jnp.dot(mine, out_proj[pl.ds(at, half), :], preferred_element_type=jnp.float32) + jnp.dot(
        theirs, out_proj[pl.ds(other, half), :], preferred_element_type=jnp.float32
    )
    hidden = (residual[...].astype(jnp.float32) + projected).astype(jnp.bfloat16)
    hidden_ref[...] = hidden
    wide = hidden.astype(jnp.float32)
    normed = wide * lax.rsqrt(jnp.mean(wide * wide, axis=-1, keepdims=True) + EPSILON)
    normed = (normed * gain[...]).astype(jnp.bfloat16)
    slot = lax.broadcasted_iota(jnp.int32, (outgoing_ref.shape[0], hidden.shape[0]), 0)
    pick = (slot == slots[0:1, :]) | (slot == slots[1:2, :])
    pick = jnp.where(pick, 1.0, 0.0).astype(jnp.bfloat16)
    outgoing_ref[...] = jnp.dot(pick, normed, preferred_element_type=jnp.float32).astype(jnp.bfloat16)


def project(core, messages, out_proj, residual, gain, slots):
    width = residual.shape[1]
    vmem = pl.BlockSpec(memory_space=pltpu.VMEM)
    return pl.pallas_call(
        project_body,
        out_shape=(
            jax.ShapeDtypeStruct((ROWS, width), jnp.bfloat16),
            jax.ShapeDtypeStruct((N_SP * CAP, width), jnp.bfloat16),
        ),
        in_specs=[pl.BlockSpec(memory_space=pltpu.SMEM)] + [vmem] * 8,
        out_specs=(vmem, vmem),
        compiler_params=pltpu.CompilerParams(vmem_limit_bytes=20 * 2**20),
        name="project",
    )(core, *messages, out_proj, residual, gain, slots)


def experts_body(rows, gate_a, up_a, down_a, gate_b, up_b, down_b, out_ref):
    x = rows[...]
    halves = []
    for gate, up, down in ((gate_a, up_a, down_a), (gate_b, up_b, down_b)):
        gated = jnp.dot(x, gate[...], preferred_element_type=jnp.float32)
        raised = jnp.dot(x, up[...], preferred_element_type=jnp.float32)
        active = (gated / (1.0 + jnp.exp(-gated)) * raised).astype(jnp.bfloat16)
        halves.append(jnp.dot(active, down[...], preferred_element_type=jnp.float32).astype(jnp.bfloat16))
    out_ref[...] = (halves[0].astype(jnp.float32) + halves[1].astype(jnp.float32)).astype(jnp.bfloat16)


def experts(rows, own, other):
    count, width = rows.shape
    block = 256
    whole = lambda a: pl.BlockSpec(a.shape, lambda n: (0, 0))
    return pl.pallas_call(
        experts_body,
        grid=(count // block,),
        out_shape=jax.ShapeDtypeStruct((count, width), jnp.bfloat16),
        in_specs=[pl.BlockSpec((block, width), lambda n: (n, 0))] + [whole(a) for a in (*own, *other)],
        out_specs=pl.BlockSpec((block, width), lambda n: (n, 0)),
        compiler_params=pltpu.CompilerParams(
            dimension_semantics=("arbitrary",), vmem_limit_bytes=24 * 2**20
        ),
        name="experts",
    )(rows, *own, *other)


def combine_body(back, hidden, slots, weights, out_ref):
    slot = lax.broadcasted_iota(jnp.int32, (hidden.shape[0], back.shape[0]), 1)
    pick = jnp.where(slot == slots[:, 0:1], weights[:, 0:1], 0.0) + jnp.where(
        slot == slots[:, 1:2], weights[:, 1:2], 0.0
    )
    high = pick.astype(jnp.bfloat16)
    low = (pick - high.astype(jnp.float32)).astype(jnp.bfloat16)
    rows = back[...]
    mixed = jnp.dot(high, rows, preferred_element_type=jnp.float32) + jnp.dot(
        low, rows, preferred_element_type=jnp.float32
    )
    out_ref[...] = (hidden[...].astype(jnp.float32) + mixed).astype(jnp.bfloat16)


def combine(back, hidden, slots, weights):
    vmem = pl.BlockSpec(memory_space=pltpu.VMEM)
    return pl.pallas_call(
        combine_body,
        out_shape=jax.ShapeDtypeStruct(hidden.shape, jnp.bfloat16),
        in_specs=[vmem] * 4,
        out_specs=vmem,
        compiler_params=pltpu.CompilerParams(vmem_limit_bytes=16 * 2**20),
        name="combine",
    )(back, hidden, slots, weights)


def rotary(values, positions):
    half_width = values.shape[-1] // 2
    inverse = ROPE_BASE ** (-2.0 * jnp.arange(half_width, dtype=jnp.float32) / values.shape[-1])
    angles = positions.astype(jnp.float32)[:, None] * inverse[None, :]
    cosine = jnp.cos(angles)
    sine_part = jnp.sin(angles)
    if values.ndim == 3:
        cosine = cosine[:, None, :]
        sine_part = sine_part[:, None, :]
    first_half = values[..., :half_width]
    second = values[..., half_width:]
    return jnp.concatenate(
        [first_half * cosine - second * sine_part, second * cosine + first_half * sine_part],
        axis=-1,
    )


def local(
    residual,
    query_nope,
    query_rope,
    latent,
    key_rope,
    key_up,
    value_up,
    out_proj,
    norm_gain,
    routes,
    route_weight,
    w_gate,
    w_up,
    w_down,
):
    tp_index = lax.axis_index("tp")
    sp_index = lax.axis_index("sp")
    tok_dev = query_nope.shape[0]
    query_first = sp_index * tok_dev
    swap = [(0, 1), (1, 0)]

    key_pos = query_first + tp_index * ROWS + jnp.arange(ROWS, dtype=jnp.int32)
    key_rot = rotary(key_rope.astype(jnp.float32), key_pos).astype(jnp.bfloat16)
    packed = jnp.concatenate([key_rot[0:32], key_rot[64:96], key_rot[32:64], key_rot[96:128]], axis=1)
    shard = jnp.concatenate([latent, packed], axis=0)
    near = lax.ppermute(shard, AXES, plane_pairs(Z_FIRST))
    far = lax.ppermute(shard, AXES, plane_pairs(Z_SECOND))
    main = (tp_index == 0) == (sp_index < 2 * PLANE)
    both = jnp.concatenate([jnp.where(main, shard, far), near], axis=0)

    query_pos = query_first + jnp.arange(tok_dev, dtype=jnp.int32)
    query_rot = rotary(
        query_rope.astype(jnp.float32).reshape(tok_dev, HEADS_HERE, QK_ROPE), query_pos
    ).astype(jnp.bfloat16)
    queries = jnp.concatenate([query_nope, query_rot.reshape(tok_dev, HEADS_HERE * QK_ROPE)], axis=1)
    mirror = [
        (s * N_TP + t, (N_SP - 1 - s) * N_TP + t) for s in range(N_SP) for t in range(N_TP)
    ]
    crossing = [
        (s * N_TP + t, (N_SP - 1 - s) * N_TP + 1 - t) for s in range(N_SP) for t in range(N_TP)
    ]
    received = lax.ppermute(queries, AXES, mirror)

    got = [both] + [lax.ppermute(both, AXES, shift_pairs(0, by)) for by in SHIFTS[1:]]
    both = jnp.concatenate(got, axis=0)
    both, received = lax.optimization_barrier((both, received))
    own_parts = [both] + [lax.ppermute(both, AXES, shift_pairs(1, by)) for by in SHIFTS[1:]]
    other_parts = [lax.ppermute(part, "tp", swap) for part in own_parts]

    sets = jnp.concatenate([queries, received], axis=0).reshape(GROUPS, ROWS, -1)
    qn = sets[:, :, : HEADS_HERE * QK_NOPE]
    rot = sets[:, :, HEADS_HERE * QK_NOPE :].reshape(GROUPS, ROWS, HEADS_HERE, QK_ROPE)
    rot = jnp.swapaxes(rot, 1, 2).reshape(GROUPS, QROWS, QK_ROPE)
    none = jnp.zeros_like(rot)
    q4 = jnp.stack(
        [jnp.concatenate([rot, none], axis=-1), jnp.concatenate([none, rot], axis=-1)], axis=1
    )
    table = lax.dynamic_index_in_dim(
        jnp.asarray(work_table()[1]), sp_index * N_TP + tp_index, 0, keepdims=False
    )
    attn = attention(table, qn, q4, key_up, value_up, own_parts + other_parts)
    mirror_same = lax.ppermute(attn[2], AXES, mirror)
    mirror_cross = lax.ppermute(attn[3], AXES, crossing)
    swapped = lax.ppermute(attn[1], "tp", swap)
    messages = (attn[0], mirror_same, swapped, mirror_cross)

    flat = routes.reshape(-1)
    order = jnp.arange(flat.shape[0], dtype=jnp.int32)
    earlier = (flat[:, None] == flat[None, :]) & (order[None, :] < order[:, None])
    rank = jnp.sum(earlier.astype(jnp.int32), axis=1)
    slots = (flat * CAP + rank).reshape(routes.shape)

    hidden, outgoing = project(
        tp_index.reshape(1).astype(jnp.int32), messages, out_proj, residual, norm_gain[None, :], slots.T
    )
    width = residual.shape[1]
    arrived = lax.all_to_all(
        outgoing.reshape(N_SP, CAP, width), "sp", split_axis=0, concat_axis=0, tiled=True
    ).reshape(N_SP * CAP, width)
    own = (w_gate[0], w_up[0], w_down[0])
    other = tuple(lax.ppermute(w, "tp", swap) for w in own)
    produced = experts(arrived, own, other)
    back = lax.all_to_all(
        produced.reshape(N_SP, CAP, width), "sp", split_axis=0, concat_axis=0, tiled=True
    ).reshape(N_SP * CAP, width)
    return combine(back, hidden, slots, route_weight)


def solution(mesh):
    return jax.shard_map(
        local,
        mesh=mesh,
        in_specs=(
            P(("sp", "tp"), None),
            P("sp", "tp"),
            P("sp", "tp"),
            P(("sp", "tp"), None),
            P(("sp", "tp"), None),
            P(None, "tp"),
            P(None, "tp"),
            P(),
            P(),
            P(("sp", "tp"), None),
            P(("sp", "tp"), None),
            P("sp", None, "tp"),
            P("sp", None, "tp"),
            P("sp", "tp", None),
        ),
        out_specs=P(("sp", "tp"), None),
        check_vma=False,
    )
```

```python
import functools
import jax
import jax.numpy as jnp
import numpy as np
from jax import lax
from jax.experimental import pallas as pl
from jax.experimental.pallas import tpu as pltpu
from jax.sharding import PartitionSpec as P

QK_NOPE = 128
QK_ROPE = 64
V_DIM = 128
LATENT = 256
SEGMENT = 64
EPSILON = 1e-06
ROPE_BASE = 10000.0
NEG_LARGE = -1e30

N_SP = 64
N_TP = 2
HEADS_HERE = 4
ROWS = 128
SHARD = 160
UNIT = 4
KEYS = UNIT * ROWS
QROWS = HEADS_HERE * ROWS
CAP = 8
AXES = ("sp", "tp")
STEP = {"x": 1, "y": 4, "z": 16}
Z_FIRST = {(0, 0): (3, 0), (1, 0): (2, 0), (0, 1): (1, 0), (1, 1): (0, 0), (2, 1): (1, 1), (3, 1): (0, 1), (2, 0): (3, 1), (3, 0): (2, 1)}
Z_SECOND = {(0, 1): (2, 0), (1, 1): (3, 0), (2, 0): (0, 1), (3, 0): (1, 1)}
ORDER = (("y", "x"), ("x", "y"))
SHIFTS = (0, 1, -1, 2)
SCALE2 = float((QK_NOPE + QK_ROPE) ** (-0.5) * np.log2(np.e))
PLANE = 16
GROUPS = 4
CHUNK = 64
MESSAGE = HEADS_HERE * V_DIM + 128


def moved(s, dim, by):
    step = STEP[dim]
    c = (s // step) % 4
    return s + step * ((c + by) % 4 - c)


def shift_pairs(phase, by):
    return [
        (s * N_TP + t, moved(s, ORDER[t][phase], by) * N_TP + t)
        for s in range(N_SP)
        for t in range(N_TP)
    ]


def plane_pairs(table):
    return [
        ((from_z * PLANE + r) * N_TP + from_core, (z * PLANE + r) * N_TP + core)
        for (z, core), (from_z, from_core) in table.items()
        for r in range(PLANE)
    ]


def shard_first(s, t, k3, k2, kz):
    s = moved(s, ORDER[t][1], -SHIFTS[k3])
    s = moved(s, ORDER[t][0], -SHIFTS[k2])
    z, r = divmod(s, PLANE)
    source = (z, t)
    if kz == 1:
        source = Z_FIRST[source]
    elif source in Z_SECOND:
        source = Z_SECOND[source]
    return 4 * (source[0] * PLANE + r) + 2 * source[1]


CALLS = (((0, 0), (1, 0)), ((0, 1), (0, 2), (0, 3)), ((1, 1), (1, 2), (1, 3)))
PART_SHARDS = 8


@functools.lru_cache(None)
def work_table(call):
    lists = []
    for s in range(N_SP):
        for t in range(N_TP):
            firsts = [
                shard_first(s, t if own == 0 else 1 - t, k3, k2, kz)
                for own, k3 in CALLS[call]
                for k2 in range(4)
                for kz in range(2)
            ]
            rows = []
            for group in range(GROUPS):
                block = s if group < 2 else N_SP - 1 - s
                base = 4 * block + 2 * (group % 2)
                needed = [n for n in range(len(firsts)) if firsts[n] <= base + 1]
                for at in range(0, len(needed), UNIT):
                    part = needed[at : at + UNIT]
                    segs = [firsts[n] for n in part] + [1 << 20] * (UNIT - len(part))
                    part = part + [part[-1]] * (UNIT - len(part))
                    bits = 0
                    for half in range(2):
                        for j in range(UNIT):
                            for late in range(2):
                                if segs[j] + half > base + late:
                                    bits |= 1 << ((half * UNIT + j) * 2 + late)
                    rows.append([group, bits, t] + part)
            lists.append(rows)
    count = max(len(rows) for rows in lists)
    count += 1 - count % 2
    everything = (1 << (4 * UNIT)) - 1
    idle = lambda rows, t: rows[-1][:1] + [everything] + rows[-1][2:] if rows else [0, everything, t] + [0] * UNIT
    table = []
    for n, rows in enumerate(lists):
        table.append(rows + [idle(rows, n % N_TP)] * (count + 1 - len(rows)))
    return count, np.array(table, np.int32).reshape(len(lists), -1)


NT = (((1,), (1,)), ((), ()))


def attention_body(call, steps, part_count, table, *rest):
    first, last = call == 0, call == len(CALLS) - 1
    if first:
        qn_ref, key_up_ref, q4_ref = rest[:3]
        taken = 3
    else:
        q4_ref, qabs, m_in, l_in, acc_in = rest[:5]
        taken = 5
    if last:
        value_up_ref = rest[taken]
        taken += 1
    parts = rest[taken : taken + part_count]
    taken += part_count
    if first:
        qabs, m_ref, l_ref, acc_ref = rest[taken : taken + 4]
        taken += 4
    elif last:
        out_ref, m_ref, l_ref, acc_ref = rest[taken : taken + 4]
        taken += 4
    else:
        m_ref, l_ref, acc_ref = rest[taken : taken + 3]
        taken += 3
    keys, s0, s1, p0, p1, shrink0, shrink1, sems = rest[taken:]
    part_rows = parts[0].shape[0]
    copies = []
    for n in range(part_count):
        copy = pltpu.make_async_copy(parts[n], keys.at[pl.ds(n * part_rows, part_rows)], sems.at[n])
        copy.start()
        copies.append(copy)
    if first:
        for g in range(GROUPS):
            for h in range(HEADS_HERE):
                cols = pl.ds(h * QK_NOPE, QK_NOPE)
                qabs[g, pl.ds(h * ROWS, ROWS), :] = lax.dot_general(
                    qn_ref[g, :, cols], key_up_ref[:, cols], NT, preferred_element_type=jnp.float32
                ).astype(jnp.bfloat16)
        m_ref[...] = jnp.full(m_ref.shape, NEG_LARGE, jnp.float32)
        l_ref[...] = jnp.zeros(l_ref.shape, jnp.float32)
        acc_ref[...] = jnp.zeros(acc_ref.shape, jnp.float32)
    else:
        m_ref[...] = m_in[...]
        l_ref[...] = l_in[...]
        acc_ref[...] = acc_in[...]
    for copy in copies:
        copy.wait()

    cols_per_step = 3 + UNIT

    def field(u, n):
        return table[u * cols_per_step + n]

    def latent_tile(u, half):
        return jnp.concatenate(
            [
                keys[pl.ds(pl.multiple_of(field(u, 3 + j) * SHARD + half * SEGMENT, 32), SEGMENT), :]
                for j in range(UNIT)
            ],
            axis=0,
        )

    note_lane = lax.broadcasted_iota(jnp.int32, (16, 128), 1)

    def scores(u, s_ref):
        g = field(u, 0)
        bits = field(u, 1)
        rot = jnp.concatenate(
            [
                keys[pl.ds(pl.multiple_of(field(u, 3 + j) * SHARD + ROWS, 32), 32), pl.ds(h * 128, 128)]
                for j in range(UNIT)
                for h in range(2)
            ],
            axis=0,
        )
        q = qabs[g]
        for half in range(2):
            notes = []
            for j in range(UNIT):
                at = (half * UNIT + j) * 2
                early, late = (
                    jnp.where((bits >> (at + n)) & 1 == 1, jnp.float32(NEG_LARGE), jnp.float32(0.0)) for n in range(2)
                )
                note = jnp.where(note_lane == 0, early, jnp.where(note_lane == 1, late, 0.0)).astype(jnp.bfloat16)
                notes += [note] * (SEGMENT // 16)
            extra = jnp.concatenate([rot, jnp.concatenate(notes, axis=0)], axis=1)
            s_ref[:, pl.ds(half * 256, 256)] = lax.dot_general(
                q, latent_tile(u, half), NT, preferred_element_type=jnp.float32
            ) + lax.dot_general(q4_ref[g, half], extra, NT, preferred_element_type=jnp.float32)

    def absorb(u, s_ref, p_ref, shrink_ref):
        g = field(u, 0)
        for at in range(0, QROWS, CHUNK):
            rows = pl.ds(at, CHUNK)
            s = s_ref[rows, :]
            before = m_ref[g, rows, :]
            top = s[:, :128]
            for k in range(1, KEYS // 128):
                top = jnp.maximum(top, s[:, k * 128 : (k + 1) * 128])
            after = jnp.maximum(before, jnp.max(top, axis=1, keepdims=True))
            m_ref[g, rows, :] = after
            shrink = jnp.exp2((before - after) * SCALE2)
            shrink_ref[rows, :] = shrink
            after = after * SCALE2
            partial = l_ref[g, rows, :] * shrink
            for k in range(KEYS // 128):
                p = jnp.exp2(s[:, k * 128 : (k + 1) * 128] * SCALE2 - after)
                partial = partial + p
                p_ref[rows, pl.ds(k * 128, 128)] = p.astype(jnp.bfloat16)
            l_ref[g, rows, :] = partial
        values = jnp.concatenate([latent_tile(u, 0), latent_tile(u, 1)], axis=0)
        for at in range(0, QROWS, QROWS // 2):
            rows = pl.ds(at, QROWS // 2)
            product = jnp.dot(p_ref[rows, :], values, preferred_element_type=jnp.float32)
            for k in range(LATENT // 128):
                cols = pl.ds(k * 128, 128)
                acc_ref[g, rows, cols] = (
                    acc_ref[g, rows, cols] * shrink_ref[rows, :] + product[:, k * 128 : (k + 1) * 128]
                )

    scores(0, s0)

    def pair(k, carry):
        u = k * 2
        scores(u + 1, s1)
        absorb(u, s0, p0, shrink0)
        scores(u + 2, s0)
        absorb(u + 1, s1, p1, shrink1)
        return carry

    lax.fori_loop(0, steps // 2, pair, 0)
    absorb(steps - 1, s0, p0, shrink0)
    if not last:
        return
    core = field(0, 2)
    lane = lax.broadcasted_iota(jnp.int32, (ROWS, 128), 1)
    for g in range(GROUPS):
        place = 2 * (g // 2) + jnp.where(core == g % 2, 0, 1)
        total = jnp.sum(l_ref[g], axis=1, keepdims=True)
        total = jnp.where(total > 0.0, total, 1.0)
        mean = (acc_ref[g] / total).astype(jnp.bfloat16)
        size = m_ref[g] * SCALE2 + jnp.log2(total)
        notes = jnp.zeros((ROWS, 128), jnp.bfloat16)
        for h in range(HEADS_HERE):
            cols = pl.ds(h * V_DIM, V_DIM)
            rows = slice(h * ROWS, (h + 1) * ROWS)
            out_ref[place, :, cols] = jnp.dot(
                mean[rows], value_up_ref[:, cols], preferred_element_type=jnp.float32
            ).astype(jnp.bfloat16)
            left = size[rows]
            for n in range(3):
                term = left.astype(jnp.bfloat16)
                notes = jnp.where(lane == n * HEADS_HERE + h, term, notes)
                left = left - term.astype(jnp.float32)
        out_ref[place, :, pl.ds(HEADS_HERE * V_DIM, 128)] = notes


def attention(call, table, operands, parts):
    vmem = pl.BlockSpec(memory_space=pltpu.VMEM)
    steps = work_table(call)[0]
    first, last = call == 0, call == len(CALLS) - 1
    f32 = lambda width: jax.ShapeDtypeStruct((GROUPS, QROWS, width), jnp.float32)
    state = [f32(128), f32(128), f32(LATENT)]
    scratch = []
    if first:
        outs = [jax.ShapeDtypeStruct((GROUPS, QROWS, LATENT), jnp.bfloat16)] + state
    elif last:
        outs = [jax.ShapeDtypeStruct((4, ROWS, MESSAGE), jnp.bfloat16)]
        scratch = [pltpu.VMEM(s.shape, s.dtype) for s in state]
    else:
        outs = state
    work = steps * QROWS * KEYS * 3 * LATENT * 2
    return pl.pallas_call(
        functools.partial(attention_body, call, steps, len(parts)),
        out_shape=outs,
        in_specs=[pl.BlockSpec(memory_space=pltpu.SMEM)]
        + [vmem] * len(operands)
        + [pl.BlockSpec(memory_space=pl.ANY)] * len(parts),
        out_specs=[vmem] * len(outs),
        scratch_shapes=scratch
        + [
            pltpu.VMEM((len(parts) * PART_SHARDS * SHARD, LATENT), jnp.bfloat16),
            pltpu.VMEM((QROWS, KEYS), jnp.float32),
            pltpu.VMEM((QROWS, KEYS), jnp.float32),
            pltpu.VMEM((QROWS, KEYS), jnp.bfloat16),
            pltpu.VMEM((QROWS, KEYS), jnp.bfloat16),
            pltpu.VMEM((QROWS, 128), jnp.float32),
            pltpu.VMEM((QROWS, 128), jnp.float32),
            pltpu.SemaphoreType.DMA((len(parts),)),
        ],
        cost_estimate=pl.CostEstimate(
            flops=work, bytes_accessed=2**20, transcendentals=steps * QROWS * KEYS
        ),
        compiler_params=pltpu.CompilerParams(vmem_limit_bytes=24 * 2**20),
    )(table, *operands, *parts)


def in_hbm(x):
    return pltpu.with_memory_space_constraint(x, pltpu.HBM)


def merged(one, two):
    width = HEADS_HERE * V_DIM
    outs = []
    for h in range(HEADS_HERE):
        sizes = []
        for part in (one, two):
            notes = part[:, width : width + 128].astype(jnp.float32)
            sizes.append(
                notes[:, h : h + 1] + notes[:, HEADS_HERE + h : HEADS_HERE + h + 1]
                + notes[:, 2 * HEADS_HERE + h : 2 * HEADS_HERE + h + 1]
            )
        most = jnp.maximum(sizes[0], sizes[1])
        first, second = (jnp.exp2(size - most) for size in sizes)
        cols = slice(h * V_DIM, (h + 1) * V_DIM)
        value = first * one[:, cols].astype(jnp.float32) + second * two[:, cols].astype(jnp.float32)
        outs.append((value / (first + second)).astype(jnp.bfloat16))
    return jnp.concatenate(outs, axis=1)


PIECES = 4


def project_body(
    core, local_part, mirror_same, swapped, mirror_cross, gain, slots, residual_hbm, out_proj_hbm,
    hidden_hbm, outgoing_hbm, residual, out_proj, projected, hidden, outgoing, sems, out_sems,
):
    width = residual.shape[1]
    piece = width // PIECES
    loads = [pltpu.make_async_copy(residual_hbm, residual, sems.at[PIECES])]
    for n in range(PIECES):
        cols = pl.ds(n * piece, piece)
        loads.append(pltpu.make_async_copy(out_proj_hbm.at[:, cols], out_proj.at[:, cols], sems.at[n]))
    for load in loads[1:] + loads[:1]:
        load.start()
    half = HEADS_HERE * V_DIM
    mine = merged(local_part[...], mirror_same[...])
    theirs = merged(swapped[...], mirror_cross[...])
    at = pl.multiple_of(core[0] * half, half)
    other = pl.multiple_of((1 - core[0]) * half, half)
    for n in range(PIECES):
        cols = pl.ds(n * piece, piece)
        loads[1 + n].wait()
        projected[:, cols] = jnp.dot(
            mine, out_proj[pl.ds(at, half), cols], preferred_element_type=jnp.float32
        ) + jnp.dot(theirs, out_proj[pl.ds(other, half), cols], preferred_element_type=jnp.float32)
    loads[0].wait()
    result = (residual[...].astype(jnp.float32) + projected[...]).astype(jnp.bfloat16)
    hidden[...] = result
    store = pltpu.make_async_copy(hidden, hidden_hbm, out_sems.at[PIECES])
    store.start()
    wide = result.astype(jnp.float32)
    normed = wide * lax.rsqrt(jnp.mean(wide * wide, axis=-1, keepdims=True) + EPSILON)
    normed = (normed * gain[...]).astype(jnp.bfloat16)
    count = outgoing.shape[0] // PIECES
    stores = [store]
    for n in range(PIECES):
        slot = lax.broadcasted_iota(jnp.int32, (count, normed.shape[0]), 0) + n * count
        pick = (slot == slots[0:1, :]) | (slot == slots[1:2, :])
        pick = jnp.where(pick, 1.0, 0.0).astype(jnp.bfloat16)
        rows = pl.ds(n * count, count)
        outgoing[rows, :] = jnp.dot(pick, normed, preferred_element_type=jnp.float32).astype(jnp.bfloat16)
        store = pltpu.make_async_copy(outgoing.at[rows], outgoing_hbm.at[rows], out_sems.at[n])
        store.start()
        stores.append(store)
    for store in stores:
        store.wait()


def project(core, messages, out_proj, residual, gain, slots):
    width = residual.shape[1]
    vmem = pl.BlockSpec(memory_space=pltpu.VMEM)
    hbm = pl.BlockSpec(memory_space=pltpu.HBM)
    return pl.pallas_call(
        project_body,
        out_shape=(
            pltpu.HBM((ROWS, width), jnp.bfloat16),
            pltpu.HBM((N_SP * CAP, width), jnp.bfloat16),
        ),
        in_specs=[pl.BlockSpec(memory_space=pltpu.SMEM)] + [vmem] * 6 + [hbm] * 2,
        out_specs=(hbm, hbm),
        scratch_shapes=[
            pltpu.VMEM((ROWS, width), jnp.bfloat16),
            pltpu.VMEM(out_proj.shape, jnp.bfloat16),
            pltpu.VMEM((ROWS, width), jnp.float32),
            pltpu.VMEM((ROWS, width), jnp.bfloat16),
            pltpu.VMEM((N_SP * CAP, width), jnp.bfloat16),
            pltpu.SemaphoreType.DMA((PIECES + 1,)),
            pltpu.SemaphoreType.DMA((PIECES + 1,)),
        ],
        compiler_params=pltpu.CompilerParams(vmem_limit_bytes=20 * 2**20),
        name="project",
    )(core, *messages, gain, slots, in_hbm(residual), in_hbm(out_proj))


def experts_body(rows, *rest):
    sources = rest[:6]
    out_hbm = rest[6]
    weights = rest[7:13]
    first, out, sems, out_sems = rest[13:]
    loads = []
    for n in range(6):
        load = pltpu.make_async_copy(sources[n], weights[n], sems.at[n])
        load.start()
        loads.append(load)
    count = rows.shape[0]
    block = count // 2
    stores = []
    for n in range(2):
        gate, up, down = weights[3 * n : 3 * n + 3]
        for k in range(2):
            at = pl.ds(k * block, block)
            x = rows[at, :]
            if k == 0:
                loads[3 * n].wait()
            gated = jnp.dot(x, gate[...], preferred_element_type=jnp.float32)
            if k == 0:
                loads[3 * n + 1].wait()
            raised = jnp.dot(x, up[...], preferred_element_type=jnp.float32)
            active = (gated / (1.0 + jnp.exp(-gated)) * raised).astype(jnp.bfloat16)
            if k == 0:
                loads[3 * n + 2].wait()
            product = jnp.dot(active, down[...], preferred_element_type=jnp.float32).astype(jnp.bfloat16)
            if n == 0:
                first[at, :] = product
            else:
                out[at, :] = (first[at, :].astype(jnp.float32) + product.astype(jnp.float32)).astype(jnp.bfloat16)
                store = pltpu.make_async_copy(out.at[at], out_hbm.at[at], out_sems.at[k])
                store.start()
                stores.append(store)
    for store in stores:
        store.wait()


def experts(rows, own, other):
    count, width = rows.shape
    hbm = pl.BlockSpec(memory_space=pltpu.HBM)
    return pl.pallas_call(
        experts_body,
        out_shape=pltpu.HBM((count, width), jnp.bfloat16),
        in_specs=[pl.BlockSpec(memory_space=pltpu.VMEM)] + [hbm] * 6,
        out_specs=hbm,
        scratch_shapes=[pltpu.VMEM(w.shape, w.dtype) for w in (*own, *other)]
        + [
            pltpu.VMEM((count, width), jnp.bfloat16),
            pltpu.VMEM((count, width), jnp.bfloat16),
            pltpu.SemaphoreType.DMA((6,)),
            pltpu.SemaphoreType.DMA((2,)),
        ],
        compiler_params=pltpu.CompilerParams(vmem_limit_bytes=28 * 2**20),
        name="experts",
    )(rows, *[in_hbm(w) for w in (*own, *other)])


def combine_body(back, hidden, slots, weights, out_ref):
    slot = lax.broadcasted_iota(jnp.int32, (hidden.shape[0], back.shape[0]), 1)
    pick = jnp.where(slot == slots[:, 0:1], weights[:, 0:1], 0.0) + jnp.where(
        slot == slots[:, 1:2], weights[:, 1:2], 0.0
    )
    high = pick.astype(jnp.bfloat16)
    low = (pick - high.astype(jnp.float32)).astype(jnp.bfloat16)
    rows = back[...]
    mixed = jnp.dot(high, rows, preferred_element_type=jnp.float32) + jnp.dot(
        low, rows, preferred_element_type=jnp.float32
    )
    out_ref[...] = (hidden[...].astype(jnp.float32) + mixed).astype(jnp.bfloat16)


def combine(back, hidden, slots, weights):
    vmem = pl.BlockSpec(memory_space=pltpu.VMEM)
    return pl.pallas_call(
        combine_body,
        out_shape=jax.ShapeDtypeStruct(hidden.shape, jnp.bfloat16),
        in_specs=[vmem] * 4,
        out_specs=vmem,
        compiler_params=pltpu.CompilerParams(vmem_limit_bytes=16 * 2**20),
        name="combine",
    )(back, hidden, slots, weights)


def rotary(values, positions):
    half_width = values.shape[-1] // 2
    inverse = ROPE_BASE ** (-2.0 * jnp.arange(half_width, dtype=jnp.float32) / values.shape[-1])
    angles = positions.astype(jnp.float32)[:, None] * inverse[None, :]
    cosine = jnp.cos(angles)
    sine_part = jnp.sin(angles)
    if values.ndim == 3:
        cosine = cosine[:, None, :]
        sine_part = sine_part[:, None, :]
    first_half = values[..., :half_width]
    second = values[..., half_width:]
    return jnp.concatenate(
        [first_half * cosine - second * sine_part, second * cosine + first_half * sine_part],
        axis=-1,
    )


def local(
    residual,
    query_nope,
    query_rope,
    latent,
    key_rope,
    key_up,
    value_up,
    out_proj,
    norm_gain,
    routes,
    route_weight,
    w_gate,
    w_up,
    w_down,
):
    tp_index = lax.axis_index("tp")
    sp_index = lax.axis_index("sp")
    tok_dev = query_nope.shape[0]
    query_first = sp_index * tok_dev
    swap = [(0, 1), (1, 0)]

    key_pos = query_first + tp_index * ROWS + jnp.arange(ROWS, dtype=jnp.int32)
    key_rot = rotary(key_rope.astype(jnp.float32), key_pos).astype(jnp.bfloat16)
    packed = jnp.concatenate([key_rot[0:32], key_rot[64:96], key_rot[32:64], key_rot[96:128]], axis=1)
    shard = jnp.concatenate([latent, packed], axis=0)
    mirror = [
        (s * N_TP + t, (N_SP - 1 - s) * N_TP + t) for s in range(N_SP) for t in range(N_TP)
    ]
    crossing = [
        (s * N_TP + t, (N_SP - 1 - s) * N_TP + 1 - t) for s in range(N_SP) for t in range(N_TP)
    ]
    received_nope = lax.ppermute(query_nope, AXES, mirror)
    received_rope = lax.ppermute(query_rope, AXES, mirror)

    near = lax.ppermute(shard, AXES, plane_pairs(Z_FIRST))
    far = lax.ppermute(shard, AXES, plane_pairs(Z_SECOND))
    main = (tp_index == 0) == (sp_index < 2 * PLANE)
    both = jnp.concatenate([jnp.where(main, shard, far), near], axis=0)
    got = [both] + [lax.ppermute(both, AXES, shift_pairs(0, by)) for by in SHIFTS[1:]]
    both = jnp.concatenate(got, axis=0)

    tokens = jnp.arange(tok_dev, dtype=jnp.int32)
    query_pos = jnp.concatenate([query_first + tokens, (N_SP - 1 - sp_index) * tok_dev + tokens])
    query_rot = rotary(
        jnp.concatenate([query_rope, received_rope], axis=0)
        .astype(jnp.float32)
        .reshape(2 * tok_dev, HEADS_HERE, QK_ROPE),
        query_pos,
    ).astype(jnp.bfloat16)
    rot = jnp.swapaxes(query_rot.reshape(GROUPS, ROWS, HEADS_HERE, QK_ROPE), 1, 2)
    rot = rot.reshape(GROUPS, QROWS, QK_ROPE)
    none = jnp.zeros_like(rot)
    late = (jnp.arange(QROWS) % ROWS) // SEGMENT
    marks = (late[:, None] == jnp.arange(128)[None, :]).astype(jnp.bfloat16)
    marks = jnp.broadcast_to(marks[None], (GROUPS, QROWS, 128))
    q4 = jnp.stack(
        [jnp.concatenate([rot, none, marks], axis=-1), jnp.concatenate([none, rot, marks], axis=-1)], axis=1
    )
    qn = jnp.concatenate([query_nope, received_nope], axis=0).reshape(GROUPS, ROWS, -1)

    both, qn, q4 = lax.optimization_barrier((both, qn, q4))
    own_parts = [both]
    for by in SHIFTS[1:]:
        own_parts.append(lax.ppermute(both, AXES, shift_pairs(1, by)))
    pieces = (own_parts, [lax.ppermute(part, "tp", swap) for part in own_parts])

    state = ()
    for call in range(len(CALLS)):
        table = lax.dynamic_index_in_dim(
            jnp.asarray(work_table(call)[1]), sp_index * N_TP + tp_index, 0, keepdims=False
        )
        operands = (qn, key_up, q4) if call == 0 else (q4, qabs, *state)
        if call == len(CALLS) - 1:
            operands = (*operands, value_up)
        state = attention(call, table, operands, [pieces[own][k3] for own, k3 in CALLS[call]])
        if call == 0:
            qabs, *state = state
    attn = state[0]
    mirror_same = lax.ppermute(attn[2], AXES, mirror)
    mirror_cross = lax.ppermute(attn[3], AXES, crossing)
    swapped = lax.ppermute(attn[1], "tp", swap)
    messages = (attn[0], mirror_same, swapped, mirror_cross)

    flat = routes.reshape(-1)
    order = jnp.arange(flat.shape[0], dtype=jnp.int32)
    earlier = (flat[:, None] == flat[None, :]) & (order[None, :] < order[:, None])
    rank = jnp.sum(earlier.astype(jnp.int32), axis=1)
    slots = (flat * CAP + rank).reshape(routes.shape)

    hidden, outgoing = project(
        tp_index.reshape(1).astype(jnp.int32), messages, out_proj, residual, norm_gain[None, :], slots.T
    )
    width = residual.shape[1]
    arrived = lax.all_to_all(
        outgoing.reshape(N_SP, CAP, width), "sp", split_axis=0, concat_axis=0, tiled=True
    ).reshape(N_SP * CAP, width)
    own = (w_gate[0], w_up[0], w_down[0])
    other = tuple(lax.ppermute(w, "tp", swap) for w in own)
    produced = experts(arrived, own, other)
    back = lax.all_to_all(
        produced.reshape(N_SP, CAP, width), "sp", split_axis=0, concat_axis=0, tiled=True
    ).reshape(N_SP * CAP, width)
    return combine(back, hidden, slots, route_weight)


def solution(mesh):
    return jax.shard_map(
        local,
        mesh=mesh,
        in_specs=(
            P(("sp", "tp"), None),
            P("sp", "tp"),
            P("sp", "tp"),
            P(("sp", "tp"), None),
            P(("sp", "tp"), None),
            P(None, "tp"),
            P(None, "tp"),
            P(),
            P(),
            P(("sp", "tp"), None),
            P(("sp", "tp"), None),
            P("sp", None, "tp"),
            P("sp", None, "tp"),
            P("sp", "tp", None),
        ),
        out_specs=P(("sp", "tp"), None),
        check_vma=False,
    )
```

```python
import functools
import jax
import jax.numpy as jnp
import numpy as np
from jax import lax
from jax.experimental import pallas as pl
from jax.experimental.pallas import tpu as pltpu
from jax.sharding import PartitionSpec as P

QK_NOPE = 128
QK_ROPE = 64
V_DIM = 128
LATENT = 256
SEGMENT = 64
EPSILON = 1e-06
ROPE_BASE = 10000.0
NEG_LARGE = -1e30

N_SP = 64
N_TP = 2
HEADS_HERE = 4
ROWS = 128
SHARD = 160
UNIT = 4
KEYS = UNIT * ROWS
QROWS = HEADS_HERE * ROWS
CAP = 8
AXES = ("sp", "tp")
STEP = {"x": 1, "y": 4, "z": 16}
Z_FIRST = {(0, 0): (3, 0), (1, 0): (2, 0), (0, 1): (1, 0), (1, 1): (0, 0), (2, 1): (1, 1), (3, 1): (0, 1), (2, 0): (3, 1), (3, 0): (2, 1)}
Z_SECOND = {(0, 1): (2, 0), (1, 1): (3, 0), (2, 0): (0, 1), (3, 0): (1, 1)}
ORDER = (("y", "x"), ("x", "y"))
SHIFTS = (0, 1, -1, 2)
SCALE2 = float((QK_NOPE + QK_ROPE) ** (-0.5) * np.log2(np.e))
PLANE = 16
GROUPS = 4
CHUNK = 64
MESSAGE = HEADS_HERE * V_DIM + 128
EARLY = 1024


def moved(s, dim, by):
    step = STEP[dim]
    c = (s // step) % 4
    return s + step * ((c + by) % 4 - c)


def shift_pairs(phase, by):
    return [
        (s * N_TP + t, moved(s, ORDER[t][phase], by) * N_TP + t)
        for s in range(N_SP)
        for t in range(N_TP)
    ]


def plane_pairs(table):
    return [
        ((from_z * PLANE + r) * N_TP + from_core, (z * PLANE + r) * N_TP + core)
        for (z, core), (from_z, from_core) in table.items()
        for r in range(PLANE)
    ]


def shard_first(s, t, k3, k2, kz):
    s = moved(s, ORDER[t][1], -SHIFTS[k3])
    s = moved(s, ORDER[t][0], -SHIFTS[k2])
    z, r = divmod(s, PLANE)
    source = (z, t)
    if kz == 1:
        source = Z_FIRST[source]
    elif source in Z_SECOND:
        source = Z_SECOND[source]
    return 4 * (source[0] * PLANE + r) + 2 * source[1]


CALLS = (((0, 0), (1, 0)), ((0, 1), (0, 2), (0, 3)), ((1, 1), (1, 2), (1, 3)))
PART_SHARDS = 8


@functools.lru_cache(None)
def work_table(call):
    lists = []
    for s in range(N_SP):
        for t in range(N_TP):
            firsts = [
                shard_first(s, t if own == 0 else 1 - t, k3, k2, kz)
                for own, k3 in CALLS[call]
                for k2 in range(4)
                for kz in range(2)
            ]
            rows = []
            for group in range(GROUPS):
                block = s if group < 2 else N_SP - 1 - s
                base = 4 * block + 2 * (group % 2)
                needed = [n for n in range(len(firsts)) if firsts[n] <= base + 1]
                for at in range(0, len(needed), UNIT):
                    part = needed[at : at + UNIT]
                    segs = [firsts[n] for n in part] + [1 << 20] * (UNIT - len(part))
                    part = part + [part[-1]] * (UNIT - len(part))
                    bits = 0
                    for half in range(2):
                        for j in range(UNIT):
                            for late in range(2):
                                if segs[j] + half > base + late:
                                    bits |= 1 << ((half * UNIT + j) * 2 + late)
                    rows.append([group, bits, t] + part)
            lists.append(rows)
    count = max(len(rows) for rows in lists)
    everything = (1 << (4 * UNIT)) - 1
    idle = lambda rows, t: rows[-1][:1] + [everything] + rows[-1][2:] if rows else [0, everything, t] + [0] * UNIT
    table = []
    for n, rows in enumerate(lists):
        table.append(rows + [idle(rows, n % N_TP)] * (count + 1 - len(rows)))
    return count, np.array(table, np.int32).reshape(len(lists), -1)


NT = (((1,), (1,)), ((), ()))


def attention_body(call, steps, offset, part_count, table, *rest):
    first, last = call == 0, call == len(CALLS) - 1
    rest = list(rest)
    take = lambda n: [rest.pop(0) for _ in range(n)]
    if first:
        own_ref, own_rope_ref, received_ref, key_up_ref, cosine_ref, sine_ref = take(6)
    else:
        q4_ref, qabs, _, _, _ = take(5)
    if last:
        value_up_ref, out_proj_hbm, residual_hbm = take(3)
    parts = take(part_count)
    if last:
        out_ref, out_proj_ref, residual_ref = take(3)
    if first:
        qabs, q4_ref = take(2)
    m_ref, l_ref, acc_ref, keys, s0, s1, p0, p1, shrink0, shrink1 = take(10)
    fetches = []
    if last:
        (sems,) = rest
        early = pl.ds(0, out_proj_ref.shape[1])
        for n, (source, target) in enumerate(((out_proj_hbm.at[:, early], out_proj_ref), (residual_hbm, residual_ref))):
            fetch = pltpu.make_async_copy(source, target, sems.at[n])
            fetch.start()
            fetches.append(fetch)
    part_rows = parts[0].shape[0]
    for n in range(part_count):
        for k in range(2):
            keys[k, pl.ds(n * part_rows, part_rows), :] = parts[n][:, pl.ds(k * 128, 128)]
    if first:
        for g in range(GROUPS):
            source = own_ref if g < 2 else received_ref
            for h in range(HEADS_HERE):
                cols = pl.ds(h * QK_NOPE, QK_NOPE)
                latent_query = lax.dot_general(
                    source[pl.ds((g % 2) * ROWS, ROWS), cols],
                    key_up_ref[:, cols],
                    NT,
                    preferred_element_type=jnp.float32,
                ).astype(jnp.bfloat16)
                for k in range(2):
                    qabs[g, k, pl.ds(h * ROWS, ROWS), :] = latent_query[:, k * 128 : (k + 1) * 128]
        lane = lax.broadcasted_iota(jnp.int32, (ROWS, 128), 1)
        for g in range(GROUPS):
            tokens = pl.ds((g % 2) * ROWS, ROWS)
            for k in range(2):
                cols = pl.ds(k * 128, 128)
                if g < 2:
                    x = own_rope_ref[tokens, cols]
                else:
                    x = received_ref[tokens, pl.ds(HEADS_HERE * QK_NOPE + k * 128, 128)]
                x = x.astype(jnp.float32)
                opposite = jnp.where(lane % QK_ROPE < QK_ROPE // 2, pltpu.roll(x, 96, 1), pltpu.roll(x, 32, 1))
                at = pl.ds(g * ROWS, ROWS)
                turned = (x * cosine_ref[at, cols] + opposite * sine_ref[at, cols]).astype(jnp.bfloat16).astype(jnp.float32)
                flipped = pltpu.roll(turned, QK_ROPE, 1)
                for odd in range(2):
                    rows = pl.ds((2 * k + odd) * ROWS, ROWS)
                    for half in range(2):
                        source = turned if odd == half else flipped
                        keep = lane < QK_ROPE if half == 0 else lane >= QK_ROPE
                        q4_ref[g, half, rows, :] = jnp.where(keep, source, 0.0).astype(jnp.bfloat16)
        m_ref[...] = jnp.full(m_ref.shape, NEG_LARGE, jnp.float32)
        l_ref[...] = jnp.zeros(l_ref.shape, jnp.float32)
        acc_ref[...] = jnp.zeros(acc_ref.shape, jnp.float32)

    cols_per_step = 3 + UNIT

    def field(u, n):
        return table[offset + u * cols_per_step + n]

    def wide(at, count):
        rows = pl.ds(pl.multiple_of(at, 32), count)
        return jnp.concatenate([keys[k, rows, :] for k in range(2)], axis=1)

    def latent_tile(u, half):
        return jnp.concatenate([wide(field(u, 3 + j) * SHARD + half * SEGMENT, SEGMENT) for j in range(UNIT)], axis=0)

    note_lane = lax.broadcasted_iota(jnp.int32, (16, 128), 1)
    mark = [jnp.where(note_lane == n, 1.0, 0.0).astype(jnp.bfloat16) for n in range(2)]
    marks = jnp.concatenate(([mark[0]] * (SEGMENT // 16) + [mark[1]] * (SEGMENT // 16)) * HEADS_HERE, axis=0)

    def scores(u, s_ref):
        g = field(u, 0)
        bits = field(u, 1)
        rot = jnp.concatenate(
            [
                keys[h, pl.ds(pl.multiple_of(field(u, 3 + j) * SHARD + ROWS, 32), 32), :]
                for j in range(UNIT)
                for h in range(2)
            ],
            axis=0,
        )
        q = jnp.concatenate([qabs[g, k] for k in range(2)], axis=1)
        for half in range(2):
            notes = []
            for j in range(UNIT):
                at = (half * UNIT + j) * 2
                early, late = (
                    jnp.where((bits >> (at + n)) & 1 == 1, jnp.float32(NEG_LARGE), jnp.float32(0.0)) for n in range(2)
                )
                note = jnp.where(note_lane == 0, early, jnp.where(note_lane == 1, late, 0.0)).astype(jnp.bfloat16)
                notes += [note] * (SEGMENT // 16)
            extra = jnp.concatenate([rot, jnp.concatenate(notes, axis=0)], axis=1)
            total = lax.dot_general(
                q, latent_tile(u, half), NT, preferred_element_type=jnp.float32
            ) + lax.dot_general(
                jnp.concatenate([q4_ref[g, half], marks], axis=1), extra, NT, preferred_element_type=jnp.float32
            )
            for k in range(2):
                s_ref[half * 2 + k, pl.ds(0, QROWS), :] = total[:, k * 128 : (k + 1) * 128]

    def absorb(u, s_ref, p_ref, shrink_ref):
        g = field(u, 0)
        for at in range(0, QROWS, CHUNK):
            rows = pl.ds(at, CHUNK)
            s = [s_ref[k, rows, :] for k in range(KEYS // 128)]
            before = m_ref[g, rows, :]
            top = jnp.maximum(jnp.maximum(s[0], s[1]), jnp.maximum(s[2], s[3]))
            after = jnp.maximum(before, jnp.max(top, axis=1, keepdims=True))
            m_ref[g, rows, :] = after
            shrink = jnp.exp2((before - after) * SCALE2)
            shrink_ref[rows, :] = shrink
            after = after * SCALE2
            partial = l_ref[g, rows, :] * shrink
            for k in range(KEYS // 128):
                p = jnp.exp2(s[k] * SCALE2 - after)
                partial = partial + p
                p_ref[k, rows, :] = p.astype(jnp.bfloat16)
            l_ref[g, rows, :] = partial
        values = jnp.concatenate([latent_tile(u, 0), latent_tile(u, 1)], axis=0)
        for at in range(0, QROWS, QROWS // 2):
            rows = pl.ds(at, QROWS // 2)
            weights = jnp.concatenate([p_ref[k, rows, :] for k in range(KEYS // 128)], axis=1)
            product = jnp.dot(weights, values, preferred_element_type=jnp.float32)
            for k in range(LATENT // 128):
                acc_ref[g, k, rows, :] = (
                    acc_ref[g, k, rows, :] * shrink_ref[rows, :] + product[:, k * 128 : (k + 1) * 128]
                )

    scores(0, s0)

    def pair(k, carry):
        u = k * 2
        scores(u + 1, s1)
        absorb(u, s0, p0, shrink0)
        scores(u + 2, s0)
        absorb(u + 1, s1, p1, shrink1)
        return carry

    lax.fori_loop(0, (steps - 1) // 2, pair, 0)
    if steps % 2 == 0:
        scores(steps - 1, s1)
        absorb(steps - 2, s0, p0, shrink0)
        absorb(steps - 1, s1, p1, shrink1)
    else:
        absorb(steps - 1, s0, p0, shrink0)
    if not last:
        return
    core = field(0, 2)
    lane = lax.broadcasted_iota(jnp.int32, (ROWS, 128), 1)
    for g in range(GROUPS):
        place = 2 * (g // 2) + jnp.where(core == g % 2, 0, 1)
        total = jnp.sum(l_ref[g], axis=1, keepdims=True)
        total = jnp.where(total > 0.0, total, 1.0)
        mean = jnp.concatenate([acc_ref[g, k] / total for k in range(2)], axis=1).astype(jnp.bfloat16)
        size = m_ref[g] * SCALE2 + jnp.log2(total)
        notes = jnp.zeros((ROWS, 128), jnp.bfloat16)
        for h in range(HEADS_HERE):
            cols = pl.ds(h * V_DIM, V_DIM)
            rows = slice(h * ROWS, (h + 1) * ROWS)
            out_ref[place, :, cols] = jnp.dot(
                mean[rows], value_up_ref[:, cols], preferred_element_type=jnp.float32
            ).astype(jnp.bfloat16)
            left = size[rows]
            for n in range(3):
                term = left.astype(jnp.bfloat16)
                notes = jnp.where(lane == n * HEADS_HERE + h, term, notes)
                left = left - term.astype(jnp.float32)
        out_ref[place, :, pl.ds(HEADS_HERE * V_DIM, 128)] = notes
    for fetch in fetches:
        fetch.wait()


def attention(call, table, operands, parts):
    vmem = pl.BlockSpec(memory_space=pltpu.VMEM)
    hbm = pl.BlockSpec(memory_space=pltpu.HBM)
    steps = work_table(call)[0]
    offset = sum(work_table(n)[1].shape[1] for n in range(call))
    first, last = call == 0, call == len(CALLS) - 1
    outs = [
        pltpu.VMEM((GROUPS, QROWS, 128), jnp.float32),
        pltpu.VMEM((GROUPS, QROWS, 128), jnp.float32),
        pltpu.VMEM((GROUPS, 2, QROWS, 128), jnp.float32),
    ]
    specs = [vmem] * len(operands)
    scratch = []
    aliases = {}
    if first:
        outs = [pltpu.VMEM((GROUPS, 2, QROWS, 128), jnp.bfloat16)] * 2 + outs
    elif last:
        fetched = operands[-2:]
        outs = [
            pltpu.VMEM((4, ROWS, MESSAGE), jnp.bfloat16),
            pltpu.VMEM((fetched[0].shape[0], EARLY), jnp.bfloat16),
            pltpu.VMEM(fetched[1].shape, jnp.bfloat16),
        ] + outs
        specs = specs[:-2] + [hbm] * 2
        operands = (*operands[:-2], *[in_hbm(f) for f in fetched])
        scratch = [pltpu.SemaphoreType.DMA((2,))]
    if not first:
        aliases = {3 + n: len(outs) - 3 + n for n in range(3)}
        operands = tuple(in_vmem(x) if 1 <= n < 5 else x for n, x in enumerate(operands))
    work = steps * QROWS * KEYS * 3 * LATENT * 2
    return pl.pallas_call(
        functools.partial(attention_body, call, steps, offset, len(parts)),
        out_shape=outs,
        in_specs=[pl.BlockSpec(memory_space=pltpu.SMEM)] + specs + [vmem] * len(parts),
        out_specs=[vmem] * len(outs),
        input_output_aliases=aliases,
        scratch_shapes=[
            pltpu.VMEM((2, len(parts) * PART_SHARDS * SHARD, 128), jnp.bfloat16),
            pltpu.VMEM((KEYS // 128, QROWS, 128), jnp.float32),
            pltpu.VMEM((KEYS // 128, QROWS, 128), jnp.float32),
            pltpu.VMEM((KEYS // 128, QROWS, 128), jnp.bfloat16),
            pltpu.VMEM((KEYS // 128, QROWS, 128), jnp.bfloat16),
            pltpu.VMEM((QROWS, 128), jnp.float32),
            pltpu.VMEM((QROWS, 128), jnp.float32),
        ]
        + scratch,
        cost_estimate=pl.CostEstimate(
            flops=work, bytes_accessed=2**20, transcendentals=steps * QROWS * KEYS
        ),
        compiler_params=pltpu.CompilerParams(vmem_limit_bytes=24 * 2**20),
    )(table, *operands, *[in_vmem(part) for part in parts])


def in_vmem(x):
    return pltpu.with_memory_space_constraint(x, pltpu.VMEM)


def in_hbm(x):
    return pltpu.with_memory_space_constraint(x, pltpu.HBM)


def merged(one, two):
    width = HEADS_HERE * V_DIM
    outs = []
    for h in range(HEADS_HERE):
        sizes = []
        for part in (one, two):
            notes = part[:, width : width + 128].astype(jnp.float32)
            sizes.append(
                notes[:, h : h + 1] + notes[:, HEADS_HERE + h : HEADS_HERE + h + 1]
                + notes[:, 2 * HEADS_HERE + h : 2 * HEADS_HERE + h + 1]
            )
        most = jnp.maximum(sizes[0], sizes[1])
        first, second = (jnp.exp2(size - most) for size in sizes)
        cols = slice(h * V_DIM, (h + 1) * V_DIM)
        value = first * one[:, cols].astype(jnp.float32) + second * two[:, cols].astype(jnp.float32)
        outs.append((value / (first + second)).astype(jnp.bfloat16))
    return jnp.concatenate(outs, axis=1)


PIECES = 4


def project_body(
    core, local_part, mirror_same, swapped, mirror_cross, gain, slots, residual, out_early, out_proj_hbm,
    hidden_hbm, outgoing_hbm, hidden, outgoing, out_late, out_sems, late_sem,
):
    fetch = pltpu.make_async_copy(out_proj_hbm.at[:, pl.ds(EARLY, out_late.shape[1])], out_late, late_sem)
    fetch.start()
    half = HEADS_HERE * V_DIM
    mine = merged(local_part[...], mirror_same[...])
    theirs = merged(swapped[...], mirror_cross[...])
    at = pl.multiple_of(core[0] * half, half)
    other = pl.multiple_of((1 - core[0]) * half, half)
    projected = []
    for weights in (out_early, out_late):
        if weights is out_late:
            fetch.wait()
        projected.append(
            jnp.dot(mine, weights[pl.ds(at, half), :], preferred_element_type=jnp.float32)
            + jnp.dot(theirs, weights[pl.ds(other, half), :], preferred_element_type=jnp.float32)
        )
    projected = jnp.concatenate(projected, axis=1)
    result = (residual[...].astype(jnp.float32) + projected).astype(jnp.bfloat16)
    hidden[...] = result
    store = pltpu.make_async_copy(hidden, hidden_hbm, out_sems.at[PIECES])
    store.start()
    wide = result.astype(jnp.float32)
    normed = wide * lax.rsqrt(jnp.mean(wide * wide, axis=-1, keepdims=True) + EPSILON)
    normed = (normed * gain[...]).astype(jnp.bfloat16)
    count = outgoing.shape[0] // PIECES
    stores = [store]
    for n in range(PIECES):
        slot = lax.broadcasted_iota(jnp.int32, (count, normed.shape[0]), 0) + n * count
        pick = (slot == slots[0:1, :]) | (slot == slots[1:2, :])
        pick = jnp.where(pick, 1.0, 0.0).astype(jnp.bfloat16)
        rows = pl.ds(n * count, count)
        outgoing[rows, :] = jnp.dot(pick, normed, preferred_element_type=jnp.float32).astype(jnp.bfloat16)
        store = pltpu.make_async_copy(outgoing.at[rows], outgoing_hbm.at[rows], out_sems.at[n])
        store.start()
        stores.append(store)
    for store in stores:
        store.wait()


def project(core, messages, out_early, out_proj, residual, gain, slots):
    width = residual.shape[1]
    vmem = pl.BlockSpec(memory_space=pltpu.VMEM)
    hbm = pl.BlockSpec(memory_space=pltpu.HBM)
    return pl.pallas_call(
        project_body,
        out_shape=(
            pltpu.HBM((ROWS, width), jnp.bfloat16),
            pltpu.HBM((N_SP * CAP, width), jnp.bfloat16),
        ),
        in_specs=[pl.BlockSpec(memory_space=pltpu.SMEM)] + [vmem] * 8 + [hbm],
        out_specs=(hbm, hbm),
        scratch_shapes=[
            pltpu.VMEM((ROWS, width), jnp.bfloat16),
            pltpu.VMEM((N_SP * CAP, width), jnp.bfloat16),
            pltpu.VMEM((out_proj.shape[0], width - EARLY), jnp.bfloat16),
            pltpu.SemaphoreType.DMA((PIECES + 1,)),
            pltpu.SemaphoreType.DMA,
        ],
        compiler_params=pltpu.CompilerParams(vmem_limit_bytes=16 * 2**20),
        name="project",
    )(core, *messages, gain, slots, in_vmem(residual), in_vmem(out_early), in_hbm(out_proj))


def experts_body(rows, *rest):
    sources = rest[:6]
    out_hbm = rest[6]
    weights = rest[7:13]
    first, out, sems, out_sems = rest[13:]
    loads = []
    for n in range(6):
        load = pltpu.make_async_copy(sources[n], weights[n], sems.at[n])
        load.start()
        loads.append(load)
    count = rows.shape[0]
    block = count // 2
    stores = []
    for n in range(2):
        gate, up, down = weights[3 * n : 3 * n + 3]
        loads[3 * n].wait()
        loads[3 * n + 1].wait()
        actives = []
        for k in range(2):
            x = rows[pl.ds(k * block, block), :]
            gated = jnp.dot(x, gate[...], preferred_element_type=jnp.float32)
            raised = jnp.dot(x, up[...], preferred_element_type=jnp.float32)
            actives.append((gated / (1.0 + jnp.exp(-gated)) * raised).astype(jnp.bfloat16))
        loads[3 * n + 2].wait()
        for k in range(2):
            at = pl.ds(k * block, block)
            product = jnp.dot(actives[k], down[...], preferred_element_type=jnp.float32).astype(jnp.bfloat16)
            if n == 0:
                first[at, :] = product
            else:
                out[at, :] = (first[at, :].astype(jnp.float32) + product.astype(jnp.float32)).astype(jnp.bfloat16)
                store = pltpu.make_async_copy(out.at[at], out_hbm.at[at], out_sems.at[k])
                store.start()
                stores.append(store)
    for store in stores:
        store.wait()


def experts(rows, own, other):
    count, width = rows.shape
    hbm = pl.BlockSpec(memory_space=pltpu.HBM)
    return pl.pallas_call(
        experts_body,
        out_shape=pltpu.HBM((count, width), jnp.bfloat16),
        in_specs=[pl.BlockSpec(memory_space=pltpu.VMEM)] + [hbm] * 6,
        out_specs=hbm,
        scratch_shapes=[pltpu.VMEM(w.shape, w.dtype) for w in (*own, *other)]
        + [
            pltpu.VMEM((count, width), jnp.bfloat16),
            pltpu.VMEM((count, width), jnp.bfloat16),
            pltpu.SemaphoreType.DMA((6,)),
            pltpu.SemaphoreType.DMA((2,)),
        ],
        compiler_params=pltpu.CompilerParams(vmem_limit_bytes=28 * 2**20),
        name="experts",
    )(rows, *[in_hbm(w) for w in (*own, *other)])


def combine_body(back, hidden, slots, weights, out_ref):
    slot = lax.broadcasted_iota(jnp.int32, (hidden.shape[0], back.shape[0]), 1)
    pick = jnp.where(slot == slots[:, 0:1], weights[:, 0:1], 0.0) + jnp.where(
        slot == slots[:, 1:2], weights[:, 1:2], 0.0
    )
    high = pick.astype(jnp.bfloat16)
    low = (pick - high.astype(jnp.float32)).astype(jnp.bfloat16)
    rows = back[...]
    mixed = jnp.dot(high, rows, preferred_element_type=jnp.float32) + jnp.dot(
        low, rows, preferred_element_type=jnp.float32
    )
    out_ref[...] = (hidden[...].astype(jnp.float32) + mixed).astype(jnp.bfloat16)


def combine(back, hidden, slots, weights):
    vmem = pl.BlockSpec(memory_space=pltpu.VMEM)
    return pl.pallas_call(
        combine_body,
        out_shape=jax.ShapeDtypeStruct(hidden.shape, jnp.bfloat16),
        in_specs=[vmem] * 4,
        out_specs=vmem,
        compiler_params=pltpu.CompilerParams(vmem_limit_bytes=16 * 2**20),
        name="combine",
    )(back, hidden, slots, weights)


def rotary(values, positions):
    half_width = values.shape[-1] // 2
    inverse = ROPE_BASE ** (-2.0 * jnp.arange(half_width, dtype=jnp.float32) / values.shape[-1])
    angles = positions.astype(jnp.float32)[:, None] * inverse[None, :]
    cosine = jnp.cos(angles)
    sine_part = jnp.sin(angles)
    if values.ndim == 3:
        cosine = cosine[:, None, :]
        sine_part = sine_part[:, None, :]
    first_half = values[..., :half_width]
    second = values[..., half_width:]
    return jnp.concatenate(
        [first_half * cosine - second * sine_part, second * cosine + first_half * sine_part],
        axis=-1,
    )


def local(
    residual,
    query_nope,
    query_rope,
    latent,
    key_rope,
    key_up,
    value_up,
    out_proj,
    norm_gain,
    routes,
    route_weight,
    w_gate,
    w_up,
    w_down,
):
    tp_index = lax.axis_index("tp")
    sp_index = lax.axis_index("sp")
    tok_dev = query_nope.shape[0]
    query_first = sp_index * tok_dev
    swap = [(0, 1), (1, 0)]

    key_pos = query_first + tp_index * ROWS + jnp.arange(ROWS, dtype=jnp.int32)
    key_rot = rotary(key_rope.astype(jnp.float32), key_pos).astype(jnp.bfloat16)
    packed = jnp.concatenate([key_rot[0:32], key_rot[64:96], key_rot[32:64], key_rot[96:128]], axis=1)
    shard = jnp.concatenate([latent, packed], axis=0)
    mirror = [
        (s * N_TP + t, (N_SP - 1 - s) * N_TP + t) for s in range(N_SP) for t in range(N_TP)
    ]
    crossing = [
        (s * N_TP + t, (N_SP - 1 - s) * N_TP + 1 - t) for s in range(N_SP) for t in range(N_TP)
    ]
    queries = jnp.concatenate([query_nope, query_rope], axis=1)
    received = lax.ppermute(queries, AXES, mirror)

    near = lax.ppermute(shard, AXES, plane_pairs(Z_FIRST))
    far = lax.ppermute(shard, AXES, plane_pairs(Z_SECOND))
    main = (tp_index == 0) == (sp_index < 2 * PLANE)
    both = jnp.concatenate([jnp.where(main, shard, far), near], axis=0)

    flat = routes.reshape(-1)
    order = jnp.arange(flat.shape[0], dtype=jnp.int32)
    earlier = (flat[:, None] == flat[None, :]) & (order[None, :] < order[:, None])
    rank = jnp.sum(earlier.astype(jnp.int32), axis=1)
    slots = (flat * CAP + rank).reshape(routes.shape)
    slots_across = slots.T
    tables = np.concatenate([work_table(call)[1] for call in range(len(CALLS))], axis=1)
    table = lax.dynamic_index_in_dim(jnp.asarray(tables), sp_index * N_TP + tp_index, 0, keepdims=False)
    tokens = jnp.arange(tok_dev, dtype=jnp.int32)
    query_pos = jnp.concatenate([query_first + tokens, (N_SP - 1 - sp_index) * tok_dev + tokens])
    half_width = QK_ROPE // 2
    pair = jnp.arange(HEADS_HERE * QK_ROPE, dtype=jnp.int32) % half_width
    inverse = ROPE_BASE ** (-2.0 * pair.astype(jnp.float32) / QK_ROPE)
    angles = query_pos.astype(jnp.float32)[:, None] * inverse[None, :]
    behind = jnp.arange(HEADS_HERE * QK_ROPE, dtype=jnp.int32) % QK_ROPE >= half_width
    cosine = jnp.cos(angles)
    sine = jnp.where(behind[None, :], jnp.sin(angles), -jnp.sin(angles))
    both, table, slots, slots_across, cosine, sine = lax.optimization_barrier(
        (both, table, slots, slots_across, cosine, sine)
    )
    got = [both]
    for by in SHIFTS[1:]:
        got.append(lax.ppermute(both, AXES, shift_pairs(0, by)))
    both = jnp.concatenate(got, axis=0)

    own_parts = [both]
    for by in SHIFTS[1:]:
        own_parts.append(lax.ppermute(both, AXES, shift_pairs(1, by)))
    pieces = (own_parts, [lax.ppermute(part, "tp", swap) for part in own_parts])
    own_weights = (w_gate[0], w_up[0], w_down[0])
    other_weights = []
    for w in own_weights:
        other_weights.append(lax.ppermute(w, "tp", swap))

    state = ()
    for call in range(len(CALLS)):
        operands = (
            (query_nope, query_rope, received, key_up, cosine, sine) if call == 0 else (q4, qabs, *state)
        )
        if call == len(CALLS) - 1:
            operands = (*operands, value_up, out_proj, residual)
        state = attention(call, table, operands, [pieces[own][k3] for own, k3 in CALLS[call]])
        if call == 0:
            qabs, q4, *state = state
    attn, out_early, residual = state[:3]
    mirror_same = lax.ppermute(attn[2], AXES, mirror)
    mirror_cross = lax.ppermute(attn[3], AXES, crossing)
    swapped = lax.ppermute(attn[1], "tp", swap)
    messages = (attn[0], mirror_same, swapped, mirror_cross)

    hidden, outgoing = project(
        tp_index.reshape(1).astype(jnp.int32), messages, out_early, out_proj, residual, norm_gain[None, :], slots_across
    )
    width = residual.shape[1]
    arrived = lax.all_to_all(
        outgoing.reshape(N_SP, CAP, width), "sp", split_axis=0, concat_axis=0, tiled=True
    ).reshape(N_SP * CAP, width)
    produced = experts(arrived, own_weights, other_weights)
    back = lax.all_to_all(
        produced.reshape(N_SP, CAP, width), "sp", split_axis=0, concat_axis=0, tiled=True
    ).reshape(N_SP * CAP, width)
    return combine(back, hidden, slots, route_weight)


def solution(mesh):
    return jax.shard_map(
        local,
        mesh=mesh,
        in_specs=(
            P(("sp", "tp"), None),
            P("sp", "tp"),
            P("sp", "tp"),
            P(("sp", "tp"), None),
            P(("sp", "tp"), None),
            P(None, "tp"),
            P(None, "tp"),
            P(),
            P(),
            P(("sp", "tp"), None),
            P(("sp", "tp"), None),
            P("sp", None, "tp"),
            P("sp", None, "tp"),
            P("sp", "tp", None),
        ),
        out_specs=P(("sp", "tp"), None),
        check_vma=False,
    )
```

```python
import functools
import jax
import jax.numpy as jnp
import numpy as np
from jax import lax
from jax.experimental import pallas as pl
from jax.experimental.pallas import tpu as pltpu
from jax.sharding import PartitionSpec as P

QK_NOPE = 128
QK_ROPE = 64
V_DIM = 128
LATENT = 256
SEGMENT = 64
EPSILON = 1e-06
ROPE_BASE = 10000.0
NEG_LARGE = -1e30

N_SP = 64
N_TP = 2
HEADS_HERE = 4
ROWS = 128
SHARD = 160
UNIT = 4
KEYS = UNIT * ROWS
QROWS = HEADS_HERE * ROWS
CAP = 8
AXES = ("sp", "tp")
STEP = {"x": 1, "y": 4, "z": 16}
Z_FIRST = {(0, 0): (3, 0), (1, 0): (2, 0), (0, 1): (1, 0), (1, 1): (0, 0), (2, 1): (1, 1), (3, 1): (0, 1), (2, 0): (3, 1), (3, 0): (2, 1)}
Z_SECOND = {(0, 1): (2, 0), (1, 1): (3, 0), (2, 0): (0, 1), (3, 0): (1, 1)}
ORDER = (("y", "x"), ("x", "y"))
SHIFTS = (0, 1, -1, 2)
SCALE2 = float((QK_NOPE + QK_ROPE) ** (-0.5) * np.log2(np.e))
PLANE = 16
GROUPS = 4
CHUNK = 64
MESSAGE = HEADS_HERE * V_DIM + 128
EARLY = 1024


def moved(s, dim, by):
    step = STEP[dim]
    c = (s // step) % 4
    return s + step * ((c + by) % 4 - c)


def shift_pairs(phase, by):
    return [
        (s * N_TP + t, moved(s, ORDER[t][phase], by) * N_TP + t)
        for s in range(N_SP)
        for t in range(N_TP)
    ]


def plane_pairs(table):
    return [
        ((from_z * PLANE + r) * N_TP + from_core, (z * PLANE + r) * N_TP + core)
        for (z, core), (from_z, from_core) in table.items()
        for r in range(PLANE)
    ]


def shard_first(s, t, k3, k2, kz):
    s = moved(s, ORDER[t][1], -SHIFTS[k3])
    s = moved(s, ORDER[t][0], -SHIFTS[k2])
    z, r = divmod(s, PLANE)
    source = (z, t)
    if kz == 1:
        source = Z_FIRST[source]
    elif source in Z_SECOND:
        source = Z_SECOND[source]
    return 4 * (source[0] * PLANE + r) + 2 * source[1]


CALLS = (((0, 0), (1, 0)), ((0, 1), (0, 2)), ((1, 1), (1, 2)), ((0, 3), (1, 3)))


@functools.lru_cache(None)
def work_table(call):
    lists = []
    for s in range(N_SP):
        for t in range(N_TP):
            firsts = [
                shard_first(s, t if own == 0 else 1 - t, k3, k2, kz)
                for own, k3 in CALLS[call]
                for k2 in range(4)
                for kz in range(2)
            ]
            rows = []
            for group in range(GROUPS):
                block = s if group < 2 else N_SP - 1 - s
                base = 4 * block + 2 * (group % 2)
                needed = [n for n in range(len(firsts)) if firsts[n] <= base + 1]
                for at in range(0, len(needed), UNIT):
                    part = needed[at : at + UNIT]
                    segs = [firsts[n] for n in part] + [1 << 20] * (UNIT - len(part))
                    part = part + [part[-1]] * (UNIT - len(part))
                    bits = 0
                    for half in range(2):
                        for j in range(UNIT):
                            for late in range(2):
                                if segs[j] + half > base + late:
                                    bits |= 1 << ((half * UNIT + j) * 2 + late)
                    rows.append([group, bits, t] + part)
            lists.append(rows)
    count = max(len(rows) for rows in lists)
    everything = (1 << (4 * UNIT)) - 1
    idle = lambda rows, t: rows[-1][:1] + [everything] + rows[-1][2:] if rows else [0, everything, t] + [0] * UNIT
    table = []
    for n, rows in enumerate(lists):
        table.append(rows + [idle(rows, n % N_TP)] * (count + 1 - len(rows)))
    return count, np.array(table, np.int32).reshape(len(lists), -1)


NT = (((1,), (1,)), ((), ()))


def attention_body(call, steps, offset, part_count, table, *rest):
    first, last = call == 0, call == len(CALLS) - 1
    rest = list(rest)
    take = lambda n: [rest.pop(0) for _ in range(n)]
    if first:
        own_ref, own_rope_ref, received_ref, key_up_ref, cosine_ref, sine_ref = take(6)
    else:
        q4_ref, qabs, _, _, _ = take(5)
    if last:
        value_up_ref, out_proj_hbm, residual_hbm = take(3)
    parts = take(part_count)
    if last:
        out_ref, out_proj_ref, residual_ref = take(3)
    if first:
        qabs, q4_ref = take(2)
    m_ref, l_ref, acc_ref, keys, s0, s1, p0, p1, shrink0, shrink1 = take(10)
    fetches = []
    if last:
        (sems,) = rest
        early = pl.ds(0, out_proj_ref.shape[1])
        for n, (source, target) in enumerate(((out_proj_hbm.at[:, early], out_proj_ref), (residual_hbm, residual_ref))):
            fetch = pltpu.make_async_copy(source, target, sems.at[n])
            fetch.start()
            fetches.append(fetch)
    at = 0
    for part in parts:
        for k in range(2):
            keys[k, pl.ds(at, part.shape[0]), :] = part[:, pl.ds(k * 128, 128)]
        at += part.shape[0]
    if first:
        for g in range(GROUPS):
            source = own_ref if g < 2 else received_ref
            for h in range(HEADS_HERE):
                cols = pl.ds(h * QK_NOPE, QK_NOPE)
                latent_query = lax.dot_general(
                    source[pl.ds((g % 2) * ROWS, ROWS), cols],
                    key_up_ref[:, cols],
                    NT,
                    preferred_element_type=jnp.float32,
                ).astype(jnp.bfloat16)
                for k in range(2):
                    qabs[g, k, pl.ds(h * ROWS, ROWS), :] = latent_query[:, k * 128 : (k + 1) * 128]
        lane = lax.broadcasted_iota(jnp.int32, (ROWS, 128), 1)
        for g in range(GROUPS):
            tokens = pl.ds((g % 2) * ROWS, ROWS)
            for k in range(2):
                cols = pl.ds(k * 128, 128)
                if g < 2:
                    x = own_rope_ref[tokens, cols]
                else:
                    x = received_ref[tokens, pl.ds(HEADS_HERE * QK_NOPE + k * 128, 128)]
                x = x.astype(jnp.float32)
                opposite = jnp.where(lane % QK_ROPE < QK_ROPE // 2, pltpu.roll(x, 96, 1), pltpu.roll(x, 32, 1))
                at = pl.ds(g * ROWS, ROWS)
                turned = (x * cosine_ref[at, cols] + opposite * sine_ref[at, cols]).astype(jnp.bfloat16).astype(jnp.float32)
                flipped = pltpu.roll(turned, QK_ROPE, 1)
                for odd in range(2):
                    rows = pl.ds((2 * k + odd) * ROWS, ROWS)
                    for half in range(2):
                        source = turned if odd == half else flipped
                        keep = lane < QK_ROPE if half == 0 else lane >= QK_ROPE
                        q4_ref[g, half, rows, :] = jnp.where(keep, source, 0.0).astype(jnp.bfloat16)
        m_ref[...] = jnp.full(m_ref.shape, NEG_LARGE, jnp.float32)
        l_ref[...] = jnp.zeros(l_ref.shape, jnp.float32)
        acc_ref[...] = jnp.zeros(acc_ref.shape, jnp.float32)

    cols_per_step = 3 + UNIT

    def field(u, n):
        return table[offset + u * cols_per_step + n]

    def wide(at, count):
        rows = pl.ds(pl.multiple_of(at, 32), count)
        return jnp.concatenate([keys[k, rows, :] for k in range(2)], axis=1)

    def latent_tile(u, half):
        return jnp.concatenate([wide(field(u, 3 + j) * SHARD + half * SEGMENT, SEGMENT) for j in range(UNIT)], axis=0)

    note_lane = lax.broadcasted_iota(jnp.int32, (16, 128), 1)
    mark = [jnp.where(note_lane == n, 1.0, 0.0).astype(jnp.bfloat16) for n in range(2)]
    marks = jnp.concatenate(([mark[0]] * (SEGMENT // 16) + [mark[1]] * (SEGMENT // 16)) * HEADS_HERE, axis=0)

    def scores(u, s_ref):
        g = field(u, 0)
        bits = field(u, 1)
        rot = jnp.concatenate(
            [
                keys[h, pl.ds(pl.multiple_of(field(u, 3 + j) * SHARD + ROWS, 32), 32), :]
                for j in range(UNIT)
                for h in range(2)
            ],
            axis=0,
        )
        q = jnp.concatenate([qabs[g, k] for k in range(2)], axis=1)
        for half in range(2):
            notes = []
            for j in range(UNIT):
                at = (half * UNIT + j) * 2
                early, late = (
                    jnp.where((bits >> (at + n)) & 1 == 1, jnp.float32(NEG_LARGE), jnp.float32(0.0)) for n in range(2)
                )
                note = jnp.where(note_lane == 0, early, jnp.where(note_lane == 1, late, 0.0)).astype(jnp.bfloat16)
                notes += [note] * (SEGMENT // 16)
            extra = jnp.concatenate([rot, jnp.concatenate(notes, axis=0)], axis=1)
            total = lax.dot_general(
                q, latent_tile(u, half), NT, preferred_element_type=jnp.float32
            ) + lax.dot_general(
                jnp.concatenate([q4_ref[g, half], marks], axis=1), extra, NT, preferred_element_type=jnp.float32
            )
            for k in range(2):
                s_ref[half * 2 + k, pl.ds(0, QROWS), :] = total[:, k * 128 : (k + 1) * 128]

    def absorb(u, s_ref, p_ref, shrink_ref):
        g = field(u, 0)
        for at in range(0, QROWS, CHUNK):
            rows = pl.ds(at, CHUNK)
            s = [s_ref[k, rows, :] for k in range(KEYS // 128)]
            before = m_ref[g, rows, :]
            top = jnp.maximum(jnp.maximum(s[0], s[1]), jnp.maximum(s[2], s[3]))
            after = jnp.maximum(before, jnp.max(top, axis=1, keepdims=True))
            m_ref[g, rows, :] = after
            shrink = jnp.exp2((before - after) * SCALE2)
            shrink_ref[rows, :] = shrink
            after = after * SCALE2
            partial = l_ref[g, rows, :] * shrink
            for k in range(KEYS // 128):
                p = jnp.exp2(s[k] * SCALE2 - after)
                partial = partial + p
                p_ref[k, rows, :] = p.astype(jnp.bfloat16)
            l_ref[g, rows, :] = partial
        values = jnp.concatenate([latent_tile(u, 0), latent_tile(u, 1)], axis=0)
        for at in range(0, QROWS, QROWS // 2):
            rows = pl.ds(at, QROWS // 2)
            weights = jnp.concatenate([p_ref[k, rows, :] for k in range(KEYS // 128)], axis=1)
            product = jnp.dot(weights, values, preferred_element_type=jnp.float32)
            for k in range(LATENT // 128):
                acc_ref[g, k, rows, :] = (
                    acc_ref[g, k, rows, :] * shrink_ref[rows, :] + product[:, k * 128 : (k + 1) * 128]
                )

    scores(0, s0)

    def pair(k, carry):
        u = k * 2
        scores(u + 1, s1)
        absorb(u, s0, p0, shrink0)
        scores(u + 2, s0)
        absorb(u + 1, s1, p1, shrink1)
        return carry

    lax.fori_loop(0, (steps - 1) // 2, pair, 0)
    if steps % 2 == 0:
        scores(steps - 1, s1)
        absorb(steps - 2, s0, p0, shrink0)
        absorb(steps - 1, s1, p1, shrink1)
    else:
        absorb(steps - 1, s0, p0, shrink0)
    if not last:
        return
    core = field(0, 2)
    lane = lax.broadcasted_iota(jnp.int32, (ROWS, 128), 1)
    for g in range(GROUPS):
        place = 2 * (g // 2) + jnp.where(core == g % 2, 0, 1)
        total = jnp.sum(l_ref[g], axis=1, keepdims=True)
        total = jnp.where(total > 0.0, total, 1.0)
        mean = jnp.concatenate([acc_ref[g, k] / total for k in range(2)], axis=1).astype(jnp.bfloat16)
        size = m_ref[g] * SCALE2 + jnp.log2(total)
        notes = jnp.zeros((ROWS, 128), jnp.bfloat16)
        for h in range(HEADS_HERE):
            cols = pl.ds(h * V_DIM, V_DIM)
            rows = slice(h * ROWS, (h + 1) * ROWS)
            out_ref[place, :, cols] = jnp.dot(
                mean[rows], value_up_ref[:, cols], preferred_element_type=jnp.float32
            ).astype(jnp.bfloat16)
            left = size[rows]
            for n in range(3):
                term = left.astype(jnp.bfloat16)
                notes = jnp.where(lane == n * HEADS_HERE + h, term, notes)
                left = left - term.astype(jnp.float32)
        out_ref[place, :, pl.ds(HEADS_HERE * V_DIM, 128)] = notes
    for fetch in fetches:
        fetch.wait()


def attention(call, table, operands, parts):
    vmem = pl.BlockSpec(memory_space=pltpu.VMEM)
    hbm = pl.BlockSpec(memory_space=pltpu.HBM)
    steps = work_table(call)[0]
    offset = sum(work_table(n)[1].shape[1] for n in range(call))
    first, last = call == 0, call == len(CALLS) - 1
    outs = [
        pltpu.VMEM((GROUPS, QROWS, 128), jnp.float32),
        pltpu.VMEM((GROUPS, QROWS, 128), jnp.float32),
        pltpu.VMEM((GROUPS, 2, QROWS, 128), jnp.float32),
    ]
    specs = [vmem] * len(operands)
    scratch = []
    aliases = {}
    if first:
        outs = [pltpu.VMEM((GROUPS, 2, QROWS, 128), jnp.bfloat16)] * 2 + outs
    elif last:
        fetched = operands[-2:]
        outs = [
            pltpu.VMEM((4, ROWS, MESSAGE), jnp.bfloat16),
            pltpu.VMEM((fetched[0].shape[0], EARLY), jnp.bfloat16),
            pltpu.VMEM(fetched[1].shape, jnp.bfloat16),
        ] + outs
        specs = specs[:-2] + [hbm] * 2
        operands = (*operands[:-2], *[in_hbm(f) for f in fetched])
        scratch = [pltpu.SemaphoreType.DMA((2,))]
    if not first:
        aliases = {3 + n: len(outs) - 3 + n for n in range(3)}
        operands = tuple(in_vmem(x) if 1 <= n < 5 else x for n, x in enumerate(operands))
    work = steps * QROWS * KEYS * 3 * LATENT * 2
    return pl.pallas_call(
        functools.partial(attention_body, call, steps, offset, len(parts)),
        out_shape=outs,
        in_specs=[pl.BlockSpec(memory_space=pltpu.SMEM)] + specs + [vmem] * len(parts),
        out_specs=[vmem] * len(outs),
        input_output_aliases=aliases,
        scratch_shapes=[
            pltpu.VMEM((2, sum(part.shape[0] for part in parts), 128), jnp.bfloat16),
            pltpu.VMEM((KEYS // 128, QROWS, 128), jnp.float32),
            pltpu.VMEM((KEYS // 128, QROWS, 128), jnp.float32),
            pltpu.VMEM((KEYS // 128, QROWS, 128), jnp.bfloat16),
            pltpu.VMEM((KEYS // 128, QROWS, 128), jnp.bfloat16),
            pltpu.VMEM((QROWS, 128), jnp.float32),
            pltpu.VMEM((QROWS, 128), jnp.float32),
        ]
        + scratch,
        cost_estimate=pl.CostEstimate(
            flops=work, bytes_accessed=2**20, transcendentals=steps * QROWS * KEYS
        ),
        compiler_params=pltpu.CompilerParams(vmem_limit_bytes=24 * 2**20),
    )(table, *operands, *[in_vmem(part) for part in parts])


def in_vmem(x):
    return pltpu.with_memory_space_constraint(x, pltpu.VMEM)


def in_hbm(x):
    return pltpu.with_memory_space_constraint(x, pltpu.HBM)


def merged(one, two):
    width = HEADS_HERE * V_DIM
    outs = []
    for h in range(HEADS_HERE):
        sizes = []
        for part in (one, two):
            notes = part[:, width : width + 128].astype(jnp.float32)
            sizes.append(
                notes[:, h : h + 1] + notes[:, HEADS_HERE + h : HEADS_HERE + h + 1]
                + notes[:, 2 * HEADS_HERE + h : 2 * HEADS_HERE + h + 1]
            )
        most = jnp.maximum(sizes[0], sizes[1])
        first, second = (jnp.exp2(size - most) for size in sizes)
        cols = slice(h * V_DIM, (h + 1) * V_DIM)
        value = first * one[:, cols].astype(jnp.float32) + second * two[:, cols].astype(jnp.float32)
        outs.append((value / (first + second)).astype(jnp.bfloat16))
    return jnp.concatenate(outs, axis=1)


PIECES = 4


def project_body(
    core, local_part, mirror_same, swapped, mirror_cross, gain, slots, residual, out_early, out_proj_hbm,
    hidden_hbm, outgoing_hbm, hidden, outgoing, out_late, out_sems, late_sem,
):
    fetch = pltpu.make_async_copy(out_proj_hbm.at[:, pl.ds(EARLY, out_late.shape[1])], out_late, late_sem)
    fetch.start()
    half = HEADS_HERE * V_DIM
    mine = merged(local_part[...], mirror_same[...])
    theirs = merged(swapped[...], mirror_cross[...])
    at = pl.multiple_of(core[0] * half, half)
    other = pl.multiple_of((1 - core[0]) * half, half)
    projected = []
    for weights in (out_early, out_late):
        if weights is out_late:
            fetch.wait()
        projected.append(
            jnp.dot(mine, weights[pl.ds(at, half), :], preferred_element_type=jnp.float32)
            + jnp.dot(theirs, weights[pl.ds(other, half), :], preferred_element_type=jnp.float32)
        )
    projected = jnp.concatenate(projected, axis=1)
    result = (residual[...].astype(jnp.float32) + projected).astype(jnp.bfloat16)
    hidden[...] = result
    store = pltpu.make_async_copy(hidden, hidden_hbm, out_sems.at[PIECES])
    store.start()
    wide = result.astype(jnp.float32)
    normed = wide * lax.rsqrt(jnp.mean(wide * wide, axis=-1, keepdims=True) + EPSILON)
    normed = (normed * gain[...]).astype(jnp.bfloat16)
    count = outgoing.shape[0] // PIECES
    stores = [store]
    for n in range(PIECES):
        slot = lax.broadcasted_iota(jnp.int32, (count, normed.shape[0]), 0) + n * count
        pick = (slot == slots[0:1, :]) | (slot == slots[1:2, :])
        pick = jnp.where(pick, 1.0, 0.0).astype(jnp.bfloat16)
        rows = pl.ds(n * count, count)
        outgoing[rows, :] = jnp.dot(pick, normed, preferred_element_type=jnp.float32).astype(jnp.bfloat16)
        store = pltpu.make_async_copy(outgoing.at[rows], outgoing_hbm.at[rows], out_sems.at[n])
        store.start()
        stores.append(store)
    for store in stores:
        store.wait()


def project(core, messages, out_early, out_proj, residual, gain, slots):
    width = residual.shape[1]
    vmem = pl.BlockSpec(memory_space=pltpu.VMEM)
    hbm = pl.BlockSpec(memory_space=pltpu.HBM)
    return pl.pallas_call(
        project_body,
        out_shape=(
            pltpu.HBM((ROWS, width), jnp.bfloat16),
            pltpu.HBM((N_SP * CAP, width), jnp.bfloat16),
        ),
        in_specs=[pl.BlockSpec(memory_space=pltpu.SMEM)] + [vmem] * 8 + [hbm],
        out_specs=(hbm, hbm),
        scratch_shapes=[
            pltpu.VMEM((ROWS, width), jnp.bfloat16),
            pltpu.VMEM((N_SP * CAP, width), jnp.bfloat16),
            pltpu.VMEM((out_proj.shape[0], width - EARLY), jnp.bfloat16),
            pltpu.SemaphoreType.DMA((PIECES + 1,)),
            pltpu.SemaphoreType.DMA,
        ],
        compiler_params=pltpu.CompilerParams(vmem_limit_bytes=16 * 2**20),
        name="project",
    )(core, *messages, gain, slots, in_vmem(residual), in_vmem(out_early), in_hbm(out_proj))


def experts_body(rows, *rest):
    sources = rest[:6]
    out_hbm = rest[6]
    weights = rest[7:13]
    first, out, sems, out_sems = rest[13:]
    loads = []
    for n in range(6):
        load = pltpu.make_async_copy(sources[n], weights[n], sems.at[n])
        load.start()
        loads.append(load)
    count = rows.shape[0]
    block = count // 2
    stores = []
    for n in range(2):
        gate, up, down = weights[3 * n : 3 * n + 3]
        loads[3 * n].wait()
        loads[3 * n + 1].wait()
        actives = []
        for k in range(2):
            x = rows[pl.ds(k * block, block), :]
            gated = jnp.dot(x, gate[...], preferred_element_type=jnp.float32)
            raised = jnp.dot(x, up[...], preferred_element_type=jnp.float32)
            actives.append((gated / (1.0 + jnp.exp(-gated)) * raised).astype(jnp.bfloat16))
        loads[3 * n + 2].wait()
        for k in range(2):
            at = pl.ds(k * block, block)
            product = jnp.dot(actives[k], down[...], preferred_element_type=jnp.float32).astype(jnp.bfloat16)
            if n == 0:
                first[at, :] = product
            else:
                out[at, :] = (first[at, :].astype(jnp.float32) + product.astype(jnp.float32)).astype(jnp.bfloat16)
                store = pltpu.make_async_copy(out.at[at], out_hbm.at[at], out_sems.at[k])
                store.start()
                stores.append(store)
    for store in stores:
        store.wait()


def experts(rows, own, other):
    count, width = rows.shape
    hbm = pl.BlockSpec(memory_space=pltpu.HBM)
    return pl.pallas_call(
        experts_body,
        out_shape=pltpu.HBM((count, width), jnp.bfloat16),
        in_specs=[pl.BlockSpec(memory_space=pltpu.VMEM)] + [hbm] * 6,
        out_specs=hbm,
        scratch_shapes=[pltpu.VMEM(w.shape, w.dtype) for w in (*own, *other)]
        + [
            pltpu.VMEM((count, width), jnp.bfloat16),
            pltpu.VMEM((count, width), jnp.bfloat16),
            pltpu.SemaphoreType.DMA((6,)),
            pltpu.SemaphoreType.DMA((2,)),
        ],
        compiler_params=pltpu.CompilerParams(vmem_limit_bytes=28 * 2**20),
        name="experts",
    )(rows, *[in_hbm(w) for w in (*own, *other)])


def combine_body(back, hidden, slots, weights, out_ref):
    slot = lax.broadcasted_iota(jnp.int32, (hidden.shape[0], back.shape[0]), 1)
    pick = jnp.where(slot == slots[:, 0:1], weights[:, 0:1], 0.0) + jnp.where(
        slot == slots[:, 1:2], weights[:, 1:2], 0.0
    )
    high = pick.astype(jnp.bfloat16)
    low = (pick - high.astype(jnp.float32)).astype(jnp.bfloat16)
    rows = back[...]
    mixed = jnp.dot(high, rows, preferred_element_type=jnp.float32) + jnp.dot(
        low, rows, preferred_element_type=jnp.float32
    )
    out_ref[...] = (hidden[...].astype(jnp.float32) + mixed).astype(jnp.bfloat16)


def combine(back, hidden, slots, weights):
    vmem = pl.BlockSpec(memory_space=pltpu.VMEM)
    return pl.pallas_call(
        combine_body,
        out_shape=jax.ShapeDtypeStruct(hidden.shape, jnp.bfloat16),
        in_specs=[vmem] * 4,
        out_specs=vmem,
        compiler_params=pltpu.CompilerParams(vmem_limit_bytes=16 * 2**20),
        name="combine",
    )(back, hidden, slots, weights)


def rotary(values, positions):
    half_width = values.shape[-1] // 2
    inverse = ROPE_BASE ** (-2.0 * jnp.arange(half_width, dtype=jnp.float32) / values.shape[-1])
    angles = positions.astype(jnp.float32)[:, None] * inverse[None, :]
    cosine = jnp.cos(angles)
    sine_part = jnp.sin(angles)
    if values.ndim == 3:
        cosine = cosine[:, None, :]
        sine_part = sine_part[:, None, :]
    first_half = values[..., :half_width]
    second = values[..., half_width:]
    return jnp.concatenate(
        [first_half * cosine - second * sine_part, second * cosine + first_half * sine_part],
        axis=-1,
    )


def local(
    residual,
    query_nope,
    query_rope,
    latent,
    key_rope,
    key_up,
    value_up,
    out_proj,
    norm_gain,
    routes,
    route_weight,
    w_gate,
    w_up,
    w_down,
):
    tp_index = lax.axis_index("tp")
    sp_index = lax.axis_index("sp")
    tok_dev = query_nope.shape[0]
    query_first = sp_index * tok_dev
    swap = [(0, 1), (1, 0)]

    key_pos = query_first + tp_index * ROWS + jnp.arange(ROWS, dtype=jnp.int32)
    key_rot = rotary(key_rope.astype(jnp.float32), key_pos).astype(jnp.bfloat16)
    packed = jnp.concatenate([key_rot[0:32], key_rot[64:96], key_rot[32:64], key_rot[96:128]], axis=1)
    shard = jnp.concatenate([latent, packed], axis=0)
    mirror = [
        (s * N_TP + t, (N_SP - 1 - s) * N_TP + t) for s in range(N_SP) for t in range(N_TP)
    ]
    crossing = [
        (s * N_TP + t, (N_SP - 1 - s) * N_TP + 1 - t) for s in range(N_SP) for t in range(N_TP)
    ]
    queries = jnp.concatenate([query_nope, query_rope], axis=1)
    received = lax.ppermute(queries, AXES, mirror)

    near = lax.ppermute(shard, AXES, plane_pairs(Z_FIRST))
    far = lax.ppermute(shard, AXES, plane_pairs(Z_SECOND))
    main = (tp_index == 0) == (sp_index < 2 * PLANE)
    both = jnp.concatenate([jnp.where(main, shard, far), near], axis=0)

    flat = routes.reshape(-1)
    order = jnp.arange(flat.shape[0], dtype=jnp.int32)
    earlier = (flat[:, None] == flat[None, :]) & (order[None, :] < order[:, None])
    rank = jnp.sum(earlier.astype(jnp.int32), axis=1)
    slots = (flat * CAP + rank).reshape(routes.shape)
    slots_across = slots.T
    tables = np.concatenate([work_table(call)[1] for call in range(len(CALLS))], axis=1)
    table = lax.dynamic_index_in_dim(jnp.asarray(tables), sp_index * N_TP + tp_index, 0, keepdims=False)
    tokens = jnp.arange(tok_dev, dtype=jnp.int32)
    query_pos = jnp.concatenate([query_first + tokens, (N_SP - 1 - sp_index) * tok_dev + tokens])
    half_width = QK_ROPE // 2
    pair = jnp.arange(HEADS_HERE * QK_ROPE, dtype=jnp.int32) % half_width
    inverse = ROPE_BASE ** (-2.0 * pair.astype(jnp.float32) / QK_ROPE)
    angles = query_pos.astype(jnp.float32)[:, None] * inverse[None, :]
    behind = jnp.arange(HEADS_HERE * QK_ROPE, dtype=jnp.int32) % QK_ROPE >= half_width
    cosine = jnp.cos(angles)
    sine = jnp.where(behind[None, :], jnp.sin(angles), -jnp.sin(angles))
    got = [both]
    for by in SHIFTS[1:]:
        got.append(lax.ppermute(both, AXES, shift_pairs(0, by)))
    both = jnp.concatenate(got, axis=0)

    both, table, slots, slots_across, cosine, sine = lax.optimization_barrier(
        (both, table, slots, slots_across, cosine, sine)
    )
    around = []
    for by in (1, -1):
        around.append(lax.ppermute(both, AXES, shift_pairs(1, by)))
    half = both.shape[0] // 2
    beyond = []
    for n, by in enumerate((1, -1)):
        passed = around[n][n * half : (n + 1) * half]
        beyond.append(lax.ppermute(passed, AXES, shift_pairs(1, by)))
    own_parts = [[both], [around[0]], [around[1]], beyond]
    other_parts = []
    for group in own_parts:
        other_parts.append([lax.ppermute(part, "tp", swap) for part in group])
    pieces = (own_parts, other_parts)
    own_weights = (w_gate[0], w_up[0], w_down[0])
    other_weights = []
    for w in own_weights:
        other_weights.append(lax.ppermute(w, "tp", swap))

    state = ()
    for call in range(len(CALLS)):
        operands = (
            (query_nope, query_rope, received, key_up, cosine, sine) if call == 0 else (q4, qabs, *state)
        )
        if call == len(CALLS) - 1:
            operands = (*operands, value_up, out_proj, residual)
        state = attention(call, table, operands, [part for own, k3 in CALLS[call] for part in pieces[own][k3]])
        if call == 0:
            qabs, q4, *state = state
    attn, out_early, residual = state[:3]
    mirror_same = lax.ppermute(attn[2], AXES, mirror)
    mirror_cross = lax.ppermute(attn[3], AXES, crossing)
    swapped = lax.ppermute(attn[1], "tp", swap)
    messages = (attn[0], mirror_same, swapped, mirror_cross)

    hidden, outgoing = project(
        tp_index.reshape(1).astype(jnp.int32), messages, out_early, out_proj, residual, norm_gain[None, :], slots_across
    )
    width = residual.shape[1]
    arrived = lax.all_to_all(
        outgoing.reshape(N_SP, CAP, width), "sp", split_axis=0, concat_axis=0, tiled=True
    ).reshape(N_SP * CAP, width)
    produced = experts(arrived, own_weights, other_weights)
    back = lax.all_to_all(
        produced.reshape(N_SP, CAP, width), "sp", split_axis=0, concat_axis=0, tiled=True
    ).reshape(N_SP * CAP, width)
    return combine(back, hidden, slots, route_weight)


def solution(mesh):
    return jax.shard_map(
        local,
        mesh=mesh,
        in_specs=(
            P(("sp", "tp"), None),
            P("sp", "tp"),
            P("sp", "tp"),
            P(("sp", "tp"), None),
            P(("sp", "tp"), None),
            P(None, "tp"),
            P(None, "tp"),
            P(),
            P(),
            P(("sp", "tp"), None),
            P(("sp", "tp"), None),
            P("sp", None, "tp"),
            P("sp", None, "tp"),
            P("sp", "tp", None),
        ),
        out_specs=P(("sp", "tp"), None),
        check_vma=False,
    )
```

```python
import functools
import jax
import jax.numpy as jnp
import numpy as np
from jax import lax
from jax.experimental import pallas as pl
from jax.experimental.pallas import tpu as pltpu
from jax.sharding import PartitionSpec as P

QK_NOPE = 128
QK_ROPE = 64
V_DIM = 128
LATENT = 256
SEGMENT = 64
EPSILON = 1e-06
ROPE_BASE = 10000.0
NEG_LARGE = -1e30

N_SP = 64
N_TP = 2
HEADS_HERE = 4
ROWS = 128
SHARD = 160
UNIT = 4
KEYS = UNIT * ROWS
QROWS = HEADS_HERE * ROWS
CAP = 8
AXES = ("sp", "tp")
STEP = {"x": 1, "y": 4, "z": 16}
Z_FIRST = {(0, 0): (3, 0), (1, 0): (2, 0), (0, 1): (1, 0), (1, 1): (0, 0), (2, 1): (1, 1), (3, 1): (0, 1), (2, 0): (3, 1), (3, 0): (2, 1)}
Z_SECOND = {(0, 1): (2, 0), (1, 1): (3, 0), (2, 0): (0, 1), (3, 0): (1, 1)}
ORDER = (("y", "x"), ("x", "y"))
SHIFTS = (0, 1, -1, 2)
SCALE2 = float((QK_NOPE + QK_ROPE) ** (-0.5) * np.log2(np.e))
PLANE = 16
GROUPS = 4
CHUNK = 64
MESSAGE = HEADS_HERE * V_DIM + 128
EARLY = 1024


def moved(s, dim, by):
    step = STEP[dim]
    c = (s // step) % 4
    return s + step * ((c + by) % 4 - c)


def shift_pairs(phase, by):
    return [
        (s * N_TP + t, moved(s, ORDER[t][phase], by) * N_TP + t)
        for s in range(N_SP)
        for t in range(N_TP)
    ]


def partner(s):
    z, y, x = s // 16, (s // 4) % 4, s % 4
    return (3 - z) * 16 + (3 - y) * 4 + x


def shard_source(s, t, k2, kz):
    s = moved(s, ORDER[t][0], -SHIFTS[k2])
    z, r = divmod(s, PLANE)
    source = (z, t)
    if kz == 1:
        source = Z_FIRST[source]
    elif source in Z_SECOND:
        source = Z_SECOND[source]
    return source[0] * PLANE + r, source[1]


def line_pairs(k2, kz):
    pairs = []
    for s in range(N_SP):
        for t in range(N_TP):
            chip, core = shard_source(s, t, k2, kz)
            if (chip, core) != (s, t):
                pairs.append((chip * N_TP + core, s * N_TP + t))
    return pairs


def shard_first(s, t, k3, k2, kz):
    chip, core = shard_source(moved(s, ORDER[t][1], -SHIFTS[k3]), t, k2, kz)
    return 4 * chip + 2 * core


CALLS = (((0, 0), (1, 0)), ((0, 1), (0, 2)), ((1, 1), (1, 2)), ((0, 3), (1, 3)))


@functools.lru_cache(None)
def work_table(call):
    lists = []
    for s in range(N_SP):
        for t in range(N_TP):
            firsts = [
                shard_first(s, t if own == 0 else 1 - t, k3, k2, kz)
                for own, k3 in CALLS[call]
                for k2 in range(4)
                for kz in range(2)
            ]
            rows = []
            for group in range(GROUPS):
                block = s if group < 2 else partner(s)
                base = 4 * block + 2 * (group % 2)
                needed = [n for n in range(len(firsts)) if firsts[n] <= base + 1]
                for at in range(0, len(needed), UNIT):
                    part = needed[at : at + UNIT]
                    segs = [firsts[n] for n in part] + [1 << 20] * (UNIT - len(part))
                    part = part + [part[-1]] * (UNIT - len(part))
                    bits = 0
                    for half in range(2):
                        for j in range(UNIT):
                            for late in range(2):
                                if segs[j] + half > base + late:
                                    bits |= 1 << ((half * UNIT + j) * 2 + late)
                    rows.append([group, bits, t] + part)
            lists.append(rows)
    count = max(len(rows) for rows in lists)
    everything = (1 << (4 * UNIT)) - 1
    idle = lambda rows, t: rows[-1][:1] + [everything] + rows[-1][2:] if rows else [0, everything, t] + [0] * UNIT
    table = []
    for n, rows in enumerate(lists):
        table.append(rows + [idle(rows, n % N_TP)] * (count + 1 - len(rows)))
    return count, np.array(table, np.int32).reshape(len(lists), -1)


NT = (((1,), (1,)), ((), ()))


def attention_body(call, steps, offset, part_count, table, *rest):
    first, last = call == 0, call == len(CALLS) - 1
    rest = list(rest)
    take = lambda n: [rest.pop(0) for _ in range(n)]
    if first:
        own_ref, own_rope_ref, received_ref, key_up_ref, cosine_ref, sine_ref = take(6)
    else:
        q4_ref, qabs, _, _, _ = take(5)
    if last:
        value_up_ref, out_proj_hbm, residual_hbm = take(3)
    parts = take(part_count)
    if last:
        home_same, home_cross, away_same, away_cross, out_proj_ref, residual_ref = take(6)
    if first:
        qabs, q4_ref = take(2)
    m_ref, l_ref, acc_ref, keys, s0, s1, p0, p1, shrink0, shrink1 = take(10)
    fetches = []
    if last:
        (sems,) = rest
        early = pl.ds(0, out_proj_ref.shape[1])
        for n, (source, target) in enumerate(((out_proj_hbm.at[:, early], out_proj_ref), (residual_hbm, residual_ref))):
            fetch = pltpu.make_async_copy(source, target, sems.at[n])
            fetch.start()
            fetches.append(fetch)
    at = 0
    for part in parts:
        for k in range(2):
            keys[k, pl.ds(at, part.shape[0]), :] = part[:, pl.ds(k * 128, 128)]
        at += part.shape[0]
    if first:
        for g in range(GROUPS):
            source = own_ref if g < 2 else received_ref
            for h in range(HEADS_HERE):
                cols = pl.ds(h * QK_NOPE, QK_NOPE)
                latent_query = lax.dot_general(
                    source[pl.ds((g % 2) * ROWS, ROWS), cols],
                    key_up_ref[:, cols],
                    NT,
                    preferred_element_type=jnp.float32,
                ).astype(jnp.bfloat16)
                for k in range(2):
                    qabs[g, k, pl.ds(h * ROWS, ROWS), :] = latent_query[:, k * 128 : (k + 1) * 128]
        lane = lax.broadcasted_iota(jnp.int32, (ROWS, 128), 1)
        for g in range(GROUPS):
            tokens = pl.ds((g % 2) * ROWS, ROWS)
            for k in range(2):
                cols = pl.ds(k * 128, 128)
                if g < 2:
                    x = own_rope_ref[tokens, cols]
                else:
                    x = received_ref[tokens, pl.ds(HEADS_HERE * QK_NOPE + k * 128, 128)]
                x = x.astype(jnp.float32)
                opposite = jnp.where(lane % QK_ROPE < QK_ROPE // 2, pltpu.roll(x, 96, 1), pltpu.roll(x, 32, 1))
                at = pl.ds(g * ROWS, ROWS)
                turned = (x * cosine_ref[at, cols] + opposite * sine_ref[at, cols]).astype(jnp.bfloat16).astype(jnp.float32)
                flipped = pltpu.roll(turned, QK_ROPE, 1)
                for odd in range(2):
                    rows = pl.ds((2 * k + odd) * ROWS, ROWS)
                    for half in range(2):
                        source = turned if odd == half else flipped
                        keep = lane < QK_ROPE if half == 0 else lane >= QK_ROPE
                        q4_ref[g, half, rows, :] = jnp.where(keep, source, 0.0).astype(jnp.bfloat16)
        m_ref[...] = jnp.full(m_ref.shape, NEG_LARGE, jnp.float32)
        l_ref[...] = jnp.zeros(l_ref.shape, jnp.float32)
        acc_ref[...] = jnp.zeros(acc_ref.shape, jnp.float32)

    cols_per_step = 3 + UNIT

    def field(u, n):
        return table[offset + u * cols_per_step + n]

    def wide(at, count):
        rows = pl.ds(pl.multiple_of(at, 32), count)
        return jnp.concatenate([keys[k, rows, :] for k in range(2)], axis=1)

    def latent_tile(u, half):
        return jnp.concatenate([wide(field(u, 3 + j) * SHARD + half * SEGMENT, SEGMENT) for j in range(UNIT)], axis=0)

    note_lane = lax.broadcasted_iota(jnp.int32, (16, 128), 1)
    mark = [jnp.where(note_lane == n, 1.0, 0.0).astype(jnp.bfloat16) for n in range(2)]
    marks = jnp.concatenate(([mark[0]] * (SEGMENT // 16) + [mark[1]] * (SEGMENT // 16)) * HEADS_HERE, axis=0)

    def scores(u, s_ref):
        g = field(u, 0)
        bits = field(u, 1)
        rot = jnp.concatenate(
            [
                keys[h, pl.ds(pl.multiple_of(field(u, 3 + j) * SHARD + ROWS, 32), 32), :]
                for j in range(UNIT)
                for h in range(2)
            ],
            axis=0,
        )
        q = jnp.concatenate([qabs[g, k] for k in range(2)], axis=1)
        for half in range(2):
            notes = []
            for j in range(UNIT):
                at = (half * UNIT + j) * 2
                early, late = (
                    jnp.where((bits >> (at + n)) & 1 == 1, jnp.float32(NEG_LARGE), jnp.float32(0.0)) for n in range(2)
                )
                note = jnp.where(note_lane == 0, early, jnp.where(note_lane == 1, late, 0.0)).astype(jnp.bfloat16)
                notes += [note] * (SEGMENT // 16)
            extra = jnp.concatenate([rot, jnp.concatenate(notes, axis=0)], axis=1)
            total = lax.dot_general(
                q, latent_tile(u, half), NT, preferred_element_type=jnp.float32
            ) + lax.dot_general(
                jnp.concatenate([q4_ref[g, half], marks], axis=1), extra, NT, preferred_element_type=jnp.float32
            )
            for k in range(2):
                s_ref[half * 2 + k, pl.ds(0, QROWS), :] = total[:, k * 128 : (k + 1) * 128]

    def absorb(u, s_ref, p_ref, shrink_ref):
        g = field(u, 0)
        for at in range(0, QROWS, CHUNK):
            rows = pl.ds(at, CHUNK)
            s = [s_ref[k, rows, :] for k in range(KEYS // 128)]
            before = m_ref[g, rows, :]
            top = jnp.maximum(jnp.maximum(s[0], s[1]), jnp.maximum(s[2], s[3]))
            after = jnp.maximum(before, jnp.max(top, axis=1, keepdims=True))
            m_ref[g, rows, :] = after
            shrink = jnp.exp2((before - after) * SCALE2)
            shrink_ref[rows, :] = shrink
            after = after * SCALE2
            partial = l_ref[g, rows, :] * shrink
            for k in range(KEYS // 128):
                p = jnp.exp2(s[k] * SCALE2 - after)
                partial = partial + p
                p_ref[k, rows, :] = p.astype(jnp.bfloat16)
            l_ref[g, rows, :] = partial
        values = jnp.concatenate([latent_tile(u, 0), latent_tile(u, 1)], axis=0)
        for at in range(0, QROWS, QROWS // 2):
            rows = pl.ds(at, QROWS // 2)
            weights = jnp.concatenate([p_ref[k, rows, :] for k in range(KEYS // 128)], axis=1)
            product = jnp.dot(weights, values, preferred_element_type=jnp.float32)
            for k in range(LATENT // 128):
                acc_ref[g, k, rows, :] = (
                    acc_ref[g, k, rows, :] * shrink_ref[rows, :] + product[:, k * 128 : (k + 1) * 128]
                )

    scores(0, s0)

    def pair(k, carry):
        u = k * 2
        scores(u + 1, s1)
        absorb(u, s0, p0, shrink0)
        scores(u + 2, s0)
        absorb(u + 1, s1, p1, shrink1)
        return carry

    lax.fori_loop(0, (steps - 1) // 2, pair, 0)
    if steps % 2 == 0:
        scores(steps - 1, s1)
        absorb(steps - 2, s0, p0, shrink0)
        absorb(steps - 1, s1, p1, shrink1)
    else:
        absorb(steps - 1, s0, p0, shrink0)
    if not last:
        return
    core = field(0, 2)
    lane = lax.broadcasted_iota(jnp.int32, (ROWS, 128), 1)
    for g in range(GROUPS):
        total = jnp.sum(l_ref[g], axis=1, keepdims=True)
        total = jnp.where(total > 0.0, total, 1.0)
        mean = jnp.concatenate([acc_ref[g, k] / total for k in range(2)], axis=1).astype(jnp.bfloat16)
        size = m_ref[g] * SCALE2 + jnp.log2(total)
        notes = jnp.zeros((ROWS, 128), jnp.bfloat16)
        message = []
        for h in range(HEADS_HERE):
            cols = pl.ds(h * V_DIM, V_DIM)
            rows = slice(h * ROWS, (h + 1) * ROWS)
            message.append(
                jnp.dot(mean[rows], value_up_ref[:, cols], preferred_element_type=jnp.float32).astype(jnp.bfloat16)
            )
            left = size[rows]
            for n in range(3):
                term = left.astype(jnp.bfloat16)
                notes = jnp.where(lane == n * HEADS_HERE + h, term, notes)
                left = left - term.astype(jnp.float32)
        message = jnp.concatenate(message + [notes], axis=1)
        same, cross = (home_same, home_cross) if g < 2 else (away_same, away_cross)

        @pl.when(core == g % 2)
        def _(same=same, message=message):
            same[...] = message

        @pl.when(core != g % 2)
        def _(cross=cross, message=message):
            cross[...] = message

    for fetch in fetches:
        fetch.wait()


def attention(call, table, operands, parts):
    vmem = pl.BlockSpec(memory_space=pltpu.VMEM)
    hbm = pl.BlockSpec(memory_space=pltpu.HBM)
    steps = work_table(call)[0]
    offset = sum(work_table(n)[1].shape[1] for n in range(call))
    first, last = call == 0, call == len(CALLS) - 1
    outs = [
        pltpu.VMEM((GROUPS, QROWS, 128), jnp.float32),
        pltpu.VMEM((GROUPS, QROWS, 128), jnp.float32),
        pltpu.VMEM((GROUPS, 2, QROWS, 128), jnp.float32),
    ]
    specs = [vmem] * len(operands)
    scratch = []
    aliases = {}
    if first:
        outs = [pltpu.VMEM((GROUPS, 2, QROWS, 128), jnp.bfloat16)] * 2 + outs
    elif last:
        fetched = operands[-2:]
        outs = [
            *[pltpu.VMEM((ROWS, MESSAGE), jnp.bfloat16)] * 4,
            pltpu.VMEM((fetched[0].shape[0], EARLY), jnp.bfloat16),
            pltpu.VMEM(fetched[1].shape, jnp.bfloat16),
        ] + outs
        specs = specs[:-2] + [hbm] * 2
        operands = (*operands[:-2], *[in_hbm(f) for f in fetched])
        scratch = [pltpu.SemaphoreType.DMA((2,))]
    if not first:
        aliases = {3 + n: len(outs) - 3 + n for n in range(3)}
        operands = tuple(in_vmem(x) if 1 <= n < 5 else x for n, x in enumerate(operands))
    work = steps * QROWS * KEYS * 3 * LATENT * 2
    return pl.pallas_call(
        functools.partial(attention_body, call, steps, offset, len(parts)),
        out_shape=outs,
        in_specs=[pl.BlockSpec(memory_space=pltpu.SMEM)] + specs + [vmem] * len(parts),
        out_specs=[vmem] * len(outs),
        input_output_aliases=aliases,
        scratch_shapes=[
            pltpu.VMEM((2, sum(part.shape[0] for part in parts), 128), jnp.bfloat16),
            pltpu.VMEM((KEYS // 128, QROWS, 128), jnp.float32),
            pltpu.VMEM((KEYS // 128, QROWS, 128), jnp.float32),
            pltpu.VMEM((KEYS // 128, QROWS, 128), jnp.bfloat16),
            pltpu.VMEM((KEYS // 128, QROWS, 128), jnp.bfloat16),
            pltpu.VMEM((QROWS, 128), jnp.float32),
            pltpu.VMEM((QROWS, 128), jnp.float32),
        ]
        + scratch,
        cost_estimate=pl.CostEstimate(
            flops=work, bytes_accessed=2**20, transcendentals=steps * QROWS * KEYS
        ),
        compiler_params=pltpu.CompilerParams(vmem_limit_bytes=24 * 2**20),
    )(table, *operands, *[in_vmem(part) for part in parts])


def in_vmem(x):
    return pltpu.with_memory_space_constraint(x, pltpu.VMEM)


def in_hbm(x):
    return pltpu.with_memory_space_constraint(x, pltpu.HBM)


def merged(one, two):
    width = HEADS_HERE * V_DIM
    outs = []
    for h in range(HEADS_HERE):
        sizes = []
        for part in (one, two):
            notes = part[:, width : width + 128].astype(jnp.float32)
            sizes.append(
                notes[:, h : h + 1] + notes[:, HEADS_HERE + h : HEADS_HERE + h + 1]
                + notes[:, 2 * HEADS_HERE + h : 2 * HEADS_HERE + h + 1]
            )
        most = jnp.maximum(sizes[0], sizes[1])
        first, second = (jnp.exp2(size - most) for size in sizes)
        cols = slice(h * V_DIM, (h + 1) * V_DIM)
        value = first * one[:, cols].astype(jnp.float32) + second * two[:, cols].astype(jnp.float32)
        outs.append((value / (first + second)).astype(jnp.bfloat16))
    return jnp.concatenate(outs, axis=1)


PIECES = 4


def project_body(
    core, local_part, mirror_same, swapped, mirror_cross, gain, slots, residual, out_early, out_proj_hbm,
    hidden_hbm, outgoing_hbm, hidden, outgoing, out_late, out_sems, late_sem,
):
    fetch = pltpu.make_async_copy(out_proj_hbm.at[:, pl.ds(EARLY, out_late.shape[1])], out_late, late_sem)
    fetch.start()
    half = HEADS_HERE * V_DIM
    mine = merged(local_part[...], mirror_same[...])
    theirs = merged(swapped[...], mirror_cross[...])
    at = pl.multiple_of(core[0] * half, half)
    other = pl.multiple_of((1 - core[0]) * half, half)
    projected = []
    for weights in (out_early, out_late):
        if weights is out_late:
            fetch.wait()
        projected.append(
            jnp.dot(mine, weights[pl.ds(at, half), :], preferred_element_type=jnp.float32)
            + jnp.dot(theirs, weights[pl.ds(other, half), :], preferred_element_type=jnp.float32)
        )
    projected = jnp.concatenate(projected, axis=1)
    result = (residual[...].astype(jnp.float32) + projected).astype(jnp.bfloat16)
    hidden[...] = result
    store = pltpu.make_async_copy(hidden, hidden_hbm, out_sems.at[PIECES])
    store.start()
    wide = result.astype(jnp.float32)
    normed = wide * lax.rsqrt(jnp.mean(wide * wide, axis=-1, keepdims=True) + EPSILON)
    normed = (normed * gain[...]).astype(jnp.bfloat16)
    count = outgoing.shape[0] // PIECES
    stores = [store]
    for n in range(PIECES):
        slot = lax.broadcasted_iota(jnp.int32, (count, normed.shape[0]), 0) + n * count
        pick = (slot == slots[0:1, :]) | (slot == slots[1:2, :])
        pick = jnp.where(pick, 1.0, 0.0).astype(jnp.bfloat16)
        rows = pl.ds(n * count, count)
        outgoing[rows, :] = jnp.dot(pick, normed, preferred_element_type=jnp.float32).astype(jnp.bfloat16)
        store = pltpu.make_async_copy(outgoing.at[rows], outgoing_hbm.at[rows], out_sems.at[n])
        store.start()
        stores.append(store)
    for store in stores:
        store.wait()


def project(core, messages, out_early, out_proj, residual, gain, slots):
    width = residual.shape[1]
    vmem = pl.BlockSpec(memory_space=pltpu.VMEM)
    hbm = pl.BlockSpec(memory_space=pltpu.HBM)
    return pl.pallas_call(
        project_body,
        out_shape=(
            pltpu.HBM((ROWS, width), jnp.bfloat16),
            pltpu.HBM((N_SP * CAP, width), jnp.bfloat16),
        ),
        in_specs=[pl.BlockSpec(memory_space=pltpu.SMEM)] + [vmem] * 8 + [hbm],
        out_specs=(hbm, hbm),
        scratch_shapes=[
            pltpu.VMEM((ROWS, width), jnp.bfloat16),
            pltpu.VMEM((N_SP * CAP, width), jnp.bfloat16),
            pltpu.VMEM((out_proj.shape[0], width - EARLY), jnp.bfloat16),
            pltpu.SemaphoreType.DMA((PIECES + 1,)),
            pltpu.SemaphoreType.DMA,
        ],
        compiler_params=pltpu.CompilerParams(vmem_limit_bytes=16 * 2**20),
        name="project",
    )(core, *messages, gain, slots, in_vmem(residual), in_vmem(out_early), in_hbm(out_proj))


def experts_body(rows, *rest):
    sources = rest[:6]
    out_hbm = rest[6]
    weights = rest[7:13]
    first, out, sems, out_sems = rest[13:]
    loads = []
    for n in range(6):
        load = pltpu.make_async_copy(sources[n], weights[n], sems.at[n])
        load.start()
        loads.append(load)
    count = rows.shape[0]
    block = count // 2
    stores = []
    for n in range(2):
        gate, up, down = weights[3 * n : 3 * n + 3]
        loads[3 * n].wait()
        loads[3 * n + 1].wait()
        actives = []
        for k in range(2):
            x = rows[pl.ds(k * block, block), :]
            gated = jnp.dot(x, gate[...], preferred_element_type=jnp.float32)
            raised = jnp.dot(x, up[...], preferred_element_type=jnp.float32)
            actives.append((gated / (1.0 + jnp.exp(-gated)) * raised).astype(jnp.bfloat16))
        loads[3 * n + 2].wait()
        for k in range(2):
            at = pl.ds(k * block, block)
            product = jnp.dot(actives[k], down[...], preferred_element_type=jnp.float32).astype(jnp.bfloat16)
            if n == 0:
                first[at, :] = product
            else:
                out[at, :] = (first[at, :].astype(jnp.float32) + product.astype(jnp.float32)).astype(jnp.bfloat16)
                store = pltpu.make_async_copy(out.at[at], out_hbm.at[at], out_sems.at[k])
                store.start()
                stores.append(store)
    for store in stores:
        store.wait()


def experts(rows, own, other):
    count, width = rows.shape
    hbm = pl.BlockSpec(memory_space=pltpu.HBM)
    return pl.pallas_call(
        experts_body,
        out_shape=pltpu.HBM((count, width), jnp.bfloat16),
        in_specs=[pl.BlockSpec(memory_space=pltpu.VMEM)] + [hbm] * 6,
        out_specs=hbm,
        scratch_shapes=[pltpu.VMEM(w.shape, w.dtype) for w in (*own, *other)]
        + [
            pltpu.VMEM((count, width), jnp.bfloat16),
            pltpu.VMEM((count, width), jnp.bfloat16),
            pltpu.SemaphoreType.DMA((6,)),
            pltpu.SemaphoreType.DMA((2,)),
        ],
        compiler_params=pltpu.CompilerParams(vmem_limit_bytes=28 * 2**20),
        name="experts",
    )(rows, *[in_hbm(w) for w in (*own, *other)])


def combine_body(back, hidden, slots, weights, out_ref):
    slot = lax.broadcasted_iota(jnp.int32, (hidden.shape[0], back.shape[0]), 1)
    pick = jnp.where(slot == slots[:, 0:1], weights[:, 0:1], 0.0) + jnp.where(
        slot == slots[:, 1:2], weights[:, 1:2], 0.0
    )
    high = pick.astype(jnp.bfloat16)
    low = (pick - high.astype(jnp.float32)).astype(jnp.bfloat16)
    rows = back[...]
    mixed = jnp.dot(high, rows, preferred_element_type=jnp.float32) + jnp.dot(
        low, rows, preferred_element_type=jnp.float32
    )
    out_ref[...] = (hidden[...].astype(jnp.float32) + mixed).astype(jnp.bfloat16)


def combine(back, hidden, slots, weights):
    vmem = pl.BlockSpec(memory_space=pltpu.VMEM)
    return pl.pallas_call(
        combine_body,
        out_shape=jax.ShapeDtypeStruct(hidden.shape, jnp.bfloat16),
        in_specs=[vmem] * 4,
        out_specs=vmem,
        compiler_params=pltpu.CompilerParams(vmem_limit_bytes=16 * 2**20),
        name="combine",
    )(back, hidden, slots, weights)


def rotary(values, positions):
    half_width = values.shape[-1] // 2
    inverse = ROPE_BASE ** (-2.0 * jnp.arange(half_width, dtype=jnp.float32) / values.shape[-1])
    angles = positions.astype(jnp.float32)[:, None] * inverse[None, :]
    cosine = jnp.cos(angles)
    sine_part = jnp.sin(angles)
    if values.ndim == 3:
        cosine = cosine[:, None, :]
        sine_part = sine_part[:, None, :]
    first_half = values[..., :half_width]
    second = values[..., half_width:]
    return jnp.concatenate(
        [first_half * cosine - second * sine_part, second * cosine + first_half * sine_part],
        axis=-1,
    )


def local(
    residual,
    query_nope,
    query_rope,
    latent,
    key_rope,
    key_up,
    value_up,
    out_proj,
    norm_gain,
    routes,
    route_weight,
    w_gate,
    w_up,
    w_down,
):
    tp_index = lax.axis_index("tp")
    sp_index = lax.axis_index("sp")
    tok_dev = query_nope.shape[0]
    query_first = sp_index * tok_dev
    swap = [(0, 1), (1, 0)]

    key_pos = query_first + tp_index * ROWS + jnp.arange(ROWS, dtype=jnp.int32)
    key_rot = rotary(key_rope.astype(jnp.float32), key_pos).astype(jnp.bfloat16)
    packed = jnp.concatenate([key_rot[0:32], key_rot[64:96], key_rot[32:64], key_rot[96:128]], axis=1)
    shard = jnp.concatenate([latent, packed], axis=0)
    mirror = [
        (s * N_TP + t, partner(s) * N_TP + t) for s in range(N_SP) for t in range(N_TP)
    ]
    crossing = [
        (s * N_TP + t, partner(s) * N_TP + 1 - t) for s in range(N_SP) for t in range(N_TP)
    ]
    queries = jnp.concatenate([query_nope, query_rope], axis=1)
    received = lax.ppermute(queries, AXES, mirror)

    flat = routes.reshape(-1)
    order = jnp.arange(flat.shape[0], dtype=jnp.int32)
    earlier = (flat[:, None] == flat[None, :]) & (order[None, :] < order[:, None])
    rank = jnp.sum(earlier.astype(jnp.int32), axis=1)
    slots = (flat * CAP + rank).reshape(routes.shape)
    slots_across = slots.T
    tables = np.concatenate([work_table(call)[1] for call in range(len(CALLS))], axis=1)
    table = lax.dynamic_index_in_dim(jnp.asarray(tables), sp_index * N_TP + tp_index, 0, keepdims=False)
    tokens = jnp.arange(tok_dev, dtype=jnp.int32)
    query_pos = jnp.concatenate([query_first + tokens, partner(sp_index) * tok_dev + tokens])
    half_width = QK_ROPE // 2
    pair = jnp.arange(HEADS_HERE * QK_ROPE, dtype=jnp.int32) % half_width
    inverse = ROPE_BASE ** (-2.0 * pair.astype(jnp.float32) / QK_ROPE)
    angles = query_pos.astype(jnp.float32)[:, None] * inverse[None, :]
    behind = jnp.arange(HEADS_HERE * QK_ROPE, dtype=jnp.int32) % QK_ROPE >= half_width
    cosine = jnp.cos(angles)
    sine = jnp.where(behind[None, :], jnp.sin(angles), -jnp.sin(angles))
    main = (tp_index == 0) == (sp_index < 2 * PLANE)
    got = []
    for n in range(8):
        k2, kz = divmod(n, 2)
        piece = lax.ppermute(shard, AXES, line_pairs(k2, kz))
        got.append(jnp.where(main, shard, piece) if n == 0 else piece)
    both = jnp.concatenate(got, axis=0)
    both, table, slots, slots_across, cosine, sine = lax.optimization_barrier(
        (both, table, slots, slots_across, cosine, sine)
    )
    around = []
    for by in (1, -1):
        around.append(lax.ppermute(both, AXES, shift_pairs(1, by)))
    half = both.shape[0] // 2
    beyond = []
    for n, by in enumerate((1, -1)):
        passed = around[n][n * half : (n + 1) * half]
        beyond.append(lax.ppermute(passed, AXES, shift_pairs(1, by)))
    own_parts = [[both], [around[0]], [around[1]], beyond]
    other_parts = []
    for group in own_parts:
        other_parts.append([lax.ppermute(part, "tp", swap) for part in group])
    pieces = (own_parts, other_parts)
    own_weights = (w_gate[0], w_up[0], w_down[0])
    other_weights = []
    for w in own_weights:
        other_weights.append(lax.ppermute(w, "tp", swap))

    state = ()
    for call in range(len(CALLS)):
        operands = (
            (query_nope, query_rope, received, key_up, cosine, sine) if call == 0 else (q4, qabs, *state)
        )
        if call == len(CALLS) - 1:
            operands = (*operands, value_up, out_proj, residual)
        state = attention(call, table, operands, [part for own, k3 in CALLS[call] for part in pieces[own][k3]])
        if call == 0:
            qabs, q4, *state = state
    home_same, home_cross, away_same, away_cross, out_early, residual = state[:6]
    mirror_same = lax.ppermute(away_same, AXES, mirror)
    mirror_cross = lax.ppermute(away_cross, AXES, crossing)
    swapped = lax.ppermute(home_cross, "tp", swap)
    messages = (home_same, mirror_same, swapped, mirror_cross)

    hidden, outgoing = project(
        tp_index.reshape(1).astype(jnp.int32), messages, out_early, out_proj, residual, norm_gain[None, :], slots_across
    )
    width = residual.shape[1]
    arrived = lax.all_to_all(
        outgoing.reshape(N_SP, CAP, width), "sp", split_axis=0, concat_axis=0, tiled=True
    ).reshape(N_SP * CAP, width)
    produced = experts(arrived, own_weights, other_weights)
    back = lax.all_to_all(
        produced.reshape(N_SP, CAP, width), "sp", split_axis=0, concat_axis=0, tiled=True
    ).reshape(N_SP * CAP, width)
    return combine(back, hidden, slots, route_weight)


def solution(mesh):
    return jax.shard_map(
        local,
        mesh=mesh,
        in_specs=(
            P(("sp", "tp"), None),
            P("sp", "tp"),
            P("sp", "tp"),
            P(("sp", "tp"), None),
            P(("sp", "tp"), None),
            P(None, "tp"),
            P(None, "tp"),
            P(),
            P(),
            P(("sp", "tp"), None),
            P(("sp", "tp"), None),
            P("sp", None, "tp"),
            P("sp", None, "tp"),
            P("sp", "tp", None),
        ),
        out_specs=P(("sp", "tp"), None),
        check_vma=False,
    )
```

```python
import functools
import jax
import jax.numpy as jnp
import numpy as np
from jax import lax
from jax.experimental import pallas as pl
from jax.experimental.pallas import tpu as pltpu
from jax.sharding import PartitionSpec as P

QK_NOPE = 128
QK_ROPE = 64
V_DIM = 128
LATENT = 256
SEGMENT = 64
EPSILON = 1e-06
ROPE_BASE = 10000.0
NEG_LARGE = -1e30

N_SP = 64
N_TP = 2
HEADS_HERE = 4
ROWS = 128
SHARD = 160
UNIT = 4
KEYS = UNIT * ROWS
QROWS = HEADS_HERE * ROWS
CAP = 8
AXES = ("sp", "tp")
STEP = {"x": 1, "y": 4, "z": 16}
Z_FIRST = {(0, 0): (3, 0), (1, 0): (2, 0), (0, 1): (1, 0), (1, 1): (0, 0), (2, 1): (1, 1), (3, 1): (0, 1), (2, 0): (3, 1), (3, 0): (2, 1)}
Z_SECOND = {(0, 1): (2, 0), (1, 1): (3, 0), (2, 0): (0, 1), (3, 0): (1, 1)}
ORDER = (("y", "x"), ("x", "y"))
SHIFTS = (0, 1, -1, 2)
SCALE2 = float((QK_NOPE + QK_ROPE) ** (-0.5) * np.log2(np.e))
PLANE = 16
GROUPS = 4
CHUNK = 64
MESSAGE = HEADS_HERE * V_DIM + 128
EARLY = 1024


def moved(s, dim, by):
    step = STEP[dim]
    c = (s // step) % 4
    return s + step * ((c + by) % 4 - c)


def shift_pairs(phase, by):
    return [
        (s * N_TP + t, moved(s, ORDER[t][phase], by) * N_TP + t)
        for s in range(N_SP)
        for t in range(N_TP)
    ]


def partner(s):
    z, y, x = s // 16, (s // 4) % 4, s % 4
    return (3 - z) * 16 + (3 - y) * 4 + x


def shard_source(s, t, k2, kz):
    s = moved(s, ORDER[t][0], -SHIFTS[k2])
    z, r = divmod(s, PLANE)
    source = (z, t)
    if kz == 1:
        source = Z_FIRST[source]
    elif source in Z_SECOND:
        source = Z_SECOND[source]
    return source[0] * PLANE + r, source[1]


def plane_pairs(table):
    return [
        ((from_z * PLANE + r) * N_TP + from_core, (z * PLANE + r) * N_TP + core)
        for (z, core), (from_z, from_core) in table.items()
        for r in range(PLANE)
    ]


def shard_first(s, t, k3, k2, kz):
    chip, core = shard_source(moved(s, ORDER[t][1], -SHIFTS[k3]), t, k2, kz)
    return 4 * chip + 2 * core


CALLS = (((0, 0), (1, 0)), ((0, 1), (0, 2)), ((1, 1), (1, 2)), ((0, 3), (1, 3)))


@functools.lru_cache(None)
def work_table(call):
    lists = []
    for s in range(N_SP):
        for t in range(N_TP):
            firsts = [
                shard_first(s, t if own == 0 else 1 - t, k3, k2, kz)
                for own, k3 in CALLS[call]
                for k2 in range(4)
                for kz in range(2)
            ]
            rows = []
            for group in range(GROUPS):
                block = s if group < 2 else partner(s)
                base = 4 * block + 2 * (group % 2)
                needed = [n for n in range(len(firsts)) if firsts[n] <= base + 1]
                for at in range(0, len(needed), UNIT):
                    part = needed[at : at + UNIT]
                    segs = [firsts[n] for n in part] + [1 << 20] * (UNIT - len(part))
                    part = part + [part[-1]] * (UNIT - len(part))
                    bits = 0
                    for half in range(2):
                        for j in range(UNIT):
                            for late in range(2):
                                if segs[j] + half > base + late:
                                    bits |= 1 << ((half * UNIT + j) * 2 + late)
                    rows.append([group, bits, t] + part)
            lists.append(rows)
    count = max(len(rows) for rows in lists)
    everything = (1 << (4 * UNIT)) - 1
    idle = lambda rows, t: rows[-1][:1] + [everything] + rows[-1][2:] if rows else [0, everything, t] + [0] * UNIT
    table = []
    for n, rows in enumerate(lists):
        table.append(rows + [idle(rows, n % N_TP)] * (count + 1 - len(rows)))
    return count, np.array(table, np.int32).reshape(len(lists), -1)


NT = (((1,), (1,)), ((), ()))


def attention_body(call, steps, offset, part_count, table, *rest):
    first, last = call == 0, call == len(CALLS) - 1
    rest = list(rest)
    take = lambda n: [rest.pop(0) for _ in range(n)]
    if first:
        own_ref, own_rope_ref, received_ref, key_up_ref, cosine_ref, sine_ref = take(6)
    else:
        q4_ref, qabs, _, _, _ = take(5)
    if last:
        value_up_ref, out_proj_hbm, residual_hbm = take(3)
    parts = take(part_count)
    if last:
        home_same, home_cross, away_same, away_cross, out_proj_ref, residual_ref = take(6)
    if first:
        qabs, q4_ref = take(2)
    m_ref, l_ref, acc_ref, keys, s0, s1, p0, p1, shrink0, shrink1 = take(10)
    fetches = []
    if last:
        (sems,) = rest
        early = pl.ds(0, out_proj_ref.shape[1])
        for n, (source, target) in enumerate(((out_proj_hbm.at[:, early], out_proj_ref), (residual_hbm, residual_ref))):
            fetch = pltpu.make_async_copy(source, target, sems.at[n])
            fetch.start()
            fetches.append(fetch)
    at = 0
    for part in parts:
        for k in range(2):
            keys[k, pl.ds(at, part.shape[0]), :] = part[:, pl.ds(k * 128, 128)]
        at += part.shape[0]
    if first:
        for g in range(GROUPS):
            source = own_ref if g < 2 else received_ref
            for h in range(HEADS_HERE):
                cols = pl.ds(h * QK_NOPE, QK_NOPE)
                latent_query = lax.dot_general(
                    source[pl.ds((g % 2) * ROWS, ROWS), cols],
                    key_up_ref[:, cols],
                    NT,
                    preferred_element_type=jnp.float32,
                ).astype(jnp.bfloat16)
                for k in range(2):
                    qabs[g, k, pl.ds(h * ROWS, ROWS), :] = latent_query[:, k * 128 : (k + 1) * 128]
        lane = lax.broadcasted_iota(jnp.int32, (ROWS, 128), 1)
        for g in range(GROUPS):
            tokens = pl.ds((g % 2) * ROWS, ROWS)
            for k in range(2):
                cols = pl.ds(k * 128, 128)
                if g < 2:
                    x = own_rope_ref[tokens, cols]
                else:
                    x = received_ref[tokens, pl.ds(HEADS_HERE * QK_NOPE + k * 128, 128)]
                x = x.astype(jnp.float32)
                opposite = jnp.where(lane % QK_ROPE < QK_ROPE // 2, pltpu.roll(x, 96, 1), pltpu.roll(x, 32, 1))
                at = pl.ds(g * ROWS, ROWS)
                turned = (x * cosine_ref[at, cols] + opposite * sine_ref[at, cols]).astype(jnp.bfloat16).astype(jnp.float32)
                flipped = pltpu.roll(turned, QK_ROPE, 1)
                for odd in range(2):
                    rows = pl.ds((2 * k + odd) * ROWS, ROWS)
                    for half in range(2):
                        source = turned if odd == half else flipped
                        keep = lane < QK_ROPE if half == 0 else lane >= QK_ROPE
                        q4_ref[g, half, rows, :] = jnp.where(keep, source, 0.0).astype(jnp.bfloat16)
        m_ref[...] = jnp.full(m_ref.shape, NEG_LARGE, jnp.float32)
        l_ref[...] = jnp.zeros(l_ref.shape, jnp.float32)
        acc_ref[...] = jnp.zeros(acc_ref.shape, jnp.float32)

    cols_per_step = 3 + UNIT

    def field(u, n):
        return table[offset + u * cols_per_step + n]

    def wide(at, count):
        rows = pl.ds(pl.multiple_of(at, 32), count)
        return jnp.concatenate([keys[k, rows, :] for k in range(2)], axis=1)

    def latent_tile(u, half):
        return jnp.concatenate([wide(field(u, 3 + j) * SHARD + half * SEGMENT, SEGMENT) for j in range(UNIT)], axis=0)

    note_lane = lax.broadcasted_iota(jnp.int32, (16, 128), 1)
    mark = [jnp.where(note_lane == n, 1.0, 0.0).astype(jnp.bfloat16) for n in range(2)]
    marks = jnp.concatenate(([mark[0]] * (SEGMENT // 16) + [mark[1]] * (SEGMENT // 16)) * HEADS_HERE, axis=0)

    def scores(u, s_ref):
        g = field(u, 0)
        bits = field(u, 1)
        rot = jnp.concatenate(
            [
                keys[h, pl.ds(pl.multiple_of(field(u, 3 + j) * SHARD + ROWS, 32), 32), :]
                for j in range(UNIT)
                for h in range(2)
            ],
            axis=0,
        )
        q = jnp.concatenate([qabs[g, k] for k in range(2)], axis=1)
        for half in range(2):
            notes = []
            for j in range(UNIT):
                at = (half * UNIT + j) * 2
                early, late = (
                    jnp.where((bits >> (at + n)) & 1 == 1, jnp.float32(NEG_LARGE), jnp.float32(0.0)) for n in range(2)
                )
                note = jnp.where(note_lane == 0, early, jnp.where(note_lane == 1, late, 0.0)).astype(jnp.bfloat16)
                notes += [note] * (SEGMENT // 16)
            extra = jnp.concatenate([rot, jnp.concatenate(notes, axis=0)], axis=1)
            total = lax.dot_general(
                q, latent_tile(u, half), NT, preferred_element_type=jnp.float32
            ) + lax.dot_general(
                jnp.concatenate([q4_ref[g, half], marks], axis=1), extra, NT, preferred_element_type=jnp.float32
            )
            for k in range(2):
                s_ref[half * 2 + k, pl.ds(0, QROWS), :] = total[:, k * 128 : (k + 1) * 128]

    def absorb(u, s_ref, p_ref, shrink_ref):
        g = field(u, 0)
        for at in range(0, QROWS, CHUNK):
            rows = pl.ds(at, CHUNK)
            s = [s_ref[k, rows, :] for k in range(KEYS // 128)]
            before = m_ref[g, rows, :]
            top = jnp.maximum(jnp.maximum(s[0], s[1]), jnp.maximum(s[2], s[3]))
            after = jnp.maximum(before, jnp.max(top, axis=1, keepdims=True))
            m_ref[g, rows, :] = after
            shrink = jnp.exp2((before - after) * SCALE2)
            shrink_ref[rows, :] = shrink
            after = after * SCALE2
            partial = l_ref[g, rows, :] * shrink
            for k in range(KEYS // 128):
                p = jnp.exp2(s[k] * SCALE2 - after)
                partial = partial + p
                p_ref[k, rows, :] = p.astype(jnp.bfloat16)
            l_ref[g, rows, :] = partial
        values = jnp.concatenate([latent_tile(u, 0), latent_tile(u, 1)], axis=0)
        for at in range(0, QROWS, QROWS // 2):
            rows = pl.ds(at, QROWS // 2)
            weights = jnp.concatenate([p_ref[k, rows, :] for k in range(KEYS // 128)], axis=1)
            product = jnp.dot(weights, values, preferred_element_type=jnp.float32)
            for k in range(LATENT // 128):
                acc_ref[g, k, rows, :] = (
                    acc_ref[g, k, rows, :] * shrink_ref[rows, :] + product[:, k * 128 : (k + 1) * 128]
                )

    scores(0, s0)

    def pair(k, carry):
        u = k * 2
        scores(u + 1, s1)
        absorb(u, s0, p0, shrink0)
        scores(u + 2, s0)
        absorb(u + 1, s1, p1, shrink1)
        return carry

    lax.fori_loop(0, (steps - 1) // 2, pair, 0)
    if steps % 2 == 0:
        scores(steps - 1, s1)
        absorb(steps - 2, s0, p0, shrink0)
        absorb(steps - 1, s1, p1, shrink1)
    else:
        absorb(steps - 1, s0, p0, shrink0)
    if not last:
        return
    core = field(0, 2)
    lane = lax.broadcasted_iota(jnp.int32, (ROWS, 128), 1)
    targets = ((home_same, core), (home_cross, 1 - core), (away_same, 2 + core), (away_cross, 3 - core))
    for target, g in targets:
        total = jnp.sum(l_ref[g], axis=1, keepdims=True)
        total = jnp.where(total > 0.0, total, 1.0)
        mean = jnp.concatenate([acc_ref[g, k] / total for k in range(2)], axis=1).astype(jnp.bfloat16)
        size = m_ref[g] * SCALE2 + jnp.log2(total)
        notes = jnp.zeros((ROWS, 128), jnp.bfloat16)
        for h in range(HEADS_HERE):
            cols = pl.ds(h * V_DIM, V_DIM)
            rows = slice(h * ROWS, (h + 1) * ROWS)
            target[:, cols] = jnp.dot(
                mean[rows], value_up_ref[:, cols], preferred_element_type=jnp.float32
            ).astype(jnp.bfloat16)
            left = size[rows]
            for n in range(3):
                term = left.astype(jnp.bfloat16)
                notes = jnp.where(lane == n * HEADS_HERE + h, term, notes)
                left = left - term.astype(jnp.float32)
        target[:, pl.ds(HEADS_HERE * V_DIM, 128)] = notes
    for fetch in fetches:
        fetch.wait()


def attention(call, table, operands, parts):
    vmem = pl.BlockSpec(memory_space=pltpu.VMEM)
    hbm = pl.BlockSpec(memory_space=pltpu.HBM)
    steps = work_table(call)[0]
    offset = sum(work_table(n)[1].shape[1] for n in range(call))
    first, last = call == 0, call == len(CALLS) - 1
    outs = [
        pltpu.VMEM((GROUPS, QROWS, 128), jnp.float32),
        pltpu.VMEM((GROUPS, QROWS, 128), jnp.float32),
        pltpu.VMEM((GROUPS, 2, QROWS, 128), jnp.float32),
    ]
    specs = [vmem] * len(operands)
    scratch = []
    aliases = {}
    if first:
        outs = [pltpu.VMEM((GROUPS, 2, QROWS, 128), jnp.bfloat16)] * 2 + outs
    elif last:
        fetched = operands[-2:]
        outs = [
            *[pltpu.VMEM((ROWS, MESSAGE), jnp.bfloat16)] * 4,
            pltpu.VMEM((fetched[0].shape[0], EARLY), jnp.bfloat16),
            pltpu.VMEM(fetched[1].shape, jnp.bfloat16),
        ] + outs
        specs = specs[:-2] + [hbm] * 2
        operands = (*operands[:-2], *[in_hbm(f) for f in fetched])
        scratch = [pltpu.SemaphoreType.DMA((2,))]
    if not first:
        aliases = {3 + n: len(outs) - 3 + n for n in range(3)}
        operands = tuple(in_vmem(x) if 1 <= n < 5 else x for n, x in enumerate(operands))
    work = steps * QROWS * KEYS * 3 * LATENT * 2
    return pl.pallas_call(
        functools.partial(attention_body, call, steps, offset, len(parts)),
        out_shape=outs,
        in_specs=[pl.BlockSpec(memory_space=pltpu.SMEM)] + specs + [vmem] * len(parts),
        out_specs=[vmem] * len(outs),
        input_output_aliases=aliases,
        scratch_shapes=[
            pltpu.VMEM((2, sum(part.shape[0] for part in parts), 128), jnp.bfloat16),
            pltpu.VMEM((KEYS // 128, QROWS, 128), jnp.float32),
            pltpu.VMEM((KEYS // 128, QROWS, 128), jnp.float32),
            pltpu.VMEM((KEYS // 128, QROWS, 128), jnp.bfloat16),
            pltpu.VMEM((KEYS // 128, QROWS, 128), jnp.bfloat16),
            pltpu.VMEM((QROWS, 128), jnp.float32),
            pltpu.VMEM((QROWS, 128), jnp.float32),
        ]
        + scratch,
        cost_estimate=pl.CostEstimate(
            flops=work, bytes_accessed=2**20, transcendentals=steps * QROWS * KEYS
        ),
        compiler_params=pltpu.CompilerParams(vmem_limit_bytes=24 * 2**20),
    )(table, *operands, *[in_vmem(part) for part in parts])


def in_vmem(x):
    return pltpu.with_memory_space_constraint(x, pltpu.VMEM)


def in_hbm(x):
    return pltpu.with_memory_space_constraint(x, pltpu.HBM)


def merged(one, two):
    width = HEADS_HERE * V_DIM
    outs = []
    for h in range(HEADS_HERE):
        sizes = []
        for part in (one, two):
            notes = part[:, width : width + 128].astype(jnp.float32)
            sizes.append(
                notes[:, h : h + 1] + notes[:, HEADS_HERE + h : HEADS_HERE + h + 1]
                + notes[:, 2 * HEADS_HERE + h : 2 * HEADS_HERE + h + 1]
            )
        most = jnp.maximum(sizes[0], sizes[1])
        first, second = (jnp.exp2(size - most) for size in sizes)
        cols = slice(h * V_DIM, (h + 1) * V_DIM)
        value = first * one[:, cols].astype(jnp.float32) + second * two[:, cols].astype(jnp.float32)
        outs.append((value / (first + second)).astype(jnp.bfloat16))
    return jnp.concatenate(outs, axis=1)


PIECES = 4


def project_body(
    core, local_part, mirror_same, swapped, mirror_cross, gain, slots, residual, out_early, out_proj_hbm,
    hidden_hbm, outgoing_hbm, hidden, outgoing, out_late, out_sems, late_sem,
):
    fetch = pltpu.make_async_copy(out_proj_hbm.at[:, pl.ds(EARLY, out_late.shape[1])], out_late, late_sem)
    fetch.start()
    half = HEADS_HERE * V_DIM
    mine = merged(local_part[...], mirror_same[...])
    theirs = merged(swapped[...], mirror_cross[...])
    at = pl.multiple_of(core[0] * half, half)
    other = pl.multiple_of((1 - core[0]) * half, half)
    projected = []
    for weights in (out_early, out_late):
        if weights is out_late:
            fetch.wait()
        projected.append(
            jnp.dot(mine, weights[pl.ds(at, half), :], preferred_element_type=jnp.float32)
            + jnp.dot(theirs, weights[pl.ds(other, half), :], preferred_element_type=jnp.float32)
        )
    projected = jnp.concatenate(projected, axis=1)
    result = (residual[...].astype(jnp.float32) + projected).astype(jnp.bfloat16)
    hidden[...] = result
    store = pltpu.make_async_copy(hidden, hidden_hbm, out_sems.at[PIECES])
    store.start()
    wide = result.astype(jnp.float32)
    normed = wide * lax.rsqrt(jnp.mean(wide * wide, axis=-1, keepdims=True) + EPSILON)
    normed = (normed * gain[...]).astype(jnp.bfloat16)
    count = outgoing.shape[0] // PIECES
    stores = [store]
    for n in range(PIECES):
        slot = lax.broadcasted_iota(jnp.int32, (count, normed.shape[0]), 0) + n * count
        pick = (slot == slots[0:1, :]) | (slot == slots[1:2, :])
        pick = jnp.where(pick, 1.0, 0.0).astype(jnp.bfloat16)
        rows = pl.ds(n * count, count)
        outgoing[rows, :] = jnp.dot(pick, normed, preferred_element_type=jnp.float32).astype(jnp.bfloat16)
        store = pltpu.make_async_copy(outgoing.at[rows], outgoing_hbm.at[rows], out_sems.at[n])
        store.start()
        stores.append(store)
    for store in stores:
        store.wait()


def project(core, messages, out_early, out_proj, residual, gain, slots):
    width = residual.shape[1]
    vmem = pl.BlockSpec(memory_space=pltpu.VMEM)
    hbm = pl.BlockSpec(memory_space=pltpu.HBM)
    return pl.pallas_call(
        project_body,
        out_shape=(
            pltpu.HBM((ROWS, width), jnp.bfloat16),
            pltpu.HBM((N_SP * CAP, width), jnp.bfloat16),
        ),
        in_specs=[pl.BlockSpec(memory_space=pltpu.SMEM)] + [vmem] * 8 + [hbm],
        out_specs=(hbm, hbm),
        scratch_shapes=[
            pltpu.VMEM((ROWS, width), jnp.bfloat16),
            pltpu.VMEM((N_SP * CAP, width), jnp.bfloat16),
            pltpu.VMEM((out_proj.shape[0], width - EARLY), jnp.bfloat16),
            pltpu.SemaphoreType.DMA((PIECES + 1,)),
            pltpu.SemaphoreType.DMA,
        ],
        compiler_params=pltpu.CompilerParams(vmem_limit_bytes=16 * 2**20),
        name="project",
    )(core, *messages, gain, slots, in_vmem(residual), in_vmem(out_early), in_hbm(out_proj))


def experts_body(rows, *rest):
    sources = rest[:6]
    out_hbm = rest[6]
    weights = rest[7:13]
    first, out, sems, out_sems = rest[13:]
    loads = []
    for n in range(6):
        load = pltpu.make_async_copy(sources[n], weights[n], sems.at[n])
        load.start()
        loads.append(load)
    count = rows.shape[0]
    block = count // 2
    stores = []
    for n in range(2):
        gate, up, down = weights[3 * n : 3 * n + 3]
        loads[3 * n].wait()
        loads[3 * n + 1].wait()
        actives = []
        for k in range(2):
            x = rows[pl.ds(k * block, block), :]
            gated = jnp.dot(x, gate[...], preferred_element_type=jnp.float32)
            raised = jnp.dot(x, up[...], preferred_element_type=jnp.float32)
            actives.append((gated / (1.0 + jnp.exp(-gated)) * raised).astype(jnp.bfloat16))
        loads[3 * n + 2].wait()
        for k in range(2):
            at = pl.ds(k * block, block)
            product = jnp.dot(actives[k], down[...], preferred_element_type=jnp.float32).astype(jnp.bfloat16)
            if n == 0:
                first[at, :] = product
            else:
                out[at, :] = (first[at, :].astype(jnp.float32) + product.astype(jnp.float32)).astype(jnp.bfloat16)
                store = pltpu.make_async_copy(out.at[at], out_hbm.at[at], out_sems.at[k])
                store.start()
                stores.append(store)
    for store in stores:
        store.wait()


def experts(rows, own, other):
    count, width = rows.shape
    hbm = pl.BlockSpec(memory_space=pltpu.HBM)
    return pl.pallas_call(
        experts_body,
        out_shape=pltpu.HBM((count, width), jnp.bfloat16),
        in_specs=[pl.BlockSpec(memory_space=pltpu.VMEM)] + [hbm] * 6,
        out_specs=hbm,
        scratch_shapes=[pltpu.VMEM(w.shape, w.dtype) for w in (*own, *other)]
        + [
            pltpu.VMEM((count, width), jnp.bfloat16),
            pltpu.VMEM((count, width), jnp.bfloat16),
            pltpu.SemaphoreType.DMA((6,)),
            pltpu.SemaphoreType.DMA((2,)),
        ],
        compiler_params=pltpu.CompilerParams(vmem_limit_bytes=28 * 2**20),
        name="experts",
    )(rows, *[in_hbm(w) for w in (*own, *other)])


def combine_body(back, hidden, slots, weights, out_ref):
    slot = lax.broadcasted_iota(jnp.int32, (hidden.shape[0], back.shape[0]), 1)
    pick = jnp.where(slot == slots[:, 0:1], weights[:, 0:1], 0.0) + jnp.where(
        slot == slots[:, 1:2], weights[:, 1:2], 0.0
    )
    high = pick.astype(jnp.bfloat16)
    low = (pick - high.astype(jnp.float32)).astype(jnp.bfloat16)
    rows = back[...]
    mixed = jnp.dot(high, rows, preferred_element_type=jnp.float32) + jnp.dot(
        low, rows, preferred_element_type=jnp.float32
    )
    out_ref[...] = (hidden[...].astype(jnp.float32) + mixed).astype(jnp.bfloat16)


def combine(back, hidden, slots, weights):
    vmem = pl.BlockSpec(memory_space=pltpu.VMEM)
    return pl.pallas_call(
        combine_body,
        out_shape=jax.ShapeDtypeStruct(hidden.shape, jnp.bfloat16),
        in_specs=[vmem] * 4,
        out_specs=vmem,
        compiler_params=pltpu.CompilerParams(vmem_limit_bytes=16 * 2**20),
        name="combine",
    )(back, hidden, slots, weights)


def rotary(values, positions):
    half_width = values.shape[-1] // 2
    inverse = ROPE_BASE ** (-2.0 * jnp.arange(half_width, dtype=jnp.float32) / values.shape[-1])
    angles = positions.astype(jnp.float32)[:, None] * inverse[None, :]
    cosine = jnp.cos(angles)
    sine_part = jnp.sin(angles)
    if values.ndim == 3:
        cosine = cosine[:, None, :]
        sine_part = sine_part[:, None, :]
    first_half = values[..., :half_width]
    second = values[..., half_width:]
    return jnp.concatenate(
        [first_half * cosine - second * sine_part, second * cosine + first_half * sine_part],
        axis=-1,
    )


def local(
    residual,
    query_nope,
    query_rope,
    latent,
    key_rope,
    key_up,
    value_up,
    out_proj,
    norm_gain,
    routes,
    route_weight,
    w_gate,
    w_up,
    w_down,
):
    tp_index = lax.axis_index("tp")
    sp_index = lax.axis_index("sp")
    tok_dev = query_nope.shape[0]
    query_first = sp_index * tok_dev
    swap = [(0, 1), (1, 0)]

    key_pos = query_first + tp_index * ROWS + jnp.arange(ROWS, dtype=jnp.int32)
    key_rot = rotary(key_rope.astype(jnp.float32), key_pos).astype(jnp.bfloat16)
    packed = jnp.concatenate([key_rot[0:32], key_rot[64:96], key_rot[32:64], key_rot[96:128]], axis=1)
    shard = jnp.concatenate([latent, packed], axis=0)
    mirror = [
        (s * N_TP + t, partner(s) * N_TP + t) for s in range(N_SP) for t in range(N_TP)
    ]
    crossing = [
        (s * N_TP + t, partner(s) * N_TP + 1 - t) for s in range(N_SP) for t in range(N_TP)
    ]
    queries = jnp.concatenate([query_nope, query_rope], axis=1)
    received = lax.ppermute(queries, AXES, mirror)

    near = lax.ppermute(shard, AXES, plane_pairs(Z_FIRST))
    far = lax.ppermute(shard, AXES, plane_pairs(Z_SECOND))
    main = (tp_index == 0) == (sp_index < 2 * PLANE)
    both = jnp.concatenate([jnp.where(main, shard, far), near], axis=0)
    flat = routes.reshape(-1)
    order = jnp.arange(flat.shape[0], dtype=jnp.int32)
    earlier = (flat[:, None] == flat[None, :]) & (order[None, :] < order[:, None])
    rank = jnp.sum(earlier.astype(jnp.int32), axis=1)
    slots = (flat * CAP + rank).reshape(routes.shape)
    slots_across = slots.T
    tables = np.concatenate([work_table(call)[1] for call in range(len(CALLS))], axis=1)
    table = lax.dynamic_index_in_dim(jnp.asarray(tables), sp_index * N_TP + tp_index, 0, keepdims=False)
    tokens = jnp.arange(tok_dev, dtype=jnp.int32)
    query_pos = jnp.concatenate([query_first + tokens, partner(sp_index) * tok_dev + tokens])
    half_width = QK_ROPE // 2
    pair = jnp.arange(HEADS_HERE * QK_ROPE, dtype=jnp.int32) % half_width
    inverse = ROPE_BASE ** (-2.0 * pair.astype(jnp.float32) / QK_ROPE)
    angles = query_pos.astype(jnp.float32)[:, None] * inverse[None, :]
    behind = jnp.arange(HEADS_HERE * QK_ROPE, dtype=jnp.int32) % QK_ROPE >= half_width
    cosine = jnp.cos(angles)
    sine = jnp.where(behind[None, :], jnp.sin(angles), -jnp.sin(angles))
    got = [both]
    for by in SHIFTS[1:]:
        got.append(lax.ppermute(both, AXES, shift_pairs(0, by)))
    both = jnp.concatenate(got, axis=0)
    both, table, slots, slots_across, cosine, sine = lax.optimization_barrier(
        (both, table, slots, slots_across, cosine, sine)
    )
    around = []
    for by in (1, -1):
        around.append(lax.ppermute(both, AXES, shift_pairs(1, by)))
    half = both.shape[0] // 2
    beyond = []
    for n, by in enumerate((1, -1)):
        passed = around[n][n * half : (n + 1) * half]
        beyond.append(lax.ppermute(passed, AXES, shift_pairs(1, by)))
    own_parts = [[both], [around[0]], [around[1]], beyond]
    other_parts = []
    for group in own_parts:
        other_parts.append([lax.ppermute(part, "tp", swap) for part in group])
    pieces = (own_parts, other_parts)
    state = ()
    for call in range(len(CALLS)):
        operands = (
            (query_nope, query_rope, received, key_up, cosine, sine) if call == 0 else (q4, qabs, *state)
        )
        if call == len(CALLS) - 1:
            operands = (*operands, value_up, out_proj, residual)
        state = attention(call, table, operands, [part for own, k3 in CALLS[call] for part in pieces[own][k3]])
        if call == 0:
            qabs, q4, *state = state
    home_same, home_cross, away_same, away_cross, out_early, residual = state[:6]
    mirror_same = lax.ppermute(away_same, AXES, mirror)
    mirror_cross = lax.ppermute(away_cross, AXES, crossing)
    swapped = lax.ppermute(home_cross, "tp", swap)
    messages = (home_same, mirror_same, swapped, mirror_cross)

    hidden, outgoing = project(
        tp_index.reshape(1).astype(jnp.int32), messages, out_early, out_proj, residual, norm_gain[None, :], slots_across
    )
    width = residual.shape[1]
    arrived = lax.all_to_all(
        outgoing.reshape(N_SP, CAP, width), "sp", split_axis=0, concat_axis=0, tiled=True
    ).reshape(N_SP * CAP, width)
    own_weights = (w_gate[0], w_up[0], w_down[0])
    other_weights = [lax.ppermute(w, "tp", swap) for w in own_weights]
    produced = experts(arrived, own_weights, other_weights)
    back = lax.all_to_all(
        produced.reshape(N_SP, CAP, width), "sp", split_axis=0, concat_axis=0, tiled=True
    ).reshape(N_SP * CAP, width)
    return combine(back, hidden, slots, route_weight)


def solution(mesh):
    return jax.shard_map(
        local,
        mesh=mesh,
        in_specs=(
            P(("sp", "tp"), None),
            P("sp", "tp"),
            P("sp", "tp"),
            P(("sp", "tp"), None),
            P(("sp", "tp"), None),
            P(None, "tp"),
            P(None, "tp"),
            P(),
            P(),
            P(("sp", "tp"), None),
            P(("sp", "tp"), None),
            P("sp", None, "tp"),
            P("sp", None, "tp"),
            P("sp", "tp", None),
        ),
        out_specs=P(("sp", "tp"), None),
        check_vma=False,
    )
```

```python
import functools
import jax
import jax.numpy as jnp
import numpy as np
from jax import lax
from jax.experimental import pallas as pl
from jax.experimental.pallas import tpu as pltpu
from jax.sharding import PartitionSpec as P

QK_NOPE = 128
QK_ROPE = 64
V_DIM = 128
LATENT = 256
SEGMENT = 64
EPSILON = 1e-06
ROPE_BASE = 10000.0
NEG_LARGE = -1e30

N_SP = 64
N_TP = 2
HEADS_HERE = 4
ROWS = 128
SHARD = 160
UNIT = 4
KEYS = UNIT * ROWS
QROWS = HEADS_HERE * ROWS
CAP = 8
AXES = ("sp", "tp")
STEP = {"x": 1, "y": 4, "z": 16}
Z_FIRST = {(0, 0): (3, 0), (1, 0): (2, 0), (0, 1): (1, 0), (1, 1): (0, 0), (2, 1): (1, 1), (3, 1): (0, 1), (2, 0): (3, 1), (3, 0): (2, 1)}
Z_SECOND = {(0, 1): (2, 0), (1, 1): (3, 0), (2, 0): (0, 1), (3, 0): (1, 1)}
ORDER = (("y", "x"), ("x", "y"))
SHIFTS = (0, 1, -1, 2)
SCALE2 = float((QK_NOPE + QK_ROPE) ** (-0.5) * np.log2(np.e))
PLANE = 16
GROUPS = 4
CHUNK = 64
MESSAGE = HEADS_HERE * V_DIM + 128
EARLY = 1024


def moved(s, dim, by):
    step = STEP[dim]
    c = (s // step) % 4
    return s + step * ((c + by) % 4 - c)


def shift_pairs(phase, by):
    return [
        (s * N_TP + t, moved(s, ORDER[t][phase], by) * N_TP + t)
        for s in range(N_SP)
        for t in range(N_TP)
    ]


def partner(s):
    z, y, x = s // 16, (s // 4) % 4, s % 4
    return (3 - z) * 16 + (3 - y) * 4 + x


def shard_source(s, t, k2, kz):
    s = moved(s, ORDER[t][0], -SHIFTS[k2])
    z, r = divmod(s, PLANE)
    source = (z, t)
    if kz == 1:
        source = Z_FIRST[source]
    elif source in Z_SECOND:
        source = Z_SECOND[source]
    return source[0] * PLANE + r, source[1]


def plane_pairs(table):
    return [
        ((from_z * PLANE + r) * N_TP + from_core, (z * PLANE + r) * N_TP + core)
        for (z, core), (from_z, from_core) in table.items()
        for r in range(PLANE)
    ]


def shard_first(s, t, k3, k2, kz):
    chip, core = shard_source(moved(s, ORDER[t][1], -SHIFTS[k3]), t, k2, kz)
    return 4 * chip + 2 * core


CALLS = (((0, 0), (1, 0)), ((0, 1), (0, 2)), ((1, 1), (1, 2)), ((0, 3), (1, 3)))


@functools.lru_cache(None)
def work_table(call):
    lists = []
    for s in range(N_SP):
        for t in range(N_TP):
            firsts = [
                shard_first(s, t if own == 0 else 1 - t, k3, k2, kz)
                for own, k3 in CALLS[call]
                for k2 in range(4)
                for kz in range(2)
            ]
            rows = []
            for group in range(GROUPS):
                block = s if group < 2 else partner(s)
                base = 4 * block + 2 * (group % 2)
                needed = [n for n in range(len(firsts)) if firsts[n] <= base + 1]
                for at in range(0, len(needed), UNIT):
                    part = needed[at : at + UNIT]
                    segs = [firsts[n] for n in part] + [1 << 20] * (UNIT - len(part))
                    part = part + [part[-1]] * (UNIT - len(part))
                    bits = 0
                    for half in range(2):
                        for j in range(UNIT):
                            for late in range(2):
                                if segs[j] + half > base + late:
                                    bits |= 1 << ((half * UNIT + j) * 2 + late)
                    rows.append([group, bits, t] + part)
            lists.append(rows)
    count = max(len(rows) for rows in lists)
    everything = (1 << (4 * UNIT)) - 1
    idle = lambda rows, t: rows[-1][:1] + [everything] + rows[-1][2:] if rows else [0, everything, t] + [0] * UNIT
    table = []
    for n, rows in enumerate(lists):
        table.append(rows + [idle(rows, n % N_TP)] * (count + 1 - len(rows)))
    return count, np.array(table, np.int32).reshape(len(lists), -1)


NT = (((1,), (1,)), ((), ()))


def attention_body(call, steps, offset, part_count, table, *rest):
    first, last = call == 0, call == len(CALLS) - 1
    rest = list(rest)
    take = lambda n: [rest.pop(0) for _ in range(n)]
    if first:
        own_ref, own_rope_ref, received_ref, key_up_ref, cosine_ref, sine_ref = take(6)
    else:
        q4_ref, qabs, _, _, _ = take(5)
    if last:
        value_up_ref, out_proj_hbm, residual_hbm = take(3)
    parts = take(part_count)
    if last:
        home_same, home_cross, away_same, away_cross, out_proj_ref, residual_ref = take(6)
    if first:
        qabs, q4_ref = take(2)
    m_ref, l_ref, acc_ref, keys, s0, s1, p0, p1, shrink0, shrink1 = take(10)
    fetches = []
    if last:
        (sems,) = rest
        early = pl.ds(0, out_proj_ref.shape[1])
        for n, (source, target) in enumerate(((out_proj_hbm.at[:, early], out_proj_ref), (residual_hbm, residual_ref))):
            fetch = pltpu.make_async_copy(source, target, sems.at[n])
            fetch.start()
            fetches.append(fetch)
    at = 0
    for part in parts:
        for k in range(2):
            keys[k, pl.ds(at, part.shape[0]), :] = part[:, pl.ds(k * 128, 128)]
        at += part.shape[0]
    if first:
        for g in range(GROUPS):
            source = own_ref if g < 2 else received_ref
            for h in range(HEADS_HERE):
                cols = pl.ds(h * QK_NOPE, QK_NOPE)
                latent_query = lax.dot_general(
                    source[pl.ds((g % 2) * ROWS, ROWS), cols],
                    key_up_ref[:, cols],
                    NT,
                    preferred_element_type=jnp.float32,
                ).astype(jnp.bfloat16)
                for k in range(2):
                    qabs[g, k, pl.ds(h * ROWS, ROWS), :] = latent_query[:, k * 128 : (k + 1) * 128]
        lane = lax.broadcasted_iota(jnp.int32, (ROWS, 128), 1)
        for g in range(GROUPS):
            tokens = pl.ds((g % 2) * ROWS, ROWS)
            for k in range(2):
                cols = pl.ds(k * 128, 128)
                if g < 2:
                    x = own_rope_ref[tokens, cols]
                else:
                    x = received_ref[tokens, pl.ds(HEADS_HERE * QK_NOPE + k * 128, 128)]
                x = x.astype(jnp.float32)
                opposite = jnp.where(lane % QK_ROPE < QK_ROPE // 2, pltpu.roll(x, 96, 1), pltpu.roll(x, 32, 1))
                at = pl.ds(g * ROWS, ROWS)
                turned = (x * cosine_ref[at, cols] + opposite * sine_ref[at, cols]).astype(jnp.bfloat16).astype(jnp.float32)
                flipped = pltpu.roll(turned, QK_ROPE, 1)
                for odd in range(2):
                    rows = pl.ds((2 * k + odd) * ROWS, ROWS)
                    for half in range(2):
                        source = turned if odd == half else flipped
                        keep = lane < QK_ROPE if half == 0 else lane >= QK_ROPE
                        q4_ref[g, half, rows, :] = jnp.where(keep, source, 0.0).astype(jnp.bfloat16)
        m_ref[...] = jnp.full(m_ref.shape, NEG_LARGE, jnp.float32)
        l_ref[...] = jnp.zeros(l_ref.shape, jnp.float32)
        acc_ref[...] = jnp.zeros(acc_ref.shape, jnp.float32)

    cols_per_step = 3 + UNIT

    def field(u, n):
        return table[offset + u * cols_per_step + n]

    def wide(at, count):
        rows = pl.ds(pl.multiple_of(at, 32), count)
        return jnp.concatenate([keys[k, rows, :] for k in range(2)], axis=1)

    def latent_tile(u, half):
        return jnp.concatenate([wide(field(u, 3 + j) * SHARD + half * SEGMENT, SEGMENT) for j in range(UNIT)], axis=0)

    note_lane = lax.broadcasted_iota(jnp.int32, (16, 128), 1)
    mark = [jnp.where(note_lane == n, 1.0, 0.0).astype(jnp.bfloat16) for n in range(2)]
    marks = jnp.concatenate(([mark[0]] * (SEGMENT // 16) + [mark[1]] * (SEGMENT // 16)) * HEADS_HERE, axis=0)

    def scores(u, s_ref):
        g = field(u, 0)
        bits = field(u, 1)
        rot = jnp.concatenate(
            [
                keys[h, pl.ds(pl.multiple_of(field(u, 3 + j) * SHARD + ROWS, 32), 32), :]
                for j in range(UNIT)
                for h in range(2)
            ],
            axis=0,
        )
        q = jnp.concatenate([qabs[g, k] for k in range(2)], axis=1)
        for half in range(2):
            notes = []
            for j in range(UNIT):
                at = (half * UNIT + j) * 2
                early, late = (
                    jnp.where((bits >> (at + n)) & 1 == 1, jnp.float32(NEG_LARGE), jnp.float32(0.0)) for n in range(2)
                )
                note = jnp.where(note_lane == 0, early, jnp.where(note_lane == 1, late, 0.0)).astype(jnp.bfloat16)
                notes += [note] * (SEGMENT // 16)
            extra = jnp.concatenate([rot, jnp.concatenate(notes, axis=0)], axis=1)
            total = lax.dot_general(
                q, latent_tile(u, half), NT, preferred_element_type=jnp.float32
            ) + lax.dot_general(
                jnp.concatenate([q4_ref[g, half], marks], axis=1), extra, NT, preferred_element_type=jnp.float32
            )
            for k in range(2):
                s_ref[half * 2 + k, pl.ds(0, QROWS), :] = total[:, k * 128 : (k + 1) * 128]

    def absorb(u, s_ref, p_ref, shrink_ref):
        g = field(u, 0)
        for at in range(0, QROWS, CHUNK):
            rows = pl.ds(at, CHUNK)
            s = [s_ref[k, rows, :] for k in range(KEYS // 128)]
            before = m_ref[g, rows, :]
            top = jnp.maximum(jnp.maximum(s[0], s[1]), jnp.maximum(s[2], s[3]))
            after = jnp.maximum(before, jnp.max(top, axis=1, keepdims=True))
            m_ref[g, rows, :] = after
            shrink = jnp.exp2((before - after) * SCALE2)
            shrink_ref[rows, :] = shrink
            after = after * SCALE2
            partial = l_ref[g, rows, :] * shrink
            for k in range(KEYS // 128):
                p = jnp.exp2(s[k] * SCALE2 - after)
                partial = partial + p
                p_ref[k, rows, :] = p.astype(jnp.bfloat16)
            l_ref[g, rows, :] = partial
        values = jnp.concatenate([latent_tile(u, 0), latent_tile(u, 1)], axis=0)
        for at in range(0, QROWS, QROWS // 2):
            rows = pl.ds(at, QROWS // 2)
            weights = jnp.concatenate([p_ref[k, rows, :] for k in range(KEYS // 128)], axis=1)
            product = jnp.dot(weights, values, preferred_element_type=jnp.float32)
            for k in range(LATENT // 128):
                acc_ref[g, k, rows, :] = (
                    acc_ref[g, k, rows, :] * shrink_ref[rows, :] + product[:, k * 128 : (k + 1) * 128]
                )

    scores(0, s0)

    def pair(k, carry):
        u = k * 2
        scores(u + 1, s1)
        absorb(u, s0, p0, shrink0)
        scores(u + 2, s0)
        absorb(u + 1, s1, p1, shrink1)
        return carry

    lax.fori_loop(0, (steps - 1) // 2, pair, 0)
    if steps % 2 == 0:
        scores(steps - 1, s1)
        absorb(steps - 2, s0, p0, shrink0)
        absorb(steps - 1, s1, p1, shrink1)
    else:
        absorb(steps - 1, s0, p0, shrink0)
    if not last:
        return
    core = field(0, 2)
    lane = lax.broadcasted_iota(jnp.int32, (ROWS, 128), 1)
    targets = ((home_same, core), (home_cross, 1 - core), (away_same, 2 + core), (away_cross, 3 - core))
    for target, g in targets:
        total = jnp.sum(l_ref[g], axis=1, keepdims=True)
        total = jnp.where(total > 0.0, total, 1.0)
        mean = jnp.concatenate([acc_ref[g, k] / total for k in range(2)], axis=1).astype(jnp.bfloat16)
        size = m_ref[g] * SCALE2 + jnp.log2(total)
        notes = jnp.zeros((ROWS, 128), jnp.bfloat16)
        for h in range(HEADS_HERE):
            cols = pl.ds(h * V_DIM, V_DIM)
            rows = slice(h * ROWS, (h + 1) * ROWS)
            target[:, cols] = jnp.dot(
                mean[rows], value_up_ref[:, cols], preferred_element_type=jnp.float32
            ).astype(jnp.bfloat16)
            left = size[rows]
            for n in range(3):
                term = left.astype(jnp.bfloat16)
                notes = jnp.where(lane == n * HEADS_HERE + h, term, notes)
                left = left - term.astype(jnp.float32)
        target[:, pl.ds(HEADS_HERE * V_DIM, 128)] = notes
    for fetch in fetches:
        fetch.wait()


def attention(call, table, operands, parts):
    vmem = pl.BlockSpec(memory_space=pltpu.VMEM)
    hbm = pl.BlockSpec(memory_space=pltpu.HBM)
    steps = work_table(call)[0]
    offset = sum(work_table(n)[1].shape[1] for n in range(call))
    first, last = call == 0, call == len(CALLS) - 1
    outs = [
        pltpu.VMEM((GROUPS, QROWS, 128), jnp.float32),
        pltpu.VMEM((GROUPS, QROWS, 128), jnp.float32),
        pltpu.VMEM((GROUPS, 2, QROWS, 128), jnp.float32),
    ]
    specs = [vmem] * len(operands)
    scratch = []
    aliases = {}
    if first:
        outs = [pltpu.VMEM((GROUPS, 2, QROWS, 128), jnp.bfloat16)] * 2 + outs
    elif last:
        fetched = operands[-2:]
        outs = [
            *[pltpu.VMEM((ROWS, MESSAGE), jnp.bfloat16)] * 4,
            pltpu.VMEM((fetched[0].shape[0], EARLY), jnp.bfloat16),
            pltpu.VMEM(fetched[1].shape, jnp.bfloat16),
        ] + outs
        specs = specs[:-2] + [hbm] * 2
        operands = (*operands[:-2], *[in_hbm(f) for f in fetched])
        scratch = [pltpu.SemaphoreType.DMA((2,))]
    if not first:
        aliases = {3 + n: len(outs) - 3 + n for n in range(3)}
        operands = tuple(in_vmem(x) if 1 <= n < 5 else x for n, x in enumerate(operands))
    work = steps * QROWS * KEYS * 3 * LATENT * 2
    return pl.pallas_call(
        functools.partial(attention_body, call, steps, offset, len(parts)),
        out_shape=outs,
        in_specs=[pl.BlockSpec(memory_space=pltpu.SMEM)] + specs + [vmem] * len(parts),
        out_specs=[vmem] * len(outs),
        input_output_aliases=aliases,
        scratch_shapes=[
            pltpu.VMEM((2, sum(part.shape[0] for part in parts), 128), jnp.bfloat16),
            pltpu.VMEM((KEYS // 128, QROWS, 128), jnp.float32),
            pltpu.VMEM((KEYS // 128, QROWS, 128), jnp.float32),
            pltpu.VMEM((KEYS // 128, QROWS, 128), jnp.bfloat16),
            pltpu.VMEM((KEYS // 128, QROWS, 128), jnp.bfloat16),
            pltpu.VMEM((QROWS, 128), jnp.float32),
            pltpu.VMEM((QROWS, 128), jnp.float32),
        ]
        + scratch,
        cost_estimate=pl.CostEstimate(
            flops=work, bytes_accessed=2**20, transcendentals=steps * QROWS * KEYS
        ),
        compiler_params=pltpu.CompilerParams(vmem_limit_bytes=24 * 2**20),
    )(table, *operands, *[in_vmem(part) for part in parts])


def in_vmem(x):
    return pltpu.with_memory_space_constraint(x, pltpu.VMEM)


def in_hbm(x):
    return pltpu.with_memory_space_constraint(x, pltpu.HBM)


def merged(one, two):
    width = HEADS_HERE * V_DIM
    outs = []
    for h in range(HEADS_HERE):
        sizes = []
        for part in (one, two):
            notes = part[:, width : width + 128].astype(jnp.float32)
            sizes.append(
                notes[:, h : h + 1] + notes[:, HEADS_HERE + h : HEADS_HERE + h + 1]
                + notes[:, 2 * HEADS_HERE + h : 2 * HEADS_HERE + h + 1]
            )
        most = jnp.maximum(sizes[0], sizes[1])
        first, second = (jnp.exp2(size - most) for size in sizes)
        cols = slice(h * V_DIM, (h + 1) * V_DIM)
        value = first * one[:, cols].astype(jnp.float32) + second * two[:, cols].astype(jnp.float32)
        outs.append((value / (first + second)).astype(jnp.bfloat16))
    return jnp.concatenate(outs, axis=1)


PIECES = 4


def project_body(
    core, local_part, mirror_same, swapped, mirror_cross, gain, slots, residual, out_early, out_proj_hbm,
    hidden_hbm, outgoing_hbm, hidden, outgoing, out_late, out_sems, late_sem,
):
    fetch = pltpu.make_async_copy(out_proj_hbm.at[:, pl.ds(EARLY, out_late.shape[1])], out_late, late_sem)
    fetch.start()
    half = HEADS_HERE * V_DIM
    mine = merged(local_part[...], mirror_same[...])
    theirs = merged(swapped[...], mirror_cross[...])
    at = pl.multiple_of(core[0] * half, half)
    other = pl.multiple_of((1 - core[0]) * half, half)
    projected = []
    for weights in (out_early, out_late):
        if weights is out_late:
            fetch.wait()
        projected.append(
            jnp.dot(mine, weights[pl.ds(at, half), :], preferred_element_type=jnp.float32)
            + jnp.dot(theirs, weights[pl.ds(other, half), :], preferred_element_type=jnp.float32)
        )
    projected = jnp.concatenate(projected, axis=1)
    result = (residual[...].astype(jnp.float32) + projected).astype(jnp.bfloat16)
    hidden[...] = result
    store = pltpu.make_async_copy(hidden, hidden_hbm, out_sems.at[PIECES])
    store.start()
    wide = result.astype(jnp.float32)
    normed = wide * lax.rsqrt(jnp.mean(wide * wide, axis=-1, keepdims=True) + EPSILON)
    normed = (normed * gain[...]).astype(jnp.bfloat16)
    count = outgoing.shape[0] // PIECES
    stores = [store]
    for n in range(PIECES):
        slot = lax.broadcasted_iota(jnp.int32, (count, normed.shape[0]), 0) + n * count
        pick = (slot == slots[0:1, :]) | (slot == slots[1:2, :])
        pick = jnp.where(pick, 1.0, 0.0).astype(jnp.bfloat16)
        rows = pl.ds(n * count, count)
        outgoing[rows, :] = jnp.dot(pick, normed, preferred_element_type=jnp.float32).astype(jnp.bfloat16)
        store = pltpu.make_async_copy(outgoing.at[rows], outgoing_hbm.at[rows], out_sems.at[n])
        store.start()
        stores.append(store)
    for store in stores:
        store.wait()


def project(core, messages, out_early, out_proj, residual, gain, slots):
    width = residual.shape[1]
    vmem = pl.BlockSpec(memory_space=pltpu.VMEM)
    hbm = pl.BlockSpec(memory_space=pltpu.HBM)
    return pl.pallas_call(
        project_body,
        out_shape=(
            pltpu.HBM((ROWS, width), jnp.bfloat16),
            pltpu.HBM((N_SP * CAP, width), jnp.bfloat16),
        ),
        in_specs=[pl.BlockSpec(memory_space=pltpu.SMEM)] + [vmem] * 8 + [hbm],
        out_specs=(hbm, hbm),
        scratch_shapes=[
            pltpu.VMEM((ROWS, width), jnp.bfloat16),
            pltpu.VMEM((N_SP * CAP, width), jnp.bfloat16),
            pltpu.VMEM((out_proj.shape[0], width - EARLY), jnp.bfloat16),
            pltpu.SemaphoreType.DMA((PIECES + 1,)),
            pltpu.SemaphoreType.DMA,
        ],
        compiler_params=pltpu.CompilerParams(vmem_limit_bytes=16 * 2**20),
        name="project",
    )(core, *messages, gain, slots, in_vmem(residual), in_vmem(out_early), in_hbm(out_proj))


def experts_body(rows, *rest):
    sources = rest[:6]
    out_hbm = rest[6]
    weights = rest[7:13]
    first, out, sems, out_sems = rest[13:]
    loads = []
    for n in range(6):
        load = pltpu.make_async_copy(sources[n], weights[n], sems.at[n])
        load.start()
        loads.append(load)
    count = rows.shape[0]
    block = count // 2
    stores = []
    for n in range(2):
        gate, up, down = weights[3 * n : 3 * n + 3]
        parts = []
        for weight, load in ((gate, loads[3 * n]), (up, loads[3 * n + 1])):
            load.wait()
            parts.append(
                [
                    jnp.dot(rows[pl.ds(k * block, block), :], weight[...], preferred_element_type=jnp.float32)
                    for k in range(2)
                ]
            )
        actives = [
            (gated / (1.0 + jnp.exp(-gated)) * raised).astype(jnp.bfloat16) for gated, raised in zip(*parts)
        ]
        loads[3 * n + 2].wait()
        for k in range(2):
            at = pl.ds(k * block, block)
            product = jnp.dot(actives[k], down[...], preferred_element_type=jnp.float32).astype(jnp.bfloat16)
            if n == 0:
                first[at, :] = product
            else:
                out[at, :] = (first[at, :].astype(jnp.float32) + product.astype(jnp.float32)).astype(jnp.bfloat16)
                store = pltpu.make_async_copy(out.at[at], out_hbm.at[at], out_sems.at[k])
                store.start()
                stores.append(store)
    for store in stores:
        store.wait()


def experts(rows, own, other):
    count, width = rows.shape
    hbm = pl.BlockSpec(memory_space=pltpu.HBM)
    return pl.pallas_call(
        experts_body,
        out_shape=pltpu.HBM((count, width), jnp.bfloat16),
        in_specs=[pl.BlockSpec(memory_space=pltpu.VMEM)] + [hbm] * 6,
        out_specs=hbm,
        scratch_shapes=[pltpu.VMEM(w.shape, w.dtype) for w in (*own, *other)]
        + [
            pltpu.VMEM((count, width), jnp.bfloat16),
            pltpu.VMEM((count, width), jnp.bfloat16),
            pltpu.SemaphoreType.DMA((6,)),
            pltpu.SemaphoreType.DMA((2,)),
        ],
        compiler_params=pltpu.CompilerParams(vmem_limit_bytes=28 * 2**20),
        name="experts",
    )(rows, *[in_hbm(w) for w in (*own, *other)])


def combine_body(back, hidden, slots, weights, out_ref):
    slot = lax.broadcasted_iota(jnp.int32, (hidden.shape[0], back.shape[0]), 1)
    pick = jnp.where(slot == slots[:, 0:1], weights[:, 0:1], 0.0) + jnp.where(
        slot == slots[:, 1:2], weights[:, 1:2], 0.0
    )
    high = pick.astype(jnp.bfloat16)
    low = (pick - high.astype(jnp.float32)).astype(jnp.bfloat16)
    rows = back[...]
    mixed = jnp.dot(high, rows, preferred_element_type=jnp.float32) + jnp.dot(
        low, rows, preferred_element_type=jnp.float32
    )
    out_ref[...] = (hidden[...].astype(jnp.float32) + mixed).astype(jnp.bfloat16)


def combine(back, hidden, slots, weights):
    vmem = pl.BlockSpec(memory_space=pltpu.VMEM)
    return pl.pallas_call(
        combine_body,
        out_shape=jax.ShapeDtypeStruct(hidden.shape, jnp.bfloat16),
        in_specs=[vmem] * 4,
        out_specs=vmem,
        compiler_params=pltpu.CompilerParams(vmem_limit_bytes=16 * 2**20),
        name="combine",
    )(back, hidden, slots, weights)


def rotary(values, positions):
    half_width = values.shape[-1] // 2
    inverse = ROPE_BASE ** (-2.0 * jnp.arange(half_width, dtype=jnp.float32) / values.shape[-1])
    angles = positions.astype(jnp.float32)[:, None] * inverse[None, :]
    cosine = jnp.cos(angles)
    sine_part = jnp.sin(angles)
    if values.ndim == 3:
        cosine = cosine[:, None, :]
        sine_part = sine_part[:, None, :]
    first_half = values[..., :half_width]
    second = values[..., half_width:]
    return jnp.concatenate(
        [first_half * cosine - second * sine_part, second * cosine + first_half * sine_part],
        axis=-1,
    )


def local(
    residual,
    query_nope,
    query_rope,
    latent,
    key_rope,
    key_up,
    value_up,
    out_proj,
    norm_gain,
    routes,
    route_weight,
    w_gate,
    w_up,
    w_down,
):
    tp_index = lax.axis_index("tp")
    sp_index = lax.axis_index("sp")
    tok_dev = query_nope.shape[0]
    query_first = sp_index * tok_dev
    swap = [(0, 1), (1, 0)]

    key_pos = query_first + tp_index * ROWS + jnp.arange(ROWS, dtype=jnp.int32)
    key_rot = rotary(key_rope.astype(jnp.float32), key_pos).astype(jnp.bfloat16)
    packed = jnp.concatenate([key_rot[0:32], key_rot[64:96], key_rot[32:64], key_rot[96:128]], axis=1)
    shard = jnp.concatenate([latent, packed], axis=0)
    mirror = [
        (s * N_TP + t, partner(s) * N_TP + t) for s in range(N_SP) for t in range(N_TP)
    ]
    crossing = [
        (s * N_TP + t, partner(s) * N_TP + 1 - t) for s in range(N_SP) for t in range(N_TP)
    ]
    queries = jnp.concatenate([query_nope, query_rope], axis=1)
    received = lax.ppermute(queries, AXES, mirror)

    near = lax.ppermute(shard, AXES, plane_pairs(Z_FIRST))
    far = lax.ppermute(shard, AXES, plane_pairs(Z_SECOND))
    main = (tp_index == 0) == (sp_index < 2 * PLANE)
    both = jnp.concatenate([jnp.where(main, shard, far), near], axis=0)
    flat = routes.reshape(-1)
    order = jnp.arange(flat.shape[0], dtype=jnp.int32)
    earlier = (flat[:, None] == flat[None, :]) & (order[None, :] < order[:, None])
    rank = jnp.sum(earlier.astype(jnp.int32), axis=1)
    slots = (flat * CAP + rank).reshape(routes.shape)
    slots_across = slots.T
    tables = np.concatenate([work_table(call)[1] for call in range(len(CALLS))], axis=1)
    table = lax.dynamic_index_in_dim(jnp.asarray(tables), sp_index * N_TP + tp_index, 0, keepdims=False)
    tokens = jnp.arange(tok_dev, dtype=jnp.int32)
    query_pos = jnp.concatenate([query_first + tokens, partner(sp_index) * tok_dev + tokens])
    half_width = QK_ROPE // 2
    pair = jnp.arange(HEADS_HERE * QK_ROPE, dtype=jnp.int32) % half_width
    inverse = ROPE_BASE ** (-2.0 * pair.astype(jnp.float32) / QK_ROPE)
    angles = query_pos.astype(jnp.float32)[:, None] * inverse[None, :]
    behind = jnp.arange(HEADS_HERE * QK_ROPE, dtype=jnp.int32) % QK_ROPE >= half_width
    cosine = jnp.cos(angles)
    sine = jnp.where(behind[None, :], jnp.sin(angles), -jnp.sin(angles))
    got = [both]
    for by in SHIFTS[1:]:
        got.append(lax.ppermute(both, AXES, shift_pairs(0, by)))
    both = jnp.concatenate(got, axis=0)
    both, table, slots, slots_across, cosine, sine = lax.optimization_barrier(
        (both, table, slots, slots_across, cosine, sine)
    )
    around = []
    for by in (1, -1):
        around.append(lax.ppermute(both, AXES, shift_pairs(1, by)))
    half = both.shape[0] // 2
    beyond = []
    for n, by in enumerate((1, -1)):
        passed = around[n][n * half : (n + 1) * half]
        beyond.append(lax.ppermute(passed, AXES, shift_pairs(1, by)))
    own_parts = [[both], [around[0]], [around[1]], beyond]
    other_parts = []
    for group in own_parts:
        other_parts.append([lax.ppermute(part, "tp", swap) for part in group])
    pieces = (own_parts, other_parts)
    state = ()
    for call in range(len(CALLS)):
        operands = (
            (query_nope, query_rope, received, key_up, cosine, sine) if call == 0 else (q4, qabs, *state)
        )
        if call == len(CALLS) - 1:
            operands = (*operands, value_up, out_proj, residual)
        state = attention(call, table, operands, [part for own, k3 in CALLS[call] for part in pieces[own][k3]])
        if call == 0:
            qabs, q4, *state = state
    home_same, home_cross, away_same, away_cross, out_early, residual = state[:6]
    mirror_same = lax.ppermute(away_same, AXES, mirror)
    mirror_cross = lax.ppermute(away_cross, AXES, crossing)
    swapped = lax.ppermute(home_cross, "tp", swap)
    messages = (home_same, mirror_same, swapped, mirror_cross)

    hidden, outgoing = project(
        tp_index.reshape(1).astype(jnp.int32), messages, out_early, out_proj, residual, norm_gain[None, :], slots_across
    )
    width = residual.shape[1]
    arrived = lax.all_to_all(
        outgoing.reshape(N_SP, CAP, width), "sp", split_axis=0, concat_axis=0, tiled=True
    ).reshape(N_SP * CAP, width)
    own_weights = (w_gate[0], w_up[0], w_down[0])
    other_weights = [lax.ppermute(w, "tp", swap) for w in own_weights]
    produced = experts(arrived, own_weights, other_weights)
    back = lax.all_to_all(
        produced.reshape(N_SP, CAP, width), "sp", split_axis=0, concat_axis=0, tiled=True
    ).reshape(N_SP * CAP, width)
    return combine(back, hidden, slots, route_weight)


def solution(mesh):
    return jax.shard_map(
        local,
        mesh=mesh,
        in_specs=(
            P(("sp", "tp"), None),
            P("sp", "tp"),
            P("sp", "tp"),
            P(("sp", "tp"), None),
            P(("sp", "tp"), None),
            P(None, "tp"),
            P(None, "tp"),
            P(),
            P(),
            P(("sp", "tp"), None),
            P(("sp", "tp"), None),
            P("sp", None, "tp"),
            P("sp", None, "tp"),
            P("sp", "tp", None),
        ),
        out_specs=P(("sp", "tp"), None),
        check_vma=False,
    )
```

```python
import functools
import jax
import jax.numpy as jnp
import numpy as np
from jax import lax
from jax.experimental import pallas as pl
from jax.experimental.pallas import tpu as pltpu
from jax.sharding import PartitionSpec as P

QK_NOPE = 128
QK_ROPE = 64
V_DIM = 128
LATENT = 256
SEGMENT = 64
EPSILON = 1e-06
ROPE_BASE = 10000.0
NEG_LARGE = -1e30

N_SP = 64
N_TP = 2
HEADS_HERE = 4
ROWS = 128
SHARD = 160
UNIT = 4
KEYS = UNIT * ROWS
QROWS = HEADS_HERE * ROWS
CAP = 8
AXES = ("sp", "tp")
STEP = {"x": 1, "y": 4, "z": 16}
Z_FIRST = {(0, 0): (3, 0), (1, 0): (2, 0), (0, 1): (1, 0), (1, 1): (0, 0), (2, 1): (1, 1), (3, 1): (0, 1), (2, 0): (3, 1), (3, 0): (2, 1)}
Z_SECOND = {(0, 1): (2, 0), (1, 1): (3, 0), (2, 0): (0, 1), (3, 0): (1, 1)}
ORDER = (("y", "x"), ("x", "y"))
SHIFTS = (0, 1, -1, 2)
SCALE2 = float((QK_NOPE + QK_ROPE) ** (-0.5) * np.log2(np.e))
PLANE = 16
GROUPS = 4
CHUNK = 64
MESSAGE = HEADS_HERE * V_DIM + 128
EARLY = 1024


def moved(s, dim, by):
    step = STEP[dim]
    c = (s // step) % 4
    return s + step * ((c + by) % 4 - c)


def shift_pairs(phase, by):
    return [
        (s * N_TP + t, moved(s, ORDER[t][phase], by) * N_TP + t)
        for s in range(N_SP)
        for t in range(N_TP)
    ]


def partner(s):
    z, y, x = s // 16, (s // 4) % 4, s % 4
    return (3 - z) * 16 + (3 - y) * 4 + x


def shard_source(s, t, k2, kz):
    s = moved(s, ORDER[t][0], -SHIFTS[k2])
    z, r = divmod(s, PLANE)
    source = (z, t)
    if kz == 1:
        source = Z_FIRST[source]
    elif source in Z_SECOND:
        source = Z_SECOND[source]
    return source[0] * PLANE + r, source[1]


def plane_pairs(table):
    return [
        ((from_z * PLANE + r) * N_TP + from_core, (z * PLANE + r) * N_TP + core)
        for (z, core), (from_z, from_core) in table.items()
        for r in range(PLANE)
    ]


def shard_first(s, t, k3, k2, kz):
    chip, core = shard_source(moved(s, ORDER[t][1], -SHIFTS[k3]), t, k2, kz)
    return 4 * chip + 2 * core


CALLS = (((0, 0), (1, 0)), ((0, 1), (0, 2)), ((1, 1), (1, 2)), ((0, 3), (1, 3)))


@functools.lru_cache(None)
def work_table(call):
    lists = []
    for s in range(N_SP):
        for t in range(N_TP):
            firsts = [
                shard_first(s, t if own == 0 else 1 - t, k3, k2, kz)
                for own, k3 in CALLS[call]
                for k2 in range(4)
                for kz in range(2)
            ]
            rows = []
            for group in range(GROUPS):
                block = s if group < 2 else partner(s)
                base = 4 * block + 2 * (group % 2)
                needed = [n for n in range(len(firsts)) if firsts[n] <= base + 1]
                for at in range(0, len(needed), UNIT):
                    part = needed[at : at + UNIT]
                    segs = [firsts[n] for n in part] + [1 << 20] * (UNIT - len(part))
                    part = part + [part[-1]] * (UNIT - len(part))
                    bits = 0
                    for half in range(2):
                        for j in range(UNIT):
                            for late in range(2):
                                if segs[j] + half > base + late:
                                    bits |= 1 << ((half * UNIT + j) * 2 + late)
                    rows.append([group, bits, t] + part)
            lists.append(rows)
    count = max(len(rows) for rows in lists)
    everything = (1 << (4 * UNIT)) - 1
    idle = lambda rows, t: rows[-1][:1] + [everything] + rows[-1][2:] if rows else [0, everything, t] + [0] * UNIT
    table = []
    for n, rows in enumerate(lists):
        table.append(rows + [idle(rows, n % N_TP)] * (count + 1 - len(rows)))
    return count, np.array(table, np.int32).reshape(len(lists), -1)


NT = (((1,), (1,)), ((), ()))


def attention_body(call, steps, offset, part_count, table, *rest):
    first, last = call == 0, call == len(CALLS) - 1
    rest = list(rest)
    take = lambda n: [rest.pop(0) for _ in range(n)]
    if first:
        own_ref, own_rope_ref, received_ref, key_up_ref, cosine_ref, sine_ref = take(6)
    else:
        q4_ref, qabs, _, _, _ = take(5)
    if last:
        value_up_ref, out_proj_hbm, residual_hbm = take(3)
    parts = take(part_count)
    if last:
        home_same, home_cross, away_same, away_cross, out_proj_ref, residual_ref = take(6)
    if first:
        qabs, q4_ref = take(2)
    m_ref, l_ref, acc_ref, keys, s0, s1, p0, p1, shrink0, shrink1 = take(10)
    fetches = []
    if last:
        (sems,) = rest
        early = pl.ds(0, out_proj_ref.shape[1])
        for n, (source, target) in enumerate(((out_proj_hbm.at[:, early], out_proj_ref), (residual_hbm, residual_ref))):
            fetch = pltpu.make_async_copy(source, target, sems.at[n])
            fetch.start()
            fetches.append(fetch)
    at = 0
    for part in parts:
        for k in range(2):
            keys[k, pl.ds(at, part.shape[0]), :] = part[:, pl.ds(k * 128, 128)]
        at += part.shape[0]
    if first:
        for g in range(GROUPS):
            source = own_ref if g < 2 else received_ref
            for h in range(HEADS_HERE):
                cols = pl.ds(h * QK_NOPE, QK_NOPE)
                latent_query = lax.dot_general(
                    source[pl.ds((g % 2) * ROWS, ROWS), cols],
                    key_up_ref[:, cols],
                    NT,
                    preferred_element_type=jnp.float32,
                ).astype(jnp.bfloat16)
                for k in range(2):
                    qabs[g, k, pl.ds(h * ROWS, ROWS), :] = latent_query[:, k * 128 : (k + 1) * 128]
        lane = lax.broadcasted_iota(jnp.int32, (ROWS, 128), 1)
        for g in range(GROUPS):
            tokens = pl.ds((g % 2) * ROWS, ROWS)
            for k in range(2):
                cols = pl.ds(k * 128, 128)
                if g < 2:
                    x = own_rope_ref[tokens, cols]
                else:
                    x = received_ref[tokens, pl.ds(HEADS_HERE * QK_NOPE + k * 128, 128)]
                x = x.astype(jnp.float32)
                opposite = jnp.where(lane % QK_ROPE < QK_ROPE // 2, pltpu.roll(x, 96, 1), pltpu.roll(x, 32, 1))
                at = pl.ds(g * ROWS, ROWS)
                turned = (x * cosine_ref[at, cols] + opposite * sine_ref[at, cols]).astype(jnp.bfloat16).astype(jnp.float32)
                flipped = pltpu.roll(turned, QK_ROPE, 1)
                for odd in range(2):
                    rows = pl.ds((2 * k + odd) * ROWS, ROWS)
                    for half in range(2):
                        source = turned if odd == half else flipped
                        keep = lane < QK_ROPE if half == 0 else lane >= QK_ROPE
                        q4_ref[g, half, rows, :] = jnp.where(keep, source, 0.0).astype(jnp.bfloat16)
        m_ref[...] = jnp.full(m_ref.shape, NEG_LARGE, jnp.float32)
        l_ref[...] = jnp.zeros(l_ref.shape, jnp.float32)
        acc_ref[...] = jnp.zeros(acc_ref.shape, jnp.float32)

    cols_per_step = 3 + UNIT

    def field(u, n):
        return table[offset + u * cols_per_step + n]

    def wide(at, count):
        rows = pl.ds(pl.multiple_of(at, 32), count)
        return jnp.concatenate([keys[k, rows, :] for k in range(2)], axis=1)

    def latent_tile(u, half):
        return jnp.concatenate([wide(field(u, 3 + j) * SHARD + half * SEGMENT, SEGMENT) for j in range(UNIT)], axis=0)

    note_lane = lax.broadcasted_iota(jnp.int32, (16, 128), 1)
    mark = [jnp.where(note_lane == n, 1.0, 0.0).astype(jnp.bfloat16) for n in range(2)]
    marks = jnp.concatenate(([mark[0]] * (SEGMENT // 16) + [mark[1]] * (SEGMENT // 16)) * HEADS_HERE, axis=0)

    def scores(u, s_ref):
        g = field(u, 0)
        bits = field(u, 1)
        rot = jnp.concatenate(
            [
                keys[h, pl.ds(pl.multiple_of(field(u, 3 + j) * SHARD + ROWS, 32), 32), :]
                for j in range(UNIT)
                for h in range(2)
            ],
            axis=0,
        )
        q = jnp.concatenate([qabs[g, k] for k in range(2)], axis=1)
        for half in range(2):
            notes = []
            for j in range(UNIT):
                at = (half * UNIT + j) * 2
                early, late = (
                    jnp.where((bits >> (at + n)) & 1 == 1, jnp.float32(NEG_LARGE), jnp.float32(0.0)) for n in range(2)
                )
                note = jnp.where(note_lane == 0, early, jnp.where(note_lane == 1, late, 0.0)).astype(jnp.bfloat16)
                notes += [note] * (SEGMENT // 16)
            extra = jnp.concatenate([rot, jnp.concatenate(notes, axis=0)], axis=1)
            total = lax.dot_general(
                q, latent_tile(u, half), NT, preferred_element_type=jnp.float32
            ) + lax.dot_general(
                jnp.concatenate([q4_ref[g, half], marks], axis=1), extra, NT, preferred_element_type=jnp.float32
            )
            for k in range(2):
                s_ref[half * 2 + k, pl.ds(0, QROWS), :] = total[:, k * 128 : (k + 1) * 128]

    def absorb(u, s_ref, p_ref, shrink_ref):
        g = field(u, 0)
        for at in range(0, QROWS, CHUNK):
            rows = pl.ds(at, CHUNK)
            s = [s_ref[k, rows, :] for k in range(KEYS // 128)]
            before = m_ref[g, rows, :]
            top = jnp.maximum(jnp.maximum(s[0], s[1]), jnp.maximum(s[2], s[3]))
            after = jnp.maximum(before, jnp.max(top, axis=1, keepdims=True))
            m_ref[g, rows, :] = after
            shrink = jnp.exp2((before - after) * SCALE2)
            shrink_ref[rows, :] = shrink
            after = after * SCALE2
            partial = l_ref[g, rows, :] * shrink
            for k in range(KEYS // 128):
                p = jnp.exp2(s[k] * SCALE2 - after)
                partial = partial + p
                p_ref[k, rows, :] = p.astype(jnp.bfloat16)
            l_ref[g, rows, :] = partial
        values = jnp.concatenate([latent_tile(u, 0), latent_tile(u, 1)], axis=0)
        for at in range(0, QROWS, QROWS // 2):
            rows = pl.ds(at, QROWS // 2)
            weights = jnp.concatenate([p_ref[k, rows, :] for k in range(KEYS // 128)], axis=1)
            product = jnp.dot(weights, values, preferred_element_type=jnp.float32)
            for k in range(LATENT // 128):
                acc_ref[g, k, rows, :] = (
                    acc_ref[g, k, rows, :] * shrink_ref[rows, :] + product[:, k * 128 : (k + 1) * 128]
                )

    scores(0, s0)

    def pair(k, carry):
        u = k * 2
        scores(u + 1, s1)
        absorb(u, s0, p0, shrink0)
        scores(u + 2, s0)
        absorb(u + 1, s1, p1, shrink1)
        return carry

    lax.fori_loop(0, (steps - 1) // 2, pair, 0)
    if steps % 2 == 0:
        scores(steps - 1, s1)
        absorb(steps - 2, s0, p0, shrink0)
        absorb(steps - 1, s1, p1, shrink1)
    else:
        absorb(steps - 1, s0, p0, shrink0)
    if not last:
        return
    core = field(0, 2)
    lane = lax.broadcasted_iota(jnp.int32, (ROWS, 128), 1)
    targets = ((home_same, core), (home_cross, 1 - core), (away_same, 2 + core), (away_cross, 3 - core))
    for target, g in targets:
        total = jnp.sum(l_ref[g], axis=1, keepdims=True)
        total = jnp.where(total > 0.0, total, 1.0)
        inverse = 1.0 / total
        mean = jnp.concatenate([acc_ref[g, k] * inverse for k in range(2)], axis=1).astype(jnp.bfloat16)
        size = m_ref[g] * SCALE2 + jnp.log2(total)
        notes = jnp.zeros((ROWS, 128), jnp.bfloat16)
        for h in range(HEADS_HERE):
            cols = pl.ds(h * V_DIM, V_DIM)
            rows = slice(h * ROWS, (h + 1) * ROWS)
            target[:, cols] = jnp.dot(
                mean[rows], value_up_ref[:, cols], preferred_element_type=jnp.float32
            ).astype(jnp.bfloat16)
            left = size[rows]
            for n in range(3):
                term = left.astype(jnp.bfloat16)
                notes = jnp.where(lane == n * HEADS_HERE + h, term, notes)
                left = left - term.astype(jnp.float32)
        target[:, pl.ds(HEADS_HERE * V_DIM, 128)] = notes
    for fetch in fetches:
        fetch.wait()


def attention(call, table, operands, parts):
    vmem = pl.BlockSpec(memory_space=pltpu.VMEM)
    hbm = pl.BlockSpec(memory_space=pltpu.HBM)
    steps = work_table(call)[0]
    offset = sum(work_table(n)[1].shape[1] for n in range(call))
    first, last = call == 0, call == len(CALLS) - 1
    outs = [
        pltpu.VMEM((GROUPS, QROWS, 128), jnp.float32),
        pltpu.VMEM((GROUPS, QROWS, 128), jnp.float32),
        pltpu.VMEM((GROUPS, 2, QROWS, 128), jnp.float32),
    ]
    specs = [vmem] * len(operands)
    scratch = []
    aliases = {}
    if first:
        outs = [pltpu.VMEM((GROUPS, 2, QROWS, 128), jnp.bfloat16)] * 2 + outs
    elif last:
        fetched = operands[-2:]
        outs = [
            *[pltpu.VMEM((ROWS, MESSAGE), jnp.bfloat16)] * 4,
            pltpu.VMEM((fetched[0].shape[0], EARLY), jnp.bfloat16),
            pltpu.VMEM(fetched[1].shape, jnp.bfloat16),
        ] + outs
        specs = specs[:-2] + [hbm] * 2
        operands = (*operands[:-2], *[in_hbm(f) for f in fetched])
        scratch = [pltpu.SemaphoreType.DMA((2,))]
    if not first:
        aliases = {3 + n: len(outs) - 3 + n for n in range(3)}
        operands = tuple(in_vmem(x) if 1 <= n < 5 else x for n, x in enumerate(operands))
    work = steps * QROWS * KEYS * 3 * LATENT * 2
    return pl.pallas_call(
        functools.partial(attention_body, call, steps, offset, len(parts)),
        out_shape=outs,
        in_specs=[pl.BlockSpec(memory_space=pltpu.SMEM)] + specs + [vmem] * len(parts),
        out_specs=[vmem] * len(outs),
        input_output_aliases=aliases,
        scratch_shapes=[
            pltpu.VMEM((2, sum(part.shape[0] for part in parts), 128), jnp.bfloat16),
            pltpu.VMEM((KEYS // 128, QROWS, 128), jnp.float32),
            pltpu.VMEM((KEYS // 128, QROWS, 128), jnp.float32),
            pltpu.VMEM((KEYS // 128, QROWS, 128), jnp.bfloat16),
            pltpu.VMEM((KEYS // 128, QROWS, 128), jnp.bfloat16),
            pltpu.VMEM((QROWS, 128), jnp.float32),
            pltpu.VMEM((QROWS, 128), jnp.float32),
        ]
        + scratch,
        cost_estimate=pl.CostEstimate(
            flops=work, bytes_accessed=2**20, transcendentals=steps * QROWS * KEYS
        ),
        compiler_params=pltpu.CompilerParams(vmem_limit_bytes=24 * 2**20),
    )(table, *operands, *[in_vmem(part) for part in parts])


def in_vmem(x):
    return pltpu.with_memory_space_constraint(x, pltpu.VMEM)


def in_hbm(x):
    return pltpu.with_memory_space_constraint(x, pltpu.HBM)


def merged(one, two):
    width = HEADS_HERE * V_DIM
    outs = []
    for h in range(HEADS_HERE):
        sizes = []
        for part in (one, two):
            notes = part[:, width : width + 128].astype(jnp.float32)
            sizes.append(
                notes[:, h : h + 1] + notes[:, HEADS_HERE + h : HEADS_HERE + h + 1]
                + notes[:, 2 * HEADS_HERE + h : 2 * HEADS_HERE + h + 1]
            )
        most = jnp.maximum(sizes[0], sizes[1])
        first, second = (jnp.exp2(size - most) for size in sizes)
        cols = slice(h * V_DIM, (h + 1) * V_DIM)
        inverse = 1.0 / (first + second)
        value = (first * inverse) * one[:, cols].astype(jnp.float32) + (second * inverse) * two[:, cols].astype(
            jnp.float32
        )
        outs.append(value.astype(jnp.bfloat16))
    return jnp.concatenate(outs, axis=1)


PIECES = 4


def project_body(
    core, local_part, mirror_same, swapped, mirror_cross, gain, slots, residual, out_early, out_proj_hbm,
    hidden_hbm, outgoing_hbm, hidden, outgoing, out_late, out_sems, late_sem,
):
    fetch = pltpu.make_async_copy(out_proj_hbm.at[:, pl.ds(EARLY, out_late.shape[1])], out_late, late_sem)
    fetch.start()
    half = HEADS_HERE * V_DIM
    mine = merged(local_part[...], mirror_same[...])
    theirs = merged(swapped[...], mirror_cross[...])
    at = pl.multiple_of(core[0] * half, half)
    other = pl.multiple_of((1 - core[0]) * half, half)
    projected = []
    for weights in (out_early, out_late):
        if weights is out_late:
            fetch.wait()
        projected.append(
            jnp.dot(mine, weights[pl.ds(at, half), :], preferred_element_type=jnp.float32)
            + jnp.dot(theirs, weights[pl.ds(other, half), :], preferred_element_type=jnp.float32)
        )
    projected = jnp.concatenate(projected, axis=1)
    result = (residual[...].astype(jnp.float32) + projected).astype(jnp.bfloat16)
    hidden[...] = result
    store = pltpu.make_async_copy(hidden, hidden_hbm, out_sems.at[PIECES])
    store.start()
    wide = result.astype(jnp.float32)
    normed = wide * lax.rsqrt(jnp.mean(wide * wide, axis=-1, keepdims=True) + EPSILON)
    normed = (normed * gain[...]).astype(jnp.bfloat16)
    count = outgoing.shape[0] // PIECES
    stores = [store]
    for n in range(PIECES):
        slot = lax.broadcasted_iota(jnp.int32, (count, normed.shape[0]), 0) + n * count
        pick = (slot == slots[0:1, :]) | (slot == slots[1:2, :])
        pick = jnp.where(pick, 1.0, 0.0).astype(jnp.bfloat16)
        rows = pl.ds(n * count, count)
        outgoing[rows, :] = jnp.dot(pick, normed, preferred_element_type=jnp.float32).astype(jnp.bfloat16)
        store = pltpu.make_async_copy(outgoing.at[rows], outgoing_hbm.at[rows], out_sems.at[n])
        store.start()
        stores.append(store)
    for store in stores:
        store.wait()


def project(core, messages, out_early, out_proj, residual, gain, slots):
    width = residual.shape[1]
    vmem = pl.BlockSpec(memory_space=pltpu.VMEM)
    hbm = pl.BlockSpec(memory_space=pltpu.HBM)
    return pl.pallas_call(
        project_body,
        out_shape=(
            pltpu.HBM((ROWS, width), jnp.bfloat16),
            pltpu.HBM((N_SP * CAP, width), jnp.bfloat16),
        ),
        in_specs=[pl.BlockSpec(memory_space=pltpu.SMEM)] + [vmem] * 8 + [hbm],
        out_specs=(hbm, hbm),
        scratch_shapes=[
            pltpu.VMEM((ROWS, width), jnp.bfloat16),
            pltpu.VMEM((N_SP * CAP, width), jnp.bfloat16),
            pltpu.VMEM((out_proj.shape[0], width - EARLY), jnp.bfloat16),
            pltpu.SemaphoreType.DMA((PIECES + 1,)),
            pltpu.SemaphoreType.DMA,
        ],
        compiler_params=pltpu.CompilerParams(vmem_limit_bytes=16 * 2**20),
        name="project",
    )(core, *messages, gain, slots, in_vmem(residual), in_vmem(out_early), in_hbm(out_proj))


def experts_body(rows, *rest):
    sources = rest[:6]
    out_hbm = rest[6]
    weights = rest[7:13]
    first, out, sems, out_sems = rest[13:]
    loads = []
    for n in range(6):
        load = pltpu.make_async_copy(sources[n], weights[n], sems.at[n])
        load.start()
        loads.append(load)
    count = rows.shape[0]
    block = count // 2
    stores = []
    for n in range(2):
        gate, up, down = weights[3 * n : 3 * n + 3]
        parts = []
        for weight, load in ((gate, loads[3 * n]), (up, loads[3 * n + 1])):
            load.wait()
            parts.append(
                [
                    jnp.dot(rows[pl.ds(k * block, block), :], weight[...], preferred_element_type=jnp.float32)
                    for k in range(2)
                ]
            )
        actives = [
            (gated / (1.0 + jnp.exp(-gated)) * raised).astype(jnp.bfloat16) for gated, raised in zip(*parts)
        ]
        loads[3 * n + 2].wait()
        for k in range(2):
            at = pl.ds(k * block, block)
            product = jnp.dot(actives[k], down[...], preferred_element_type=jnp.float32).astype(jnp.bfloat16)
            if n == 0:
                first[at, :] = product
            else:
                out[at, :] = (first[at, :].astype(jnp.float32) + product.astype(jnp.float32)).astype(jnp.bfloat16)
                store = pltpu.make_async_copy(out.at[at], out_hbm.at[at], out_sems.at[k])
                store.start()
                stores.append(store)
    for store in stores:
        store.wait()


def experts(rows, own, other):
    count, width = rows.shape
    hbm = pl.BlockSpec(memory_space=pltpu.HBM)
    return pl.pallas_call(
        experts_body,
        out_shape=pltpu.HBM((count, width), jnp.bfloat16),
        in_specs=[pl.BlockSpec(memory_space=pltpu.VMEM)] + [hbm] * 6,
        out_specs=hbm,
        scratch_shapes=[pltpu.VMEM(w.shape, w.dtype) for w in (*own, *other)]
        + [
            pltpu.VMEM((count, width), jnp.bfloat16),
            pltpu.VMEM((count, width), jnp.bfloat16),
            pltpu.SemaphoreType.DMA((6,)),
            pltpu.SemaphoreType.DMA((2,)),
        ],
        compiler_params=pltpu.CompilerParams(vmem_limit_bytes=28 * 2**20),
        name="experts",
    )(rows, *[in_hbm(w) for w in (*own, *other)])


def combine_body(back, hidden, slots, weights, out_ref):
    slot = lax.broadcasted_iota(jnp.int32, (hidden.shape[0], back.shape[0]), 1)
    pick = jnp.where(slot == slots[:, 0:1], weights[:, 0:1], 0.0) + jnp.where(
        slot == slots[:, 1:2], weights[:, 1:2], 0.0
    )
    high = pick.astype(jnp.bfloat16)
    low = (pick - high.astype(jnp.float32)).astype(jnp.bfloat16)
    both = jnp.dot(jnp.concatenate([high, low], axis=0), back[...], preferred_element_type=jnp.float32)
    count = hidden.shape[0]
    mixed = both[:count] + both[count:]
    out_ref[...] = (hidden[...].astype(jnp.float32) + mixed).astype(jnp.bfloat16)


def combine(back, hidden, slots, weights):
    vmem = pl.BlockSpec(memory_space=pltpu.VMEM)
    return pl.pallas_call(
        combine_body,
        out_shape=jax.ShapeDtypeStruct(hidden.shape, jnp.bfloat16),
        in_specs=[vmem] * 4,
        out_specs=vmem,
        compiler_params=pltpu.CompilerParams(vmem_limit_bytes=16 * 2**20),
        name="combine",
    )(back, hidden, slots, weights)


def rotary(values, positions):
    half_width = values.shape[-1] // 2
    inverse = ROPE_BASE ** (-2.0 * jnp.arange(half_width, dtype=jnp.float32) / values.shape[-1])
    angles = positions.astype(jnp.float32)[:, None] * inverse[None, :]
    cosine = jnp.cos(angles)
    sine_part = jnp.sin(angles)
    if values.ndim == 3:
        cosine = cosine[:, None, :]
        sine_part = sine_part[:, None, :]
    first_half = values[..., :half_width]
    second = values[..., half_width:]
    return jnp.concatenate(
        [first_half * cosine - second * sine_part, second * cosine + first_half * sine_part],
        axis=-1,
    )


def local(
    residual,
    query_nope,
    query_rope,
    latent,
    key_rope,
    key_up,
    value_up,
    out_proj,
    norm_gain,
    routes,
    route_weight,
    w_gate,
    w_up,
    w_down,
):
    tp_index = lax.axis_index("tp")
    sp_index = lax.axis_index("sp")
    tok_dev = query_nope.shape[0]
    query_first = sp_index * tok_dev
    swap = [(0, 1), (1, 0)]

    key_pos = query_first + tp_index * ROWS + jnp.arange(ROWS, dtype=jnp.int32)
    key_rot = rotary(key_rope.astype(jnp.float32), key_pos).astype(jnp.bfloat16)
    packed = jnp.concatenate([key_rot[0:32], key_rot[64:96], key_rot[32:64], key_rot[96:128]], axis=1)
    shard = jnp.concatenate([latent, packed], axis=0)
    mirror = [
        (s * N_TP + t, partner(s) * N_TP + t) for s in range(N_SP) for t in range(N_TP)
    ]
    crossing = [
        (s * N_TP + t, partner(s) * N_TP + 1 - t) for s in range(N_SP) for t in range(N_TP)
    ]
    queries = jnp.concatenate([query_nope, query_rope], axis=1)
    received = lax.ppermute(queries, AXES, mirror)

    near = lax.ppermute(shard, AXES, plane_pairs(Z_FIRST))
    far = lax.ppermute(shard, AXES, plane_pairs(Z_SECOND))
    main = (tp_index == 0) == (sp_index < 2 * PLANE)
    both = jnp.concatenate([jnp.where(main, shard, far), near], axis=0)
    flat = routes.reshape(-1)
    order = jnp.arange(flat.shape[0], dtype=jnp.int32)
    earlier = (flat[:, None] == flat[None, :]) & (order[None, :] < order[:, None])
    rank = jnp.sum(earlier.astype(jnp.int32), axis=1)
    slots = (flat * CAP + rank).reshape(routes.shape)
    slots_across = slots.T
    tables = np.concatenate([work_table(call)[1] for call in range(len(CALLS))], axis=1)
    table = lax.dynamic_index_in_dim(jnp.asarray(tables), sp_index * N_TP + tp_index, 0, keepdims=False)
    tokens = jnp.arange(tok_dev, dtype=jnp.int32)
    query_pos = jnp.concatenate([query_first + tokens, partner(sp_index) * tok_dev + tokens])
    half_width = QK_ROPE // 2
    pair = jnp.arange(HEADS_HERE * QK_ROPE, dtype=jnp.int32) % half_width
    inverse = ROPE_BASE ** (-2.0 * pair.astype(jnp.float32) / QK_ROPE)
    angles = query_pos.astype(jnp.float32)[:, None] * inverse[None, :]
    behind = jnp.arange(HEADS_HERE * QK_ROPE, dtype=jnp.int32) % QK_ROPE >= half_width
    cosine = jnp.cos(angles)
    sine = jnp.where(behind[None, :], jnp.sin(angles), -jnp.sin(angles))
    got = [both]
    for by in SHIFTS[1:]:
        got.append(lax.ppermute(both, AXES, shift_pairs(0, by)))
    both = jnp.concatenate(got, axis=0)
    both, table, slots, slots_across, cosine, sine = lax.optimization_barrier(
        (both, table, slots, slots_across, cosine, sine)
    )
    around = []
    for by in (1, -1):
        around.append(lax.ppermute(both, AXES, shift_pairs(1, by)))
    half = both.shape[0] // 2
    beyond = []
    for n, by in enumerate((1, -1)):
        passed = around[n][n * half : (n + 1) * half]
        beyond.append(lax.ppermute(passed, AXES, shift_pairs(1, by)))
    own_parts = [[both], [around[0]], [around[1]], beyond]
    other_parts = []
    for group in own_parts:
        other_parts.append([lax.ppermute(part, "tp", swap) for part in group])
    pieces = (own_parts, other_parts)
    state = ()
    for call in range(len(CALLS)):
        operands = (
            (query_nope, query_rope, received, key_up, cosine, sine) if call == 0 else (q4, qabs, *state)
        )
        if call == len(CALLS) - 1:
            operands = (*operands, value_up, out_proj, residual)
        state = attention(call, table, operands, [part for own, k3 in CALLS[call] for part in pieces[own][k3]])
        if call == 0:
            qabs, q4, *state = state
    home_same, home_cross, away_same, away_cross, out_early, residual = state[:6]
    mirror_same = lax.ppermute(away_same, AXES, mirror)
    mirror_cross = lax.ppermute(away_cross, AXES, crossing)
    swapped = lax.ppermute(home_cross, "tp", swap)
    messages = (home_same, mirror_same, swapped, mirror_cross)

    hidden, outgoing = project(
        tp_index.reshape(1).astype(jnp.int32), messages, out_early, out_proj, residual, norm_gain[None, :], slots_across
    )
    width = residual.shape[1]
    arrived = lax.all_to_all(
        outgoing.reshape(N_SP, CAP, width), "sp", split_axis=0, concat_axis=0, tiled=True
    ).reshape(N_SP * CAP, width)
    own_weights = (w_gate[0], w_up[0], w_down[0])
    other_weights = [lax.ppermute(w, "tp", swap) for w in own_weights]
    produced = experts(arrived, own_weights, other_weights)
    back = lax.all_to_all(
        produced.reshape(N_SP, CAP, width), "sp", split_axis=0, concat_axis=0, tiled=True
    ).reshape(N_SP * CAP, width)
    return combine(back, hidden, slots, route_weight)


def solution(mesh):
    return jax.shard_map(
        local,
        mesh=mesh,
        in_specs=(
            P(("sp", "tp"), None),
            P("sp", "tp"),
            P("sp", "tp"),
            P(("sp", "tp"), None),
            P(("sp", "tp"), None),
            P(None, "tp"),
            P(None, "tp"),
            P(),
            P(),
            P(("sp", "tp"), None),
            P(("sp", "tp"), None),
            P("sp", None, "tp"),
            P("sp", None, "tp"),
            P("sp", "tp", None),
        ),
        out_specs=P(("sp", "tp"), None),
        check_vma=False,
    )
```

```python
import functools
import jax
import jax.numpy as jnp
import numpy as np
from jax import lax
from jax.experimental import pallas as pl
from jax.experimental.pallas import tpu as pltpu
from jax.sharding import PartitionSpec as P

QK_NOPE = 128
QK_ROPE = 64
V_DIM = 128
LATENT = 256
SEGMENT = 64
EPSILON = 1e-06
ROPE_BASE = 10000.0
NEG_LARGE = -1e30

N_SP = 64
N_TP = 2
HEADS_HERE = 4
ROWS = 128
SHARD = 160
UNIT = 4
KEYS = UNIT * ROWS
QROWS = HEADS_HERE * ROWS
CAP = 8
AXES = ("sp", "tp")
STEP = {"x": 1, "y": 4, "z": 16}
Z_FIRST = {(0, 0): (3, 0), (1, 0): (2, 0), (0, 1): (1, 0), (1, 1): (0, 0), (2, 1): (1, 1), (3, 1): (0, 1), (2, 0): (3, 1), (3, 0): (2, 1)}
Z_SECOND = {(0, 1): (2, 0), (1, 1): (3, 0), (2, 0): (0, 1), (3, 0): (1, 1)}
ORDER = (("y", "x"), ("x", "y"))
SHIFTS = (0, 1, -1, 2)
SCALE2 = float((QK_NOPE + QK_ROPE) ** (-0.5) * np.log2(np.e))
PLANE = 16
GROUPS = 4
CHUNK = 64
MESSAGE = HEADS_HERE * V_DIM + 128
EARLY = 1024


def moved(s, dim, by):
    step = STEP[dim]
    c = (s // step) % 4
    return s + step * ((c + by) % 4 - c)


def shift_pairs(phase, by):
    return [
        (s * N_TP + t, moved(s, ORDER[t][phase], by) * N_TP + t)
        for s in range(N_SP)
        for t in range(N_TP)
    ]


def partner(s):
    z, y, x = s // 16, (s // 4) % 4, s % 4
    return (3 - z) * 16 + (3 - y) * 4 + x


def shard_source(s, t, k2, kz):
    s = moved(s, ORDER[t][0], -SHIFTS[k2])
    z, r = divmod(s, PLANE)
    source = (z, t)
    if kz == 1:
        source = Z_FIRST[source]
    elif source in Z_SECOND:
        source = Z_SECOND[source]
    return source[0] * PLANE + r, source[1]


def plane_pairs(table):
    return [
        ((from_z * PLANE + r) * N_TP + from_core, (z * PLANE + r) * N_TP + core)
        for (z, core), (from_z, from_core) in table.items()
        for r in range(PLANE)
    ]


def shard_first(s, t, k3, k2, kz):
    chip, core = shard_source(moved(s, ORDER[t][1], -SHIFTS[k3]), t, k2, kz)
    return 4 * chip + 2 * core


CALLS = (((0, 0), (1, 0)), ((0, 1), (0, 2)), ((1, 1), (1, 2)), ((0, 3), (1, 3)))


@functools.lru_cache(None)
def work_table(call):
    lists = []
    for s in range(N_SP):
        for t in range(N_TP):
            firsts = [
                shard_first(s, t if own == 0 else 1 - t, k3, k2, kz)
                for own, k3 in CALLS[call]
                for k2 in range(4)
                for kz in range(2)
            ]
            rows = []
            for group in range(GROUPS):
                block = s if group < 2 else partner(s)
                base = 4 * block + 2 * (group % 2)
                needed = [n for n in range(len(firsts)) if firsts[n] <= base + 1]
                for at in range(0, len(needed), UNIT):
                    part = needed[at : at + UNIT]
                    segs = [firsts[n] for n in part] + [1 << 20] * (UNIT - len(part))
                    part = part + [part[-1]] * (UNIT - len(part))
                    bits = 0
                    for half in range(2):
                        for j in range(UNIT):
                            for late in range(2):
                                if segs[j] + half > base + late:
                                    bits |= 1 << ((half * UNIT + j) * 2 + late)
                    rows.append([group, bits, t] + part)
            lists.append(rows)
    count = max(len(rows) for rows in lists)
    everything = (1 << (4 * UNIT)) - 1
    idle = lambda rows, t: rows[-1][:1] + [everything] + rows[-1][2:] if rows else [0, everything, t] + [0] * UNIT
    table = []
    for n, rows in enumerate(lists):
        table.append(rows + [idle(rows, n % N_TP)] * (count + 1 - len(rows)))
    return count, np.array(table, np.int32).reshape(len(lists), -1)


NT = (((1,), (1,)), ((), ()))


def attention_body(call, steps, offset, part_count, table, *rest):
    first, last = call == 0, call == len(CALLS) - 1
    rest = list(rest)
    take = lambda n: [rest.pop(0) for _ in range(n)]
    if first:
        own_ref, own_rope_ref, received_ref, key_up_ref, cosine_ref, sine_ref = take(6)
    else:
        q4_ref, qabs, _, _, _ = take(5)
    if last:
        value_up_ref, out_proj_hbm, residual_hbm = take(3)
    parts = take(part_count)
    if last:
        home_same, home_cross, away_same, away_cross, out_proj_ref, residual_ref = take(6)
    if first:
        qabs, q4_ref = take(2)
    m_ref, l_ref, acc_ref, keys, s0, s1, p0, p1, shrink0, shrink1 = take(10)
    fetches = []
    if last:
        (sems,) = rest
        early = pl.ds(0, out_proj_ref.shape[1])
        for n, (source, target) in enumerate(((out_proj_hbm.at[:, early], out_proj_ref), (residual_hbm, residual_ref))):
            fetch = pltpu.make_async_copy(source, target, sems.at[n])
            fetch.start()
            fetches.append(fetch)
    at = 0
    for part in parts:
        for k in range(2):
            keys[k, pl.ds(at, part.shape[0]), :] = part[:, pl.ds(k * 128, 128)]
        at += part.shape[0]
    if first:
        for g in range(GROUPS):
            source = own_ref if g < 2 else received_ref
            for h in range(HEADS_HERE):
                cols = pl.ds(h * QK_NOPE, QK_NOPE)
                latent_query = lax.dot_general(
                    source[pl.ds((g % 2) * ROWS, ROWS), cols],
                    key_up_ref[:, cols],
                    NT,
                    preferred_element_type=jnp.float32,
                ).astype(jnp.bfloat16)
                for k in range(2):
                    qabs[g, k, pl.ds(h * ROWS, ROWS), :] = latent_query[:, k * 128 : (k + 1) * 128]
        lane = lax.broadcasted_iota(jnp.int32, (ROWS, 128), 1)
        for g in range(GROUPS):
            tokens = pl.ds((g % 2) * ROWS, ROWS)
            for k in range(2):
                cols = pl.ds(k * 128, 128)
                if g < 2:
                    x = own_rope_ref[tokens, cols]
                else:
                    x = received_ref[tokens, pl.ds(HEADS_HERE * QK_NOPE + k * 128, 128)]
                x = x.astype(jnp.float32)
                opposite = jnp.where(lane % QK_ROPE < QK_ROPE // 2, pltpu.roll(x, 96, 1), pltpu.roll(x, 32, 1))
                at = pl.ds(g * ROWS, ROWS)
                turned = (x * cosine_ref[at, cols] + opposite * sine_ref[at, cols]).astype(jnp.bfloat16).astype(jnp.float32)
                flipped = pltpu.roll(turned, QK_ROPE, 1)
                for odd in range(2):
                    rows = pl.ds((2 * k + odd) * ROWS, ROWS)
                    for half in range(2):
                        source = turned if odd == half else flipped
                        keep = lane < QK_ROPE if half == 0 else lane >= QK_ROPE
                        q4_ref[g, half, rows, :] = jnp.where(keep, source, 0.0).astype(jnp.bfloat16)
        m_ref[...] = jnp.full(m_ref.shape, NEG_LARGE, jnp.float32)
        l_ref[...] = jnp.zeros(l_ref.shape, jnp.float32)
        acc_ref[...] = jnp.zeros(acc_ref.shape, jnp.float32)

    cols_per_step = 3 + UNIT

    def field(u, n):
        return table[offset + u * cols_per_step + n]

    def wide(at, count):
        rows = pl.ds(pl.multiple_of(at, 32), count)
        return jnp.concatenate([keys[k, rows, :] for k in range(2)], axis=1)

    def latent_tile(u, half):
        return jnp.concatenate([wide(field(u, 3 + j) * SHARD + half * SEGMENT, SEGMENT) for j in range(UNIT)], axis=0)

    note_lane = lax.broadcasted_iota(jnp.int32, (16, 128), 1)
    mark = [jnp.where(note_lane == n, 1.0, 0.0).astype(jnp.bfloat16) for n in range(2)]
    marks = jnp.concatenate(([mark[0]] * (SEGMENT // 16) + [mark[1]] * (SEGMENT // 16)) * HEADS_HERE, axis=0)

    def scores(u, s_ref):
        g = field(u, 0)
        bits = field(u, 1)
        rot = jnp.concatenate(
            [
                keys[h, pl.ds(pl.multiple_of(field(u, 3 + j) * SHARD + ROWS, 32), 32), :]
                for j in range(UNIT)
                for h in range(2)
            ],
            axis=0,
        )
        q = jnp.concatenate([qabs[g, k] for k in range(2)], axis=1)
        for half in range(2):
            notes = []
            for j in range(UNIT):
                at = (half * UNIT + j) * 2
                early, late = (
                    jnp.where((bits >> (at + n)) & 1 == 1, jnp.float32(NEG_LARGE), jnp.float32(0.0)) for n in range(2)
                )
                note = jnp.where(note_lane == 0, early, jnp.where(note_lane == 1, late, 0.0)).astype(jnp.bfloat16)
                notes += [note] * (SEGMENT // 16)
            extra = jnp.concatenate([rot, jnp.concatenate(notes, axis=0)], axis=1)
            total = lax.dot_general(
                q, latent_tile(u, half), NT, preferred_element_type=jnp.float32
            ) + lax.dot_general(
                jnp.concatenate([q4_ref[g, half], marks], axis=1), extra, NT, preferred_element_type=jnp.float32
            )
            for k in range(2):
                s_ref[half * 2 + k, pl.ds(0, QROWS), :] = total[:, k * 128 : (k + 1) * 128]

    def absorb(u, s_ref, p_ref, shrink_ref):
        g = field(u, 0)
        for at in range(0, QROWS, CHUNK):
            rows = pl.ds(at, CHUNK)
            s = [s_ref[k, rows, :] for k in range(KEYS // 128)]
            before = m_ref[g, rows, :]
            top = jnp.maximum(jnp.maximum(s[0], s[1]), jnp.maximum(s[2], s[3]))
            after = jnp.maximum(before, jnp.max(top, axis=1, keepdims=True))
            m_ref[g, rows, :] = after
            shrink = jnp.exp2((before - after) * SCALE2)
            shrink_ref[rows, :] = shrink
            after = after * SCALE2
            partial = l_ref[g, rows, :] * shrink
            for k in range(KEYS // 128):
                p = jnp.exp2(s[k] * SCALE2 - after)
                partial = partial + p
                p_ref[k, rows, :] = p.astype(jnp.bfloat16)
            l_ref[g, rows, :] = partial
        values = jnp.concatenate([latent_tile(u, 0), latent_tile(u, 1)], axis=0)
        for at in range(0, QROWS, QROWS // 2):
            rows = pl.ds(at, QROWS // 2)
            weights = jnp.concatenate([p_ref[k, rows, :] for k in range(KEYS // 128)], axis=1)
            product = jnp.dot(weights, values, preferred_element_type=jnp.float32)
            for k in range(LATENT // 128):
                acc_ref[g, k, rows, :] = (
                    acc_ref[g, k, rows, :] * shrink_ref[rows, :] + product[:, k * 128 : (k + 1) * 128]
                )

    scores(0, s0)

    def pair(k, carry):
        u = k * 2
        scores(u + 1, s1)
        absorb(u, s0, p0, shrink0)
        scores(u + 2, s0)
        absorb(u + 1, s1, p1, shrink1)
        return carry

    lax.fori_loop(0, (steps - 1) // 2, pair, 0)
    if steps % 2 == 0:
        scores(steps - 1, s1)
        absorb(steps - 2, s0, p0, shrink0)
        absorb(steps - 1, s1, p1, shrink1)
    else:
        absorb(steps - 1, s0, p0, shrink0)
    if not last:
        return
    core = field(0, 2)
    lane = lax.broadcasted_iota(jnp.int32, (ROWS, 128), 1)
    targets = ((home_same, core), (home_cross, 1 - core), (away_same, 2 + core), (away_cross, 3 - core))
    for target, g in targets:
        total = jnp.sum(l_ref[g], axis=1, keepdims=True)
        total = jnp.where(total > 0.0, total, 1.0)
        inverse = 1.0 / total
        mean = jnp.concatenate([acc_ref[g, k] * inverse for k in range(2)], axis=1).astype(jnp.bfloat16)
        size = m_ref[g] * SCALE2 + jnp.log2(total)
        notes = jnp.zeros((ROWS, 128), jnp.bfloat16)
        for h in range(HEADS_HERE):
            cols = pl.ds(h * V_DIM, V_DIM)
            rows = slice(h * ROWS, (h + 1) * ROWS)
            target[:, cols] = jnp.dot(
                mean[rows], value_up_ref[:, cols], preferred_element_type=jnp.float32
            ).astype(jnp.bfloat16)
            left = size[rows]
            for n in range(3):
                term = left.astype(jnp.bfloat16)
                notes = jnp.where(lane == n * HEADS_HERE + h, term, notes)
                left = left - term.astype(jnp.float32)
        target[:, pl.ds(HEADS_HERE * V_DIM, 128)] = notes
    for fetch in fetches:
        fetch.wait()


def attention(call, table, operands, parts):
    vmem = pl.BlockSpec(memory_space=pltpu.VMEM)
    hbm = pl.BlockSpec(memory_space=pltpu.HBM)
    steps = work_table(call)[0]
    offset = sum(work_table(n)[1].shape[1] for n in range(call))
    first, last = call == 0, call == len(CALLS) - 1
    outs = [
        pltpu.VMEM((GROUPS, QROWS, 128), jnp.float32),
        pltpu.VMEM((GROUPS, QROWS, 128), jnp.float32),
        pltpu.VMEM((GROUPS, 2, QROWS, 128), jnp.float32),
    ]
    specs = [vmem] * len(operands)
    scratch = []
    aliases = {}
    if first:
        outs = [pltpu.VMEM((GROUPS, 2, QROWS, 128), jnp.bfloat16)] * 2 + outs
    elif last:
        fetched = operands[-2:]
        outs = [
            *[pltpu.VMEM((ROWS, MESSAGE), jnp.bfloat16)] * 4,
            pltpu.VMEM((fetched[0].shape[0], EARLY), jnp.bfloat16),
            pltpu.VMEM(fetched[1].shape, jnp.bfloat16),
        ] + outs
        specs = specs[:-2] + [hbm] * 2
        operands = (*operands[:-2], *[in_hbm(f) for f in fetched])
        scratch = [pltpu.SemaphoreType.DMA((2,))]
    if not first:
        aliases = {3 + n: len(outs) - 3 + n for n in range(3)}
        operands = tuple(in_vmem(x) if 1 <= n < 5 else x for n, x in enumerate(operands))
    work = steps * QROWS * KEYS * 3 * LATENT * 2
    return pl.pallas_call(
        functools.partial(attention_body, call, steps, offset, len(parts)),
        out_shape=outs,
        in_specs=[pl.BlockSpec(memory_space=pltpu.SMEM)] + specs + [vmem] * len(parts),
        out_specs=[vmem] * len(outs),
        input_output_aliases=aliases,
        scratch_shapes=[
            pltpu.VMEM((2, sum(part.shape[0] for part in parts), 128), jnp.bfloat16),
            pltpu.VMEM((KEYS // 128, QROWS, 128), jnp.float32),
            pltpu.VMEM((KEYS // 128, QROWS, 128), jnp.float32),
            pltpu.VMEM((KEYS // 128, QROWS, 128), jnp.bfloat16),
            pltpu.VMEM((KEYS // 128, QROWS, 128), jnp.bfloat16),
            pltpu.VMEM((QROWS, 128), jnp.float32),
            pltpu.VMEM((QROWS, 128), jnp.float32),
        ]
        + scratch,
        cost_estimate=pl.CostEstimate(
            flops=work, bytes_accessed=2**20, transcendentals=steps * QROWS * KEYS
        ),
        compiler_params=pltpu.CompilerParams(vmem_limit_bytes=24 * 2**20),
    )(table, *operands, *[in_vmem(part) for part in parts])


def in_vmem(x):
    return pltpu.with_memory_space_constraint(x, pltpu.VMEM)


def in_hbm(x):
    return pltpu.with_memory_space_constraint(x, pltpu.HBM)


def merged(one, two):
    width = HEADS_HERE * V_DIM
    outs = []
    for h in range(HEADS_HERE):
        sizes = []
        for part in (one, two):
            notes = part[:, width : width + 128].astype(jnp.float32)
            sizes.append(
                notes[:, h : h + 1] + notes[:, HEADS_HERE + h : HEADS_HERE + h + 1]
                + notes[:, 2 * HEADS_HERE + h : 2 * HEADS_HERE + h + 1]
            )
        most = jnp.maximum(sizes[0], sizes[1])
        first, second = (jnp.exp2(size - most) for size in sizes)
        cols = slice(h * V_DIM, (h + 1) * V_DIM)
        value = first * one[:, cols].astype(jnp.float32) + second * two[:, cols].astype(jnp.float32)
        outs.append((value / (first + second)).astype(jnp.bfloat16))
    return jnp.concatenate(outs, axis=1)


PIECES = 4


def project_body(
    core, local_part, mirror_same, swapped, mirror_cross, gain, slots, residual, out_early, out_proj_hbm,
    hidden_hbm, outgoing_hbm, hidden, outgoing, out_late, out_sems, late_sem,
):
    fetch = pltpu.make_async_copy(out_proj_hbm.at[:, pl.ds(EARLY, out_late.shape[1])], out_late, late_sem)
    fetch.start()
    half = HEADS_HERE * V_DIM
    mine = merged(local_part[...], mirror_same[...])
    theirs = merged(swapped[...], mirror_cross[...])
    at = pl.multiple_of(core[0] * half, half)
    other = pl.multiple_of((1 - core[0]) * half, half)
    projected = []
    for weights in (out_early, out_late):
        if weights is out_late:
            fetch.wait()
        projected.append(
            jnp.dot(mine, weights[pl.ds(at, half), :], preferred_element_type=jnp.float32)
            + jnp.dot(theirs, weights[pl.ds(other, half), :], preferred_element_type=jnp.float32)
        )
    projected = jnp.concatenate(projected, axis=1)
    result = (residual[...].astype(jnp.float32) + projected).astype(jnp.bfloat16)
    hidden[...] = result
    store = pltpu.make_async_copy(hidden, hidden_hbm, out_sems.at[PIECES])
    store.start()
    wide = result.astype(jnp.float32)
    normed = wide * lax.rsqrt(jnp.mean(wide * wide, axis=-1, keepdims=True) + EPSILON)
    normed = (normed * gain[...]).astype(jnp.bfloat16)
    count = outgoing.shape[0] // PIECES
    stores = [store]
    for n in range(PIECES):
        slot = lax.broadcasted_iota(jnp.int32, (count, normed.shape[0]), 0) + n * count
        pick = (slot == slots[0:1, :]) | (slot == slots[1:2, :])
        pick = jnp.where(pick, 1.0, 0.0).astype(jnp.bfloat16)
        rows = pl.ds(n * count, count)
        outgoing[rows, :] = jnp.dot(pick, normed, preferred_element_type=jnp.float32).astype(jnp.bfloat16)
        store = pltpu.make_async_copy(outgoing.at[rows], outgoing_hbm.at[rows], out_sems.at[n])
        store.start()
        stores.append(store)
    for store in stores:
        store.wait()


def project(core, messages, out_early, out_proj, residual, gain, slots):
    width = residual.shape[1]
    vmem = pl.BlockSpec(memory_space=pltpu.VMEM)
    hbm = pl.BlockSpec(memory_space=pltpu.HBM)
    return pl.pallas_call(
        project_body,
        out_shape=(
            pltpu.HBM((ROWS, width), jnp.bfloat16),
            pltpu.HBM((N_SP * CAP, width), jnp.bfloat16),
        ),
        in_specs=[pl.BlockSpec(memory_space=pltpu.SMEM)] + [vmem] * 8 + [hbm],
        out_specs=(hbm, hbm),
        scratch_shapes=[
            pltpu.VMEM((ROWS, width), jnp.bfloat16),
            pltpu.VMEM((N_SP * CAP, width), jnp.bfloat16),
            pltpu.VMEM((out_proj.shape[0], width - EARLY), jnp.bfloat16),
            pltpu.SemaphoreType.DMA((PIECES + 1,)),
            pltpu.SemaphoreType.DMA,
        ],
        compiler_params=pltpu.CompilerParams(vmem_limit_bytes=16 * 2**20),
        name="project",
    )(core, *messages, gain, slots, in_vmem(residual), in_vmem(out_early), in_hbm(out_proj))


def stage_body(source, after, target, sem):
    load = pltpu.make_async_copy(source, target, sem)
    load.start()
    load.wait()


def stage(x, after):
    hbm = pl.BlockSpec(memory_space=pltpu.HBM)
    return pl.pallas_call(
        stage_body,
        out_shape=pltpu.VMEM(x.shape, x.dtype),
        in_specs=[hbm, hbm],
        out_specs=pl.BlockSpec(memory_space=pltpu.VMEM),
        scratch_shapes=[pltpu.SemaphoreType.DMA],
        compiler_params=pltpu.CompilerParams(vmem_limit_bytes=2**20),
        name="stage",
    )(in_hbm(x), in_hbm(after))


def experts_body(rows, ready, *rest):
    sources = (None, *rest[:5])
    out_hbm = rest[5]
    weights = (ready, *rest[6:11])
    first, out, sems, out_sems = rest[11:]
    loads = [None]
    for n in range(1, 6):
        load = pltpu.make_async_copy(sources[n], weights[n], sems.at[n])
        load.start()
        loads.append(load)
    count = rows.shape[0]
    block = count // 2
    stores = []
    for n in range(2):
        gate, up, down = weights[3 * n : 3 * n + 3]
        parts = []
        for weight, load in ((gate, loads[3 * n]), (up, loads[3 * n + 1])):
            if load is not None:
                load.wait()
            parts.append(
                [
                    jnp.dot(rows[pl.ds(k * block, block), :], weight[...], preferred_element_type=jnp.float32)
                    for k in range(2)
                ]
            )
        actives = [
            (gated / (1.0 + jnp.exp(-gated)) * raised).astype(jnp.bfloat16) for gated, raised in zip(*parts)
        ]
        loads[3 * n + 2].wait()
        for k in range(2):
            at = pl.ds(k * block, block)
            product = jnp.dot(actives[k], down[...], preferred_element_type=jnp.float32).astype(jnp.bfloat16)
            if n == 0:
                first[at, :] = product
            else:
                out[at, :] = (first[at, :].astype(jnp.float32) + product.astype(jnp.float32)).astype(jnp.bfloat16)
                store = pltpu.make_async_copy(out.at[at], out_hbm.at[at], out_sems.at[k])
                store.start()
                stores.append(store)
    for store in stores:
        store.wait()


def experts(rows, own, other):
    count, width = rows.shape
    hbm = pl.BlockSpec(memory_space=pltpu.HBM)
    return pl.pallas_call(
        experts_body,
        out_shape=pltpu.HBM((count, width), jnp.bfloat16),
        in_specs=[pl.BlockSpec(memory_space=pltpu.VMEM)] * 2 + [hbm] * 5,
        out_specs=hbm,
        scratch_shapes=[pltpu.VMEM(w.shape, w.dtype) for w in (*own[1:], *other)]
        + [
            pltpu.VMEM((count, width), jnp.bfloat16),
            pltpu.VMEM((count, width), jnp.bfloat16),
            pltpu.SemaphoreType.DMA((6,)),
            pltpu.SemaphoreType.DMA((2,)),
        ],
        compiler_params=pltpu.CompilerParams(vmem_limit_bytes=28 * 2**20),
        name="experts",
    )(rows, in_vmem(own[0]), *[in_hbm(w) for w in (*own[1:], *other)])


def combine_body(back, hidden, slots, weights, out_ref):
    slot = lax.broadcasted_iota(jnp.int32, (hidden.shape[0], back.shape[0]), 1)
    pick = jnp.where(slot == slots[:, 0:1], weights[:, 0:1], 0.0) + jnp.where(
        slot == slots[:, 1:2], weights[:, 1:2], 0.0
    )
    high = pick.astype(jnp.bfloat16)
    low = (pick - high.astype(jnp.float32)).astype(jnp.bfloat16)
    both = jnp.dot(jnp.concatenate([high, low], axis=0), back[...], preferred_element_type=jnp.float32)
    count = hidden.shape[0]
    mixed = both[:count] + both[count:]
    out_ref[...] = (hidden[...].astype(jnp.float32) + mixed).astype(jnp.bfloat16)


def combine(back, hidden, slots, weights):
    vmem = pl.BlockSpec(memory_space=pltpu.VMEM)
    return pl.pallas_call(
        combine_body,
        out_shape=jax.ShapeDtypeStruct(hidden.shape, jnp.bfloat16),
        in_specs=[vmem] * 4,
        out_specs=vmem,
        compiler_params=pltpu.CompilerParams(vmem_limit_bytes=16 * 2**20),
        name="combine",
    )(back, hidden, slots, weights)


def rotary(values, positions):
    half_width = values.shape[-1] // 2
    inverse = ROPE_BASE ** (-2.0 * jnp.arange(half_width, dtype=jnp.float32) / values.shape[-1])
    angles = positions.astype(jnp.float32)[:, None] * inverse[None, :]
    cosine = jnp.cos(angles)
    sine_part = jnp.sin(angles)
    if values.ndim == 3:
        cosine = cosine[:, None, :]
        sine_part = sine_part[:, None, :]
    first_half = values[..., :half_width]
    second = values[..., half_width:]
    return jnp.concatenate(
        [first_half * cosine - second * sine_part, second * cosine + first_half * sine_part],
        axis=-1,
    )


def local(
    residual,
    query_nope,
    query_rope,
    latent,
    key_rope,
    key_up,
    value_up,
    out_proj,
    norm_gain,
    routes,
    route_weight,
    w_gate,
    w_up,
    w_down,
):
    tp_index = lax.axis_index("tp")
    sp_index = lax.axis_index("sp")
    tok_dev = query_nope.shape[0]
    query_first = sp_index * tok_dev
    swap = [(0, 1), (1, 0)]

    key_pos = query_first + tp_index * ROWS + jnp.arange(ROWS, dtype=jnp.int32)
    key_rot = rotary(key_rope.astype(jnp.float32), key_pos).astype(jnp.bfloat16)
    packed = jnp.concatenate([key_rot[0:32], key_rot[64:96], key_rot[32:64], key_rot[96:128]], axis=1)
    shard = jnp.concatenate([latent, packed], axis=0)
    mirror = [
        (s * N_TP + t, partner(s) * N_TP + t) for s in range(N_SP) for t in range(N_TP)
    ]
    crossing = [
        (s * N_TP + t, partner(s) * N_TP + 1 - t) for s in range(N_SP) for t in range(N_TP)
    ]
    queries = jnp.concatenate([query_nope, query_rope], axis=1)
    received = lax.ppermute(queries, AXES, mirror)

    near = lax.ppermute(shard, AXES, plane_pairs(Z_FIRST))
    far = lax.ppermute(shard, AXES, plane_pairs(Z_SECOND))
    main = (tp_index == 0) == (sp_index < 2 * PLANE)
    both = jnp.concatenate([jnp.where(main, shard, far), near], axis=0)
    flat = routes.reshape(-1)
    order = jnp.arange(flat.shape[0], dtype=jnp.int32)
    earlier = (flat[:, None] == flat[None, :]) & (order[None, :] < order[:, None])
    rank = jnp.sum(earlier.astype(jnp.int32), axis=1)
    slots = (flat * CAP + rank).reshape(routes.shape)
    slots_across = slots.T
    tables = np.concatenate([work_table(call)[1] for call in range(len(CALLS))], axis=1)
    table = lax.dynamic_index_in_dim(jnp.asarray(tables), sp_index * N_TP + tp_index, 0, keepdims=False)
    tokens = jnp.arange(tok_dev, dtype=jnp.int32)
    query_pos = jnp.concatenate([query_first + tokens, partner(sp_index) * tok_dev + tokens])
    half_width = QK_ROPE // 2
    pair = jnp.arange(HEADS_HERE * QK_ROPE, dtype=jnp.int32) % half_width
    inverse = ROPE_BASE ** (-2.0 * pair.astype(jnp.float32) / QK_ROPE)
    angles = query_pos.astype(jnp.float32)[:, None] * inverse[None, :]
    behind = jnp.arange(HEADS_HERE * QK_ROPE, dtype=jnp.int32) % QK_ROPE >= half_width
    cosine = jnp.cos(angles)
    sine = jnp.where(behind[None, :], jnp.sin(angles), -jnp.sin(angles))
    got = [both]
    for by in SHIFTS[1:]:
        got.append(lax.ppermute(both, AXES, shift_pairs(0, by)))
    both = jnp.concatenate(got, axis=0)
    both, table, slots, slots_across, cosine, sine = lax.optimization_barrier(
        (both, table, slots, slots_across, cosine, sine)
    )
    around = []
    for by in (1, -1):
        around.append(lax.ppermute(both, AXES, shift_pairs(1, by)))
    half = both.shape[0] // 2
    beyond = []
    for n, by in enumerate((1, -1)):
        passed = around[n][n * half : (n + 1) * half]
        beyond.append(lax.ppermute(passed, AXES, shift_pairs(1, by)))
    own_parts = [[both], [around[0]], [around[1]], beyond]
    other_parts = []
    for group in own_parts:
        other_parts.append([lax.ppermute(part, "tp", swap) for part in group])
    pieces = (own_parts, other_parts)
    state = ()
    for call in range(len(CALLS)):
        operands = (
            (query_nope, query_rope, received, key_up, cosine, sine) if call == 0 else (q4, qabs, *state)
        )
        if call == len(CALLS) - 1:
            operands = (*operands, value_up, out_proj, residual)
        state = attention(call, table, operands, [part for own, k3 in CALLS[call] for part in pieces[own][k3]])
        if call == 0:
            qabs, q4, *state = state
    home_same, home_cross, away_same, away_cross, out_early, residual = state[:6]
    mirror_same = lax.ppermute(away_same, AXES, mirror)
    mirror_cross = lax.ppermute(away_cross, AXES, crossing)
    swapped = lax.ppermute(home_cross, "tp", swap)
    messages = (home_same, mirror_same, swapped, mirror_cross)

    hidden, outgoing = project(
        tp_index.reshape(1).astype(jnp.int32), messages, out_early, out_proj, residual, norm_gain[None, :], slots_across
    )
    width = residual.shape[1]
    arrived = lax.all_to_all(
        outgoing.reshape(N_SP, CAP, width), "sp", split_axis=0, concat_axis=0, tiled=True
    ).reshape(N_SP * CAP, width)
    own_weights = (w_gate[0], w_up[0], w_down[0])
    other_weights = [lax.ppermute(w, "tp", swap) for w in own_weights]
    own_ready = (stage(own_weights[0], outgoing), *own_weights[1:])
    produced = experts(arrived, own_ready, other_weights)
    back = lax.all_to_all(
        produced.reshape(N_SP, CAP, width), "sp", split_axis=0, concat_axis=0, tiled=True
    ).reshape(N_SP * CAP, width)
    return combine(back, hidden, slots, route_weight)


def solution(mesh):
    return jax.shard_map(
        local,
        mesh=mesh,
        in_specs=(
            P(("sp", "tp"), None),
            P("sp", "tp"),
            P("sp", "tp"),
            P(("sp", "tp"), None),
            P(("sp", "tp"), None),
            P(None, "tp"),
            P(None, "tp"),
            P(),
            P(),
            P(("sp", "tp"), None),
            P(("sp", "tp"), None),
            P("sp", None, "tp"),
            P("sp", None, "tp"),
            P("sp", "tp", None),
        ),
        out_specs=P(("sp", "tp"), None),
        check_vma=False,
    )
```
